128 devices in a mesh: sp: 16 (over z, x), tp: 8 (over y, core).
Axes of the slice: x: 4, y: 4, z: 4, core: 2. Of those that a mesh axis runs over, the one named last changes fastest.
Arguments:
- latent: bfloat16 [12288, 2048], P(('sp', 'tp')), may hold values from -6 to 6
- context: bfloat16 [1024, 2048], P('sp'), may hold values from -6 to 6
- conditioning: float32 [2, 2048], replicated, may hold values from -6 to 6
- norm_gain: float32 [2048], replicated, may hold values from 0.1 to 1.9
- mod_shift: bfloat16 [2048, 2048], P('sp', 'tp'), may hold values from -0.1875 to 0.1875
- mod_scale: bfloat16 [2048, 2048], P('sp', 'tp'), may hold values from -0.1875 to 0.1875
- mod_gate: bfloat16 [2048, 2048], P('sp', 'tp'), may hold values from -0.1875 to 0.1875
- w_query: bfloat16 [2048, 2048], P(None, 'tp'), may hold values from -4 to 4
- w_key: bfloat16 [2048, 2048], P(None, 'tp'), may hold values from -0.125 to 0.125
- w_value: bfloat16 [2048, 2048], P(None, 'tp'), may hold values from -0.125 to 0.125
- w_out: bfloat16 [2048, 2048], P('tp'), may hold values from -0.125 to 0.125
- lambdas: float32 [16], P('tp'), may hold values from 0.3 to 0.8
- context_bias: float32 [16], P('tp'), may hold values from 0.8 to 2.2
- head_gain: float32 [128], replicated, may hold values from 0.1 to 1.9
Outputs:
- updated: bfloat16 [12288, 2048], P(('sp', 'tp'))
The draws below stay inside these ranges and needn't reach their ends.
All inputs are finite; a program needn't handle non-finite values.
Results may differ from the reference program's by a relative error of at most 0.01.
The reference program's roundings to bfloat16 on the way count: a program that leaves them out, or rounds other values in their place, can miss the bound.
Values may be sent and summed in bfloat16 or wider, within the bound.
A program may use at most 128 MiB of HBM per device.

```python
import math
import jax
import jax.numpy as jnp
from jax import lax

D = 2048
HEADS = 16
HD = 64
CTX = 1024
TOKENS = 12288
N_TP = 8


def draw_w_query(key, part):
    entries = jnp.clip(jax.random.normal(key, (D, HEADS * 2 * HD), jnp.float32), -6.0, 6.0) * D ** (-0.5)
    return jnp.clip(entries, -4.0, 4.0).astype(jnp.bfloat16)


def steps_of(stream_key, extent, cuts, low, high):
    def one(axis_at, shards_of):
        heights = jax.random.uniform(jax.random.fold_in(jax.random.fold_in(stream_key, 6), axis_at), (shards_of,), jnp.float32, low / len(cuts), high / len(cuts))
        return jnp.repeat(jnp.exp(heights), extent[axis_at] // shards_of).reshape((-1,) + (1,) * (len(extent) - axis_at - 1))

    loudness = one(*cuts[0])
    for cut in cuts[1:]:
        loudness = loudness * one(*cut)
    return loudness


def noise(rng, shape, spread, bound, split=(), kind=jnp.bfloat16):
    loudness = steps_of(rng, shape, split, -0.22, 0.18) if split else 1.0
    values = jax.random.normal(rng, shape, jnp.float32) * spread * loudness
    return jnp.minimum(jnp.maximum(values, -bound), bound).astype(kind)


def setup_inputs(seed: int = 0) -> dict:
    key_list = jax.random.split(jax.random.key(seed), 15)
    latent = noise(key_list[0], (TOKENS, D), 1.0, 6.0, ((0, 128),))
    context = noise(key_list[1], (CTX, D), 1.0, 6.0, ((0, 16),))
    conditioning = noise(key_list[2], (2, D), 1.0, 6.0, (), jnp.float32)
    norm_gain = jnp.clip(1.0 + 0.18 * jax.random.normal(key_list[3], (D,), jnp.float32), 0.1, 1.9)
    mod_shift = noise(key_list[4], (D, D), (D // 2) ** -0.5, 0.1875, ((0, 16), (1, 8)))
    mod_scale = noise(key_list[5], (D, D), (D // 2) ** -0.5, 0.1875, ((0, 16), (1, 8)))
    mod_gate = noise(key_list[6], (D, D), (D // 2) ** -0.5, 0.1875, ((0, 16), (1, 8)))
    w_query = draw_w_query(jax.random.fold_in(key_list[14], 71), 0)
    w_key = noise(key_list[8], (D, HEADS * 2 * HD), D ** -0.5, 0.125, ((1, 8),))
    w_value = noise(key_list[9], (D, HEADS * 2 * HD), D ** -0.5, 0.125, ((1, 8),))
    w_out = noise(key_list[10], (HEADS * 2 * HD, D), (HEADS * 2 * HD) ** -0.5, 0.125, ((0, 8),))
    lambdas = jnp.clip(0.3 + 0.5 * jax.random.uniform(key_list[11], (HEADS,), jnp.float32) ** steps_of(key_list[11], (HEADS,), ((0, 8),), -0.2, 0.2), 0.3, 0.8)
    context_bias = jnp.clip(0.8 + 1.40000004 * jax.random.uniform(key_list[12], (HEADS,), jnp.float32) ** steps_of(key_list[12], (HEADS,), ((0, 8),), -0.2, 0.2), 0.8, 2.2)
    head_gain = jnp.clip(1.0 + 0.18 * jax.random.normal(key_list[13], (2 * HD,), jnp.float32), 0.1, 1.9)
    return dict(latent=latent, context=context, conditioning=conditioning, norm_gain=norm_gain, mod_shift=mod_shift, mod_scale=mod_scale, mod_gate=mod_gate, w_query=w_query, w_key=w_key, w_value=w_value, w_out=w_out, lambdas=lambdas, context_bias=context_bias, head_gain=head_gain)


EPS = 1e-06

def modulated(inputs, norm_scale, offset_vec, scale_vec):
    rows_float = inputs.astype(jnp.float32)
    normal = rows_float * lax.rsqrt(lax.optimization_barrier(jnp.mean(rows_float * rows_float, axis=-1, keepdims=True)) + EPS)
    return (normal * norm_scale * (1.0 + scale_vec) + offset_vec).astype(jnp.bfloat16)

def reference(latent, context, conditioning, norm_gain, mod_shift, mod_scale, mod_gate, w_query, w_key, w_value, w_out, lambdas, context_bias, head_gain):
    activated = jax.nn.silu(conditioning).astype(jnp.bfloat16)
    shifts = jnp.dot(activated, mod_shift, preferred_element_type=jnp.float32)
    scales = jnp.dot(activated, mod_scale, preferred_element_type=jnp.float32)
    gates = jnp.dot(activated, mod_gate, preferred_element_type=jnp.float32)
    hidden = modulated(latent, norm_gain, shifts[0], scales[0])
    hidden_context = modulated(context, norm_gain, shifts[1], scales[1])
    latent_len = latent.shape[0]
    context_len = context.shape[0]
    keys_len = latent_len + context_len
    queries = jnp.dot(hidden, w_query, preferred_element_type=jnp.float32).astype(jnp.bfloat16).reshape(latent_len, HEADS, 2, HD)
    both_rows = jnp.concatenate([hidden_context, hidden], axis=0)
    keys = jnp.dot(both_rows, w_key, preferred_element_type=jnp.float32).astype(jnp.bfloat16).reshape(keys_len, HEADS, 2, HD)
    values = jnp.dot(both_rows, w_value, preferred_element_type=jnp.float32).astype(jnp.bfloat16).reshape(keys_len, HEADS, 2 * HD)
    context_flags = (jnp.arange(keys_len, dtype=jnp.int32) < context_len).astype(jnp.float32)
    block_len = math.gcd(latent_len, 512)

    def per_head(operands):
        query_head, key_head, value_head, lambda_head, bias_head = operands
        biases = bias_head * context_flags
        key_float = key_head.astype(jnp.float32)

        def per_block(query_block):
            query_float = query_block.astype(jnp.float32)
            per_map = []
            for which_map in range(2):
                scores = jnp.einsum('qd,kd->qk', query_float[:, which_map], key_float[:, which_map]) * HD ** (-0.5) + biases[None, :]
                peak = lax.optimization_barrier(jnp.max(scores, axis=1, keepdims=True))
                raised = jnp.exp(scores - peak)
                totals = lax.optimization_barrier(jnp.sum(raised, axis=1, keepdims=True))
                weighted = jnp.dot(raised.astype(jnp.bfloat16), value_head, preferred_element_type=jnp.float32)
                per_map.append(weighted / totals)
            return per_map[0] - lambda_head * per_map[1]
        blocks = query_head.reshape(latent_len // block_len, block_len, 2, HD)
        return lax.map(per_block, blocks).reshape(latent_len, 2 * HD)
    mixed = lax.map(per_head, (jnp.moveaxis(queries, 1, 0), jnp.moveaxis(keys, 1, 0), jnp.moveaxis(values, 1, 0), lambdas, context_bias))
    normed = mixed * lax.rsqrt(lax.optimization_barrier(jnp.mean(mixed * mixed, axis=-1, keepdims=True)) + EPS) * head_gain
    flattened = jnp.moveaxis(normed, 0, 1).reshape(latent_len, HEADS * 2 * HD).astype(jnp.bfloat16)
    group_cols = HEADS * 2 * HD // N_TP
    summed = jnp.zeros((latent_len, w_out.shape[1]), jnp.float32)
    for group_index in range(N_TP):
        lower = group_index * group_cols
        partial_value = jnp.dot(flattened[:, lower:lower + group_cols], w_out[lower:lower + group_cols], preferred_element_type=jnp.float32).astype(jnp.bfloat16)
        partial_value = lax.optimization_barrier(partial_value)
        summed = summed + partial_value.astype(jnp.float32)
    attended = summed.astype(jnp.bfloat16)
    return (latent.astype(jnp.float32) + gates[0] * attended.astype(jnp.float32)).astype(jnp.bfloat16)
```

```python
import functools
import math

import jax
import jax.numpy as jnp
from jax import lax
from jax.experimental import pallas as pl
from jax.experimental.pallas import tpu as pltpu
from jax.sharding import PartitionSpec as P

EPS = 1e-06
MESH = pl.DeviceIdType.MESH
BF = jnp.bfloat16
F32 = jnp.float32
LOG2E = math.log2(math.e)
SCALE = LOG2E / 8.0
ROWS = 96
PAIR = 192
OWN = 768
CTXR = 64
BLOCK = 2 * OWN + 2 * CTXR
QT = 512
NQ = 3
UNITS = 6
AHEAD = 2


def gray(n):
    return n + n // 2 - 2 * ((n // 2) * (n % 2))


def remote(src, dst, send, recv, sp, tp):
    return pltpu.make_async_remote_copy(
        src_ref=src, dst_ref=dst, send_sem=send, recv_sem=recv, device_id=(sp, tp), device_id_type=MESH
    )


def round_y(own, buf, rows, send, recv, s, y, c):
    up, down = ((y + 1) % 4) * 2 + c, ((y + 3) % 4) * 2 + c
    sib = y * 2 + 1 - c
    half = rows // 2

    def at(slot, offset, size):
        return buf.at[slot, pl.ds(pl.multiple_of(c * rows + offset, 16), size)]

    return [
        remote(own, at(0, 0, rows), send.at[0], recv.at[0], s, sib),
        remote(own, at(1, 0, rows), send.at[1], recv.at[1], s, up),
        remote(own, at(2, 0, rows), send.at[2], recv.at[2], s, down),
        remote(at(1, 0, half), at(3, 0, half), send.at[3], recv.at[3], s, up),
        remote(at(2, half, half), at(3, half, half), send.at[4], recv.at[4], s, down),
        remote(at(1, 0, rows), at(1, 0, rows), send.at[5], recv.at[5], s, sib),
        remote(at(2, 0, rows), at(2, 0, rows), send.at[6], recv.at[6], s, sib),
        remote(at(3, 0, rows), at(3, 0, rows), send.at[7], recv.at[7], s, sib),
    ]


def kernel(
    latent, context, cond, gain, mod_shift, mod_scale, mod_gate, w_query, w_key, w_value, w_out, lambdas,
    context_bias, head_gain, out,
    lat, part, msg, msg2, mods, qv, kvown, qown, kv, qb, qm, vctx, sscr, acc, peak, nsend, nrm, wall,
    lsend, lrecv, wsend, wrecv, msend, mrecv, nsd, nrc, zsend, zqsend, kvrecv, qrecv, fsib, fplus, fminus,
    osend, orecv, local,
):
    s, t = lax.axis_index("sp"), lax.axis_index("tp")
    z, x, y, c = s // 4, s % 4, t // 2, t % 2
    sib = y * 2 + 1 - c

    barrier = pltpu.get_barrier_semaphore()
    for d in range(1, 16):
        pl.semaphore_signal(barrier, inc=1, device_id=((s + d) % 16, t), device_id_type=MESH)
    for d in range(1, 8):
        pl.semaphore_signal(barrier, inc=1, device_id=(s, (t + d) % 8), device_id_type=MESH)
    pl.semaphore_wait(barrier, 22)

    lcp = round_y(latent, lat, ROWS, lsend, lrecv, s, y, c)
    for k in (1, 2, 0):
        lcp[k].start()
    lat[0, pl.ds(pl.multiple_of(c * ROWS, 16), ROWS), :] = latent[...]

    cols = cond[:, pl.ds(pl.multiple_of(s * 128, 128), 128)]
    activated = (cols / (1.0 + jnp.exp(-cols))).astype(BF)
    activated = jnp.concatenate([activated.astype(F32), jnp.zeros((6, 128), F32)], axis=0).astype(BF)
    for index, matrix in enumerate((mod_shift, mod_scale, mod_gate)):
        product = jnp.dot(activated, matrix[...], preferred_element_type=F32)
        for r in range(2):
            for half in range(2):
                row = index * 4 + r * 2 + half
                msg[row : row + 1, :] = product[r : r + 1, half * 128 : half * 128 + 128]
    msg[12:16, :] = jnp.zeros((4, 128), F32)
    mcp = []
    for d in range(1, 16):
        mcp.append(remote(msg, part.at[s], msend.at[d], mrecv.at[d], (s + d) % 16, t))
        mcp[-1].start()
    part[s] = msg[...]
    for copy in mcp:
        copy.wait_recv()
    total = part[0]
    for k in range(1, 16):
        total = total + part[k]
    msg2[...] = total
    msg2[12:13, 0:2] = lambdas[...]
    msg2[13:14, 0:2] = context_bias[...]
    ncp = []
    for d in range(1, 8):
        ncp.append(remote(msg2, mods.at[t], nsd.at[d], nrc.at[d], s, (t + d) % 8))
        ncp[-1].start()
    mods[t] = msg2[...]
    for copy in ncp:
        copy.wait_recv()

    def vector(index, r):
        row = index * 4 + r * 2
        return jnp.concatenate([mods[k, row + h : row + h + 1, :] for k in range(8) for h in range(2)], axis=1)

    def modulate(rows, r):
        rows = rows.astype(F32)
        normal = rows * lax.rsqrt(jnp.mean(rows * rows, axis=1, keepdims=True) + EPS)
        return (normal * gain[...] * (1.0 + vector(1, r)) + vector(0, r)).astype(BF)

    hidden = modulate(context[...], 1)
    keys = jnp.dot(hidden, w_key[...], preferred_element_type=F32).astype(BF)
    values = jnp.dot(hidden, w_value[...], preferred_element_type=F32).astype(BF)
    for i in range(2):
        kvown[i, 2 * OWN : 2 * OWN + CTXR, :] = keys[:, 128 * i : 128 * i + 128]
        kvown[i, 2 * OWN + CTXR : BLOCK, :] = values[:, 128 * i : 128 * i + 128]

    def project(p):
        hidden = modulate(lat[p], 0)
        rows = slice(PAIR * p, PAIR * p + PAIR)
        qv[0, rows, :] = jnp.dot(hidden, w_query[...], preferred_element_type=F32)
        keys = jnp.dot(hidden, w_key[...], preferred_element_type=F32).astype(BF)
        for i in range(2):
            kvown[i, rows, :] = keys[:, 128 * i : 128 * i + 128]
        qv[1, rows, :] = jnp.dot(hidden, w_value[...], preferred_element_type=F32)

    lcp[0].wait_recv()
    project(0)
    lcp[1].wait_recv()
    lcp[3].start()
    lcp[5].start()
    lcp[2].wait_recv()
    lcp[4].start()
    lcp[6].start()
    wcp = round_y(w_out, wall, 256, wsend, wrecv, s, y, c)
    for k in (1, 2, 0):
        wcp[k].start()
    wall[0, pl.ds(pl.multiple_of(c * 256, 256), 256), :] = w_out[...]
    lcp[5].wait_recv()
    project(1)
    lcp[6].wait_recv()
    project(2)
    lcp[3].wait_recv()
    lcp[4].wait_recv()
    lcp[7].start()
    lcp[7].wait_recv()
    project(3)
    for a in range(6):
        for i in range(2):
            rows, columns = slice(128 * a, 128 * a + 128), slice(128 * i, 128 * i + 128)
            kvown[i, OWN + 128 * a : OWN + 128 * a + 128, :] = qv[1, rows, columns].T.astype(BF)
            qown[a // 3, i, a % 3] = qv[0, rows, columns].T.astype(BF)

    for i in range(2):
        j = 2 * c + i
        dest = j * 4 + x

        def q_here():
            return pltpu.make_async_copy(qown.at[0, i], qb.at[z], qrecv.at[z])

        def kv_here():
            return pltpu.make_async_copy(kvown.at[i], kv.at[s], kvrecv.at[s])

        remote(qown.at[1, i], qb.at[z], zqsend.at[i, 1], qrecv.at[z], dest, sib).start()

        @pl.when(j == z)
        def _():
            q_here().start()
            kv_here().start()

        @pl.when(j != z)
        def _():
            remote(qown.at[0, i], qb.at[z], zqsend.at[i, 0], qrecv.at[z], dest, t).start()
            remote(kvown.at[i], kv.at[s], zsend.at[i], kvrecv.at[s], dest, t).start()

    primary = c == z // 2
    plus, minus = z * 4 + (x + 1) % 4, z * 4 + (x + 3) % 4

    def to_sib(b):
        return remote(kv.at[b], kv.at[b], fsib.at[b], kvrecv.at[b], s, sib)

    def to_plus(b):
        return remote(kv.at[b], kv.at[b], fplus.at[b], kvrecv.at[b], plus, t)

    def to_minus(b):
        return remote(kv.at[b], kv.at[b], fminus.at[b], kvrecv.at[b], minus, t)

    def place(n):
        dz, dx = gray(n % 4), gray(n // 4)
        return dz, dx, ((z + dz) % 4) * 4 + (x + dx) % 4

    def goes_plus(dz, dx):
        return (dx == 0) | ((dx == 3) & (dz < 2))

    def goes_minus(dz, dx):
        return (dx == 0) | ((dx == 1) & (dz >= 2))

    def take(n):
        dz, dx, b = place(n)
        pltpu.make_async_copy(kvown.at[0], kv.at[b], kvrecv.at[b]).wait()

        @pl.when(primary)
        def _():
            @pl.when(goes_plus(dz, dx))
            def _():
                to_plus(b).start()

            @pl.when(goes_minus(dz, dx))
            def _():
                to_minus(b).start()

            to_sib(b).start()

        return b

    for k in range(4):
        pltpu.make_async_copy(qown.at[0, 0], qb.at[k], qrecv.at[k]).wait()
    for tile in range(NQ):
        for r in range(4):
            chunk = 4 * tile + r
            columns = slice(128 * r, 128 * r + 128)
            block = qb[chunk // 3, chunk % 3]
            zero = jnp.zeros((64, 128), BF)
            qm[0, tile, 0:64, columns] = block[0:64]
            qm[0, tile, 64:128, columns] = zero
            qm[1, tile, 0:64, columns] = zero
            qm[1, tile, 64:128, columns] = block[64:128]
    for u in range(UNITS):
        acc[u] = jnp.zeros_like(acc[u])
        peak[u] = jnp.full_like(peak[u], -1e30)

    units = [(m, tile) for tile in range(NQ) for m in range(2)]

    def absorb(keys, lhs, size, bias):
        tops = {}

        def score(u):
            m, tile = units[u]
            raw = jnp.dot(keys, qm[m, tile], preferred_element_type=F32)
            sscr[u % (AHEAD + 1), 0:size, :] = raw
            tops[u] = jnp.max(raw, axis=0, keepdims=True) * SCALE

        for u in range(AHEAD):
            score(u)
        for u in range(UNITS):
            if u + AHEAD < UNITS:
                score(u + AHEAD)
            top = tops[u] if bias is None else tops[u] + bias
            old = peak[u]
            new = jnp.maximum(old, top)
            peak[u] = new
            faded = jnp.exp2(old - new)
            shift = new if bias is None else new - bias
            probs = jnp.exp2(sscr[u % (AHEAD + 1), 0:size, :] * SCALE - shift).astype(BF)
            acc[u] = acc[u] * faded + jnp.dot(lhs, probs, preferred_element_type=F32)

    def latent_step(n, carry):
        b = take(n)

        @pl.when(n == 4)
        def _():
            wcp[1].wait_recv()
            wcp[3].start()
            wcp[5].start()
            wcp[2].wait_recv()
            wcp[4].start()
            wcp[6].start()

        @pl.when(n == 12)
        def _():
            wcp[3].wait_recv()
            wcp[4].wait_recv()
            wcp[7].start()

        keys = kv[b, 0:OWN, :]
        lhs = jnp.concatenate([kv[b, OWN + 128 * a : OWN + 128 * a + 128, :] for a in range(6)], axis=1)
        lhs = jnp.concatenate([lhs, jnp.ones((16, OWN), BF)], axis=0)
        absorb(keys, lhs, OWN, None)
        return carry

    lax.fori_loop(0, 16, latent_step, 0)

    lane = lax.broadcasted_iota(jnp.int32, (1, 128), 1)
    owner = y * 2 + z // 2

    def pick(row):
        return jnp.sum(jnp.where(lane == z % 2, mods[owner, row : row + 1, :], 0.0), axis=1, keepdims=True)

    for k in range(8):
        pair = jnp.concatenate([kv[2 * k, 2 * OWN + CTXR : BLOCK, :], kv[2 * k + 1, 2 * OWN + CTXR : BLOCK, :]], axis=0)
        vctx[:, 128 * k : 128 * k + 128] = pair.astype(F32).T.astype(BF)
    keys = jnp.concatenate([kv[k, 2 * OWN : 2 * OWN + CTXR, :] for k in range(16)], axis=0)
    lhs = jnp.concatenate([vctx[...], jnp.ones((16, 16 * CTXR), BF)], axis=0)
    absorb(keys, lhs, 16 * CTXR, pick(13) * LOG2E)

    lam = pick(12)
    for tile in range(NQ):
        one, two = acc[2 * tile], acc[2 * tile + 1]
        mixed = one[0:128] / one[128:129] - lam * (two[0:128] / two[128:129])
        normed = mixed * lax.rsqrt(jnp.mean(mixed * mixed, axis=0, keepdims=True) + EPS)
        for r in range(4):
            block = normed[:, 128 * r : 128 * r + 128].T * head_gain[...]
            row = QT * tile + 128 * r
            nsend[row : row + 128, :] = block.astype(BF)

    head = y * 4 + z
    half = 1 - (c == z // 2).astype(jnp.int32)
    ocp = []
    for k in range(4):
        for e in range(4):
            offset = half if e // 2 == 0 else 3 * half + 3
            target = ((y + offset) % 4) * 2 + e % 2
            src = nsend.at[pl.ds(pl.multiple_of(384 * k + ROWS * e, 16), ROWS)]
            here = (k == z) & (target == t)
            ocp.append((src, k * 4 + x, target, here, 4 * k + e))
    for src, sp, tp, here, index in ocp:

        @pl.when(here)
        def _():
            pltpu.make_async_copy(src, nrm.at[head], orecv.at[head]).start()

        @pl.when(jnp.logical_not(here))
        def _():
            remote(src, nrm.at[head], osend.at[index], orecv.at[head], sp, tp).start()

    for k in (0, 5, 6, 7):
        wcp[k].wait_recv()
    for k in range(16):
        pltpu.make_async_copy(nsend.at[0:ROWS], nrm.at[k], orecv.at[k]).wait()

    attended = jnp.zeros((ROWS, 2048), F32)
    for p in range(4):
        group = ((y + (0, 3, 1, 2)[p]) % 4) * 2
        for k in range(2):
            rows = jnp.concatenate([nrm[2 * (group + k)], nrm[2 * (group + k) + 1]], axis=1)
            product = jnp.dot(rows, wall[p, 256 * k : 256 * k + 256, :], preferred_element_type=F32)
            attended = attended + product.astype(BF).astype(F32)
    gate = vector(2, 0)
    out[...] = (latent[...].astype(F32) + gate * attended.astype(BF).astype(F32)).astype(BF)

    for copy in lcp + wcp + mcp + ncp:
        copy.wait_send()
    for i in range(2):
        j = 2 * c + i
        remote(qown.at[1, i], qb.at[z], zqsend.at[i, 1], qrecv.at[z], j * 4 + x, sib).wait_send()

        @pl.when(j != z)
        def _():
            remote(qown.at[0, i], qb.at[z], zqsend.at[i, 0], qrecv.at[z], j * 4 + x, t).wait_send()
            remote(kvown.at[i], kv.at[s], zsend.at[i], kvrecv.at[s], j * 4 + x, t).wait_send()

    @pl.when(primary)
    def _():
        def sent(n, carry):
            dz, dx, b = place(n)

            @pl.when(goes_plus(dz, dx))
            def _():
                to_plus(b).wait_send()

            @pl.when(goes_minus(dz, dx))
            def _():
                to_minus(b).wait_send()

            to_sib(b).wait_send()
            return carry

        lax.fori_loop(0, 16, sent, 0)

    for src, sp, tp, here, index in ocp:

        @pl.when(jnp.logical_not(here))
        def _():
            remote(src, nrm.at[head], osend.at[index], orecv.at[head], sp, tp).wait_send()


def per_device(
    latent, context, conditioning, norm_gain, mod_shift, mod_scale, mod_gate, w_query, w_key, w_value, w_out,
    lambdas, context_bias, head_gain,
):
    dma = pltpu.SemaphoreType.DMA
    vmem = pl.BlockSpec(memory_space=pltpu.VMEM)
    return pl.pallas_call(
        kernel,
        name="block",
        out_shape=jax.ShapeDtypeStruct(latent.shape, BF),
        in_specs=[vmem] * 14,
        out_specs=vmem,
        scratch_shapes=[
            pltpu.VMEM((4, PAIR, 2048), BF),
            pltpu.VMEM((16, 16, 128), F32),
            pltpu.VMEM((16, 128), F32),
            pltpu.VMEM((16, 128), F32),
            pltpu.VMEM((8, 16, 128), F32),
            pltpu.VMEM((2, OWN, 256), F32),
            pltpu.VMEM((2, BLOCK, 128), BF),
            pltpu.VMEM((2, 2, 3, 128, 128), BF),
            pltpu.VMEM((16, BLOCK, 128), BF),
            pltpu.VMEM((4, 3, 128, 128), BF),
            pltpu.VMEM((2, NQ, 128, QT), BF),
            pltpu.VMEM((128, 16 * CTXR), BF),
            pltpu.VMEM((AHEAD + 1, 16 * CTXR, QT), F32),
            pltpu.VMEM((UNITS, 144, QT), F32),
            pltpu.VMEM((UNITS, 1, QT), F32),
            pltpu.VMEM((1536, 128), BF),
            pltpu.VMEM((16, ROWS, 128), BF),
            pltpu.VMEM((4, 512, 2048), BF),
            dma((8,)), dma((8,)), dma((8,)), dma((8,)),
            dma((16,)), dma((16,)), dma((8,)), dma((8,)),
            dma((2,)), dma((2, 2)), dma((16,)), dma((4,)),
            dma((16,)), dma((16,)), dma((16,)),
            dma((16,)), dma((16,)), dma((1,)),
        ],
        compiler_params=pltpu.CompilerParams(
            collective_id=0, has_side_effects=True, vmem_limit_bytes=60 * 2**20
        ),
    )(
        latent, context, conditioning, norm_gain.reshape(1, -1), mod_shift, mod_scale, mod_gate, w_query, w_key,
        w_value, w_out, lambdas.reshape(1, -1), context_bias.reshape(1, -1), head_gain.reshape(1, -1),
    )


def solution(mesh):
    return jax.shard_map(
        per_device,
        mesh=mesh,
        in_specs=(
            P(("sp", "tp"), None),
            P("sp", None),
            P(),
            P(),
            P("sp", "tp"),
            P("sp", "tp"),
            P("sp", "tp"),
            P(None, "tp"),
            P(None, "tp"),
            P(None, "tp"),
            P("tp", None),
            P("tp"),
            P("tp"),
            P(),
        ),
        out_specs=P(("sp", "tp"), None),
        check_vma=False,
    )
```

```python
import functools
import math

import jax
import jax.numpy as jnp
from jax import lax
from jax.experimental import pallas as pl
from jax.experimental.pallas import tpu as pltpu
from jax.sharding import PartitionSpec as P

EPS = 1e-06
MESH = pl.DeviceIdType.MESH
BF = jnp.bfloat16
F32 = jnp.float32
LOG2E = math.log2(math.e)
SCALE = LOG2E / 8.0
ROWS = 96
PAIR = 192
OWN = 768
CTXR = 64
BLOCK = 2 * OWN + 2 * CTXR
QT = 256
NQ = 6
UNITS = 12
AHEAD = 3
ORDER = (
    (0, 0), (1, 0), (3, 0), (0, 1), (0, 3), (1, 1), (1, 3), (3, 1), (2, 0), (3, 3), (0, 2), (2, 1), (1, 2), (3, 2),
    (2, 3), (2, 2),
)
PASS = {
    1: ((3, 0),), 2: ((0, 1), (0, 3)), 4: ((1, 1), (1, 3)), 5: ((2, 0),), 6: ((3, 1), (3, 3)), 8: ((0, 2),),
    9: ((2, 1),), 10: ((1, 2), (3, 2)), 12: ((2, 3), (2, 2)),
}


def remote(src, dst, send, recv, sp, tp):
    return pltpu.make_async_remote_copy(
        src_ref=src, dst_ref=dst, send_sem=send, recv_sem=recv, device_id=(sp, tp), device_id_type=MESH
    )


def round_y(buf, rows, send, recv, s, y, c):
    up, down = ((y + 1) % 4) * 2 + c, ((y + 3) % 4) * 2 + c
    sib = y * 2 + 1 - c
    half = rows // 2

    def at(slot, offset, size):
        return buf.at[slot, pl.ds(pl.multiple_of(c * rows + offset, 16), size)]

    def one(k, source, slot, offset, size, to):
        return remote(at(source, offset, size), at(slot, offset, size), send.at[k], recv.at[k], s, to)

    return [
        one(0, 0, 0, 0, rows, sib),
        one(1, 0, 1, 0, half, up),
        one(2, 0, 2, half, half, down),
        one(3, 0, 1, half, half, up),
        one(4, 0, 2, 0, half, down),
        one(5, 1, 3, 0, half, up),
        one(6, 2, 3, half, half, down),
        one(7, 1, 1, 0, rows, sib),
        one(8, 2, 2, 0, rows, sib),
        one(9, 3, 3, 0, rows, sib),
    ]


def kernel(
    latent, context, cond, gain, mod_shift, mod_scale, mod_gate, w_query, w_key, w_value, w_out, lambdas,
    context_bias, head_gain, out,
    lat, ctx, mod, wqkv, part, msg, msg2, mods, qv, kvown, qown, kv, qb, qm, vctx, sscr, tops, acc, peak, nsend, nrm,
    wall, lsend, lrecv, wsend, wrecv, msend, mrecv, nsd, nrc, zsend, zqsend, kvrecv, qrecv, fsib, fplus, fminus,
    osend, orecv, local,
):
    s, t = lax.axis_index("sp"), lax.axis_index("tp")
    z, x, y, c = s // 4, s % 4, t // 2, t % 2
    sib = y * 2 + 1 - c

    barrier = pltpu.get_barrier_semaphore()
    for d in range(1, 8):
        pl.semaphore_signal(barrier, inc=1, device_id=(s, (t + d) % 8), device_id_type=MESH)
    for d in range(1, 16):
        pl.semaphore_signal(barrier, inc=1, device_id=((s + d) % 16, t), device_id_type=MESH)
    loads = [
        pltpu.make_async_copy(src, dst, local.at[k])
        for k, (src, dst) in enumerate(
            (
                (mod_shift, mod.at[0]),
                (mod_scale, mod.at[1]),
                (mod_gate, mod.at[2]),
                (latent, lat.at[0, pl.ds(pl.multiple_of(c * ROWS, 16), ROWS)]),
                (context, ctx),
                (w_query, wqkv.at[0]),
                (w_key, wqkv.at[1]),
                (w_value, wqkv.at[2]),
                (w_out, wall.at[0, pl.ds(pl.multiple_of(c * 256, 256), 256)]),
            )
        )
    ]
    for copy in loads:
        copy.start()

    cols = cond[:, pl.ds(pl.multiple_of(s * 128, 128), 128)]
    activated = (cols / (1.0 + jnp.exp(-cols))).astype(BF)
    activated = jnp.concatenate([activated.astype(F32), jnp.zeros((6, 128), F32)], axis=0).astype(BF)
    msg[12:16, :] = jnp.zeros((4, 128), F32)
    for index in range(3):
        loads[index].wait()
        product = jnp.dot(activated, mod[index], preferred_element_type=F32)
        for r in range(2):
            for half in range(2):
                row = index * 4 + r * 2 + half
                msg[row : row + 1, :] = product[r : r + 1, half * 128 : half * 128 + 128]
    loads[3].wait()
    pl.semaphore_wait(barrier, 22)

    mcp = [remote(msg, part.at[s], msend.at[d], mrecv.at[d], (s + d) % 16, t) for d in range(1, 16)]
    for copy in mcp:
        copy.start()
    lcp = round_y(lat, ROWS, lsend, lrecv, s, y, c)
    for k in (1, 2, 0):
        lcp[k].start()
    part[s] = msg[...]
    for copy in mcp:
        copy.wait_recv()
    total = part[0]
    for k in range(1, 16):
        total = total + part[k]
    msg2[...] = total
    msg2[12:13, 0:2] = lambdas[...]
    msg2[13:14, 0:2] = context_bias[...]
    ncp = [remote(msg2, mods.at[t], nsd.at[d], nrc.at[d], s, (t + d) % 8) for d in range(1, 8)]
    for copy in ncp:
        copy.start()
    lcp[3].start()
    lcp[4].start()
    mods[t] = msg2[...]
    lcp[1].wait_recv()
    lcp[5].start()
    lcp[2].wait_recv()
    lcp[6].start()
    for copy in ncp:
        copy.wait_recv()

    def vector(index, r):
        row = index * 4 + r * 2
        return jnp.concatenate([mods[k, row + h : row + h + 1, :] for k in range(8) for h in range(2)], axis=1)

    def modulate(rows, r):
        rows = rows.astype(F32)
        normal = rows * lax.rsqrt(jnp.mean(rows * rows, axis=1, keepdims=True) + EPS)
        return (normal * (gain[...] * (1.0 + vector(1, r))) + vector(0, r)).astype(BF)

    def project(p):
        hidden = modulate(lat[p], 0)
        rows = slice(PAIR * p, PAIR * p + PAIR)
        qv[0, rows, :] = jnp.dot(hidden, wqkv[0], preferred_element_type=F32)
        keys = jnp.dot(hidden, wqkv[1], preferred_element_type=F32).astype(BF)
        for i in range(2):
            kvown[i, rows, :] = keys[:, 128 * i : 128 * i + 128]
        qv[1, rows, :] = jnp.dot(hidden, wqkv[2], preferred_element_type=F32)

    for copy in loads[4:]:
        copy.wait()
    hidden = modulate(ctx[...], 1)
    keys = jnp.dot(hidden, wqkv[1], preferred_element_type=F32).astype(BF)
    values = jnp.dot(hidden, wqkv[2], preferred_element_type=F32).astype(BF)
    for i in range(2):
        kvown[i, 2 * OWN : 2 * OWN + CTXR, :] = keys[:, 128 * i : 128 * i + 128]
        kvown[i, 2 * OWN + CTXR : BLOCK, :] = values[:, 128 * i : 128 * i + 128]
    lcp[0].wait_recv()
    project(0)
    lcp[3].wait_recv()
    lcp[7].start()
    lcp[4].wait_recv()
    lcp[8].start()
    wcp = round_y(wall, 256, wsend, wrecv, s, y, c)
    for k in (1, 2, 3, 4, 0):
        wcp[k].start()
    lcp[7].wait_recv()
    project(1)
    lcp[8].wait_recv()
    project(2)
    lcp[5].wait_recv()
    lcp[6].wait_recv()
    lcp[9].start()
    lcp[9].wait_recv()
    project(3)
    for a in range(6):
        for i in range(2):
            rows, columns = slice(128 * a, 128 * a + 128), slice(128 * i, 128 * i + 128)
            qown[a // 3, i, a % 3] = qv[0, rows, columns].T.astype(BF)
    for a in range(6):
        for i in range(2):
            rows, columns = slice(128 * a, 128 * a + 128), slice(128 * i, 128 * i + 128)
            kvown[i, OWN + 128 * a : OWN + 128 * a + 128, :] = qv[1, rows, columns].T.astype(BF)

    primary = c == z // 2
    plus, minus = z * 4 + (x + 1) % 4, z * 4 + (x + 3) % 4

    def q_sib(i):
        return remote(qown.at[1, i], qb.at[z], zqsend.at[i, 1], qrecv.at[z], (2 * c + i) * 4 + x, sib)

    def q_own(i):
        return remote(qown.at[0, i], qb.at[z], zqsend.at[i, 0], qrecv.at[z], (2 * c + i) * 4 + x, t)

    def kv_own(i):
        return remote(kvown.at[i], kv.at[s], zsend.at[i], kvrecv.at[s], (2 * c + i) * 4 + x, t)

    def distance(i):
        return (2 * c + i - z + 4) % 4

    for i in range(2):
        q_sib(i).start()

        @pl.when(distance(i) != 0)
        def _():
            q_own(i).start()

        @pl.when(distance(i) == 0)
        def _():
            pltpu.make_async_copy(qown.at[0, i], qb.at[z], qrecv.at[z]).start()
            pltpu.make_async_copy(kvown.at[i], kv.at[s], kvrecv.at[s]).start()

    def source(dz, dx):
        return ((z + dz) % 4) * 4 + (x + dx) % 4

    def onward(dz, dx):
        b = source(dz, dx)
        block = kvown.at[z % 2] if (dz, dx) == (0, 0) else kv.at[b]
        copies = []
        if dx == 0 or (dx == 3 and dz < 2):
            copies.append(remote(block, kv.at[b], fplus.at[b], kvrecv.at[b], plus, t))
        if dx == 0 or (dx == 1 and dz >= 2):
            copies.append(remote(block, kv.at[b], fminus.at[b], kvrecv.at[b], minus, t))
        copies.append(remote(block, kv.at[b], fsib.at[b], kvrecv.at[b], s, sib))
        return copies

    def arrive(b):
        pltpu.make_async_copy(kvown.at[0], kv.at[b], kvrecv.at[b]).wait()

    def pass_on(dz, dx):
        arrive(source(dz, dx))
        for copy in onward(dz, dx):
            copy.start()

    @pl.when(primary)
    def _():
        for copy in onward(0, 0):
            copy.start()

    for i in range(2):

        @pl.when(distance(i) % 2 == 1)
        def _():
            kv_own(i).start()

    for u in range(UNITS):
        acc[u] = jnp.zeros_like(acc[u])
        peak[u] = jnp.full_like(peak[u], -1e30)
    for k in range(4):
        pltpu.make_async_copy(qown.at[0, 0], qb.at[k], qrecv.at[k]).wait()
    for i in range(2):

        @pl.when(distance(i) == 2)
        def _():
            kv_own(i).start()

    for chunk in range(12):
        tile, columns = chunk // 2, slice(128 * (chunk % 2), 128 * (chunk % 2) + 128)
        block = qb[chunk // 3, chunk % 3]
        zero = jnp.zeros((64, 128), BF)
        qm[0, tile, 0:64, columns] = block[0:64]
        qm[0, tile, 64:128, columns] = zero
        qm[1, tile, 0:64, columns] = zero
        qm[1, tile, 64:128, columns] = block[64:128]

    def score(u, keys, size):
        raw = jnp.dot(keys, qm[u % 2, u // 2], preferred_element_type=F32)
        sscr[u % (AHEAD + 1), 0:size, :] = raw
        tops[u % (AHEAD + 1)] = jnp.max(raw, axis=0, keepdims=True) * SCALE

    def weigh(u, lhs, size, bias):
        slot = u % (AHEAD + 1)
        top = tops[slot] if bias is None else tops[slot] + bias
        old = peak[u]
        new = jnp.maximum(old, top)
        peak[u] = new
        faded = jnp.exp2(old - new)
        shift = new if bias is None else new - bias
        probs = jnp.exp2(sscr[slot, 0:size, :] * SCALE - shift).astype(BF)
        acc[u] = acc[u] * faded + jnp.dot(lhs, probs, preferred_element_type=F32)

    def latent_keys(b):
        return kv[b, 0:OWN, :]

    def latent_lhs(b):
        lhs = jnp.concatenate([kv[b, OWN + 128 * a : OWN + 128 * a + 128, :] for a in range(6)], axis=1)
        return jnp.concatenate([lhs, jnp.ones((16, OWN), BF)], axis=0)

    def block_at(n):
        return sum((n == k).astype(jnp.int32) * source(*place) for k, place in enumerate(ORDER))

    arrive(s)
    keys, lhs = latent_keys(s), latent_lhs(s)
    for u in range(AHEAD):
        score(u, keys, OWN)
    for u in range(UNITS):
        if u + AHEAD < UNITS:
            score(u + AHEAD, keys, OWN)
        weigh(u, lhs, OWN, None)


    @pl.when(primary)
    def _():
        pass_on(*ORDER[1])

    @pl.when(jnp.logical_not(primary))
    def _():
        arrive(source(*ORDER[1]))

    keys = latent_keys(source(*ORDER[1]))
    for u in range(AHEAD):
        score(u, keys, OWN)

    def step(n, carry):
        for k, blocks in PASS.items():

            @pl.when(primary & (n == k))
            def _():
                for place in blocks:
                    pass_on(*place)

        following = block_at(jnp.minimum(n + 1, 15))

        @pl.when(jnp.logical_not(primary) & (n < 15))
        def _():
            arrive(following)

        @pl.when(n == 5)
        def _():
            for k in (1, 2):
                wcp[k].wait_recv()
                wcp[k + 4].start()
            for k in (3, 4):
                wcp[k].wait_recv()
                wcp[k + 4].start()

        @pl.when(n == 12)
        def _():
            wcp[5].wait_recv()
            wcp[6].wait_recv()
            wcp[9].start()

        b = block_at(n)
        keys, later, lhs = latent_keys(b), latent_keys(following), latent_lhs(b)
        for u in range(UNITS):
            if u + AHEAD < UNITS:
                score(u + AHEAD, keys, OWN)
            else:
                score(u + AHEAD - UNITS, later, OWN)
            weigh(u, lhs, OWN, None)
        return carry

    lax.fori_loop(1, 16, step, 0)

    lane = lax.broadcasted_iota(jnp.int32, (1, 128), 1)
    owner = y * 2 + z // 2

    def pick(row):
        return jnp.sum(jnp.where(lane == z % 2, mods[owner, row : row + 1, :], 0.0), axis=1, keepdims=True)

    bias, lam = pick(13) * LOG2E, pick(12)
    head = y * 4 + z
    half = 1 - primary.astype(jnp.int32)
    ocp = []
    for k in range(4):
        for e in range(4):
            offset = half if e // 2 == 0 else 3 * half + 3
            target = ((y + offset) % 4) * 2 + e % 2
            src = nsend.at[pl.ds(pl.multiple_of(384 * k + ROWS * e, 16), ROWS)]
            here = (k == z) & (target == t)
            ocp.append((src, k * 4 + x, target, here, 4 * k + e))

    for k in range(8):
        pair = jnp.concatenate([kv[2 * k, 2 * OWN + CTXR : BLOCK, :], kv[2 * k + 1, 2 * OWN + CTXR : BLOCK, :]], axis=0)
        vctx[:, 128 * k : 128 * k + 128] = pair.astype(F32).T.astype(BF)
    keys = jnp.concatenate([kv[k, 2 * OWN : 2 * OWN + CTXR, :] for k in range(16)], axis=0)
    lhs = jnp.concatenate([vctx[...], jnp.ones((16, 16 * CTXR), BF)], axis=0)
    size = 16 * CTXR
    for u in range(AHEAD):
        score(u, keys, size)
    pieces = 0
    for tile in range(NQ):
        for u in (2 * tile, 2 * tile + 1):
            if u + AHEAD < UNITS:
                score(u + AHEAD, keys, size)
            weigh(u, lhs, size, bias)
        one, two = acc[2 * tile], acc[2 * tile + 1]
        mixed = one[0:128] / one[128:129] - lam * (two[0:128] / two[128:129])
        normed = mixed * lax.rsqrt(jnp.mean(mixed * mixed, axis=0, keepdims=True) + EPS)
        for r in range(QT // 128):
            block = normed[:, 128 * r : 128 * r + 128].T * head_gain[...]
            row = QT * tile + 128 * r
            nsend[row : row + 128, :] = block.astype(BF)
        ready = QT * (tile + 1) // ROWS
        for src, sp, tp, here, index in ocp[pieces:ready]:

            @pl.when(here)
            def _():
                pltpu.make_async_copy(src, nrm.at[head], orecv.at[head]).start()

            @pl.when(jnp.logical_not(here))
            def _():
                remote(src, nrm.at[head], osend.at[index], orecv.at[head], sp, tp).start()

        pieces = ready

    attended = jnp.zeros((ROWS, 2048), F32)
    for p in range(4):
        group = ((y + (0, 3, 1, 2)[p]) % 4) * 2
        for k in {0: (0,), 1: (7,), 2: (8,), 3: (9,)}[p]:
            wcp[k].wait_recv()
        for k in range(4):
            pltpu.make_async_copy(nsend.at[0:ROWS], nrm.at[2 * group + k], orecv.at[2 * group + k]).wait()
        for k in range(2):
            rows = jnp.concatenate([nrm[2 * (group + k)], nrm[2 * (group + k) + 1]], axis=1)
            product = jnp.dot(rows, wall[p, 256 * k : 256 * k + 256, :], preferred_element_type=F32)
            attended = attended + product.astype(BF).astype(F32)
    rows = lat[0, pl.ds(pl.multiple_of(c * ROWS, 16), ROWS), :].astype(F32)
    out[...] = (rows + vector(2, 0) * attended.astype(BF).astype(F32)).astype(BF)

    for copy in lcp + wcp + mcp + ncp:
        copy.wait_send()
    for i in range(2):
        q_sib(i).wait_send()

        @pl.when(distance(i) != 0)
        def _():
            q_own(i).wait_send()
            kv_own(i).wait_send()

    @pl.when(primary)
    def _():
        for place in ORDER:
            for copy in onward(*place):
                copy.wait_send()

    for src, sp, tp, here, index in ocp:

        @pl.when(jnp.logical_not(here))
        def _():
            remote(src, nrm.at[head], osend.at[index], orecv.at[head], sp, tp).wait_send()


def per_device(
    latent, context, conditioning, norm_gain, mod_shift, mod_scale, mod_gate, w_query, w_key, w_value, w_out,
    lambdas, context_bias, head_gain,
):
    dma = pltpu.SemaphoreType.DMA
    vmem = pl.BlockSpec(memory_space=pltpu.VMEM)
    hbm = pl.BlockSpec(memory_space=pl.ANY)
    return pl.pallas_call(
        kernel,
        name="block",
        out_shape=jax.ShapeDtypeStruct(latent.shape, BF),
        in_specs=[hbm, hbm, vmem, vmem] + [hbm] * 7 + [vmem] * 3,
        out_specs=vmem,
        scratch_shapes=[
            pltpu.VMEM((4, PAIR, 2048), BF),
            pltpu.VMEM((CTXR, 2048), BF),
            pltpu.VMEM((3, 128, 256), BF),
            pltpu.VMEM((3, 2048, 256), BF),
            pltpu.VMEM((16, 16, 128), F32),
            pltpu.VMEM((16, 128), F32),
            pltpu.VMEM((16, 128), F32),
            pltpu.VMEM((8, 16, 128), F32),
            pltpu.VMEM((2, OWN, 256), F32),
            pltpu.VMEM((2, BLOCK, 128), BF),
            pltpu.VMEM((2, 2, 3, 128, 128), BF),
            pltpu.VMEM((16, BLOCK, 128), BF),
            pltpu.VMEM((4, 3, 128, 128), BF),
            pltpu.VMEM((2, NQ, 128, QT), BF),
            pltpu.VMEM((128, 16 * CTXR), BF),
            pltpu.VMEM((AHEAD + 1, 16 * CTXR, QT), F32),
            pltpu.VMEM((AHEAD + 1, 1, QT), F32),
            pltpu.VMEM((UNITS, 144, QT), F32),
            pltpu.VMEM((UNITS, 1, QT), F32),
            pltpu.VMEM((1536, 128), BF),
            pltpu.VMEM((16, ROWS, 128), BF),
            pltpu.VMEM((4, 512, 2048), BF),
            dma((10,)), dma((10,)), dma((10,)), dma((10,)),
            dma((16,)), dma((16,)), dma((8,)), dma((8,)),
            dma((2,)), dma((2, 2)), dma((16,)), dma((4,)),
            dma((16,)), dma((16,)), dma((16,)),
            dma((16,)), dma((16,)), dma((9,)),
        ],
        compiler_params=pltpu.CompilerParams(
            collective_id=0, has_side_effects=True, vmem_limit_bytes=60 * 2**20
        ),
    )(
        latent, context, conditioning, norm_gain.reshape(1, -1), mod_shift, mod_scale, mod_gate, w_query, w_key,
        w_value, w_out, lambdas.reshape(1, -1), context_bias.reshape(1, -1), head_gain.reshape(1, -1),
    )


def solution(mesh):
    return jax.shard_map(
        per_device,
        mesh=mesh,
        in_specs=(
            P(("sp", "tp"), None),
            P("sp", None),
            P(),
            P(),
            P("sp", "tp"),
            P("sp", "tp"),
            P("sp", "tp"),
            P(None, "tp"),
            P(None, "tp"),
            P(None, "tp"),
            P("tp", None),
            P("tp"),
            P("tp"),
            P(),
        ),
        out_specs=P(("sp", "tp"), None),
        check_vma=False,
    )
```

```python
import functools
import math

import jax
import jax.numpy as jnp
from jax import lax
from jax.experimental import pallas as pl
from jax.experimental.pallas import tpu as pltpu
from jax.sharding import PartitionSpec as P

EPS = 1e-06
MESH = pl.DeviceIdType.MESH
BF = jnp.bfloat16
F32 = jnp.float32
LOG2E = math.log2(math.e)
SCALE = LOG2E / 8.0
ROWS = 96
PAIR = 192
OWN = 768
CTXR = 64
BLOCK = 2 * OWN + 2 * CTXR
QT = 256
NQ = 6
UNITS = 12
AHEAD = 3
ORDER = (
    (0, 0), (0, 1), (0, 3), (1, 0), (3, 0), (1, 1), (1, 3), (3, 1), (3, 3), (2, 0), (0, 2), (1, 2), (3, 2), (2, 1),
    (2, 3), (2, 2),
)
PACKED = tuple(sum(place[k] << 2 * (n % 8) for n, place in enumerate(ORDER[8 * h : 8 * h + 8])) for k in range(2) for h in range(2))
PASS = {
    0: ((0, 1, 0), (0, 1, 1), (0, 3, 0), (1, 0, 0), (3, 0, 0)), 1: ((0, 3, 1),), 2: ((1, 0, 1), (3, 0, 1)),
    4: ((1, 1, 0), (1, 1, 1), (1, 3, 0), (1, 3, 1)), 6: ((3, 1, 0), (3, 1, 1), (3, 3, 0), (3, 3, 1)),
    7: ((2, 0, 0), (2, 0, 1)), 8: ((0, 2, 0), (0, 2, 1)),
    10: ((1, 2, 0), (1, 2, 1), (3, 2, 0), (3, 2, 1), (2, 1, 0), (2, 1, 1)), 11: ((2, 3, 0), (2, 3, 1)),
    13: ((2, 2, 0), (2, 2, 1)),
}
HALF = OWN // 2
PARTS = ((0, OWN), (OWN, BLOCK - OWN))


def remote(src, dst, send, recv, sp, tp):
    return pltpu.make_async_remote_copy(
        src_ref=src, dst_ref=dst, send_sem=send, recv_sem=recv, device_id=(sp, tp), device_id_type=MESH
    )


def round_y(buf, rows, send, recv, s, y, c):
    up, down = ((y + 1) % 4) * 2 + c, ((y + 3) % 4) * 2 + c
    sib = y * 2 + 1 - c
    half = rows // 2

    def at(slot, offset, size):
        return buf.at[slot, pl.ds(pl.multiple_of(c * rows + offset, 16), size)]

    def one(k, source, slot, offset, size, to):
        return remote(at(source, offset, size), at(slot, offset, size), send.at[k], recv.at[k], s, to)

    return [
        one(0, 0, 0, 0, rows, sib),
        one(1, 0, 1, 0, half, up),
        one(2, 0, 2, half, half, down),
        one(3, 0, 1, half, half, up),
        one(4, 0, 2, 0, half, down),
        one(5, 1, 3, 0, half, up),
        one(6, 2, 3, half, half, down),
        one(7, 1, 1, 0, rows, sib),
        one(8, 2, 2, 0, rows, sib),
        one(9, 3, 3, 0, rows, sib),
    ]


def kernel(
    latent, context, cond, gain, mod_shift, mod_scale, mod_gate, w_query, w_key, w_value, w_out, lambdas,
    context_bias, head_gain, out,
    lat, ctx, mod, wqkv, part, msg, row, msg2, mods, qv, kvown, qown, kv, qb, qm, vctx, sscr, tops, acc, peak, nsend, nrm,
    wall, lsend, lrecv, wsend, wrecv, msend, mrecv, nsd, nrc, zsend, zqsend, kvrecv, qrecv, fsib, fplus, fminus,
    osend, orecv, local,
):
    s, t = lax.axis_index("sp"), lax.axis_index("tp")
    z, x, y, c = s // 4, s % 4, t // 2, t % 2
    sib = y * 2 + 1 - c

    barrier = pltpu.get_barrier_semaphore()
    for d in range(1, 8):
        pl.semaphore_signal(barrier, inc=1, device_id=(s, (t + d) % 8), device_id_type=MESH)
    for d in range(1, 4):
        pl.semaphore_signal(barrier, inc=1, device_id=(z * 4 + (x + d) % 4, t), device_id_type=MESH)
        pl.semaphore_signal(barrier, inc=1, device_id=((z + d) % 4 * 4 + x, t), device_id_type=MESH)
    loads = [
        pltpu.make_async_copy(src, dst, local.at[k])
        for k, (src, dst) in enumerate(
            (
                (mod_shift, mod.at[0]),
                (mod_scale, mod.at[1]),
                (mod_gate, mod.at[2]),
                (latent, lat.at[0, pl.ds(pl.multiple_of(c * ROWS, 16), ROWS)]),
                (context, ctx),
                (w_query, wqkv.at[0]),
                (w_key, wqkv.at[1]),
                (w_value, wqkv.at[2]),
                (w_out, wall.at[0, pl.ds(pl.multiple_of(c * 256, 256), 256)]),
            )
        )
    ]
    for copy in loads:
        copy.start()

    cols = cond[:, pl.ds(pl.multiple_of(s * 128, 128), 128)]
    activated = (cols / (1.0 + jnp.exp(-cols))).astype(BF)
    activated = jnp.concatenate([activated.astype(F32), jnp.zeros((6, 128), F32)], axis=0).astype(BF)
    msg[12:16, :] = jnp.zeros((4, 128), F32)
    for index in range(3):
        loads[index].wait()
        product = jnp.dot(activated, mod[index], preferred_element_type=F32)
        for r in range(2):
            for half in range(2):
                line = index * 4 + r * 2 + half
                msg[line : line + 1, :] = product[r : r + 1, half * 128 : half * 128 + 128]
    loads[3].wait()
    pl.semaphore_wait(barrier, 13)

    mcp = [
        remote(msg, part.at[0, x], msend.at[0, d], mrecv.at[0, d], z * 4 + (x + d) % 4, t) for d in range(1, 4)
    ]
    for copy in mcp:
        copy.start()
    lcp = round_y(lat, ROWS, lsend, lrecv, s, y, c)
    for k in (1, 2, 3, 4, 0):
        lcp[k].start()
    part[0, x] = msg[...]
    for copy in mcp:
        copy.wait_recv()
    row[...] = part[0, 0] + part[0, 1] + part[0, 2] + part[0, 3]
    zcp = [
        remote(row, part.at[1, z], msend.at[1, d], mrecv.at[1, d], (z + d) % 4 * 4 + x, t) for d in range(1, 4)
    ]
    for copy in zcp:
        copy.start()
    part[1, z] = row[...]
    for copy in zcp:
        copy.wait_recv()
    msg2[...] = part[1, 0] + part[1, 1] + part[1, 2] + part[1, 3]
    msg2[12:13, 0:2] = lambdas[...]
    msg2[13:14, 0:2] = context_bias[...]
    ncp = [remote(msg2, mods.at[t], nsd.at[d], nrc.at[d], s, (t + d) % 8) for d in range(1, 8)]
    for copy in ncp:
        copy.start()
    mods[t] = msg2[...]
    lcp[1].wait_recv()
    lcp[5].start()
    lcp[2].wait_recv()
    lcp[6].start()
    lcp[3].wait_recv()
    lcp[7].start()
    lcp[4].wait_recv()
    lcp[8].start()
    for copy in ncp:
        copy.wait_recv()

    def vector(index, r):
        row = index * 4 + r * 2
        return jnp.concatenate([mods[k, row + h : row + h + 1, :] for k in range(8) for h in range(2)], axis=1)

    def modulate(rows, r):
        rows = rows.astype(F32)
        normal = rows * lax.rsqrt(jnp.mean(rows * rows, axis=1, keepdims=True) + EPS)
        return (normal * (gain[...] * (1.0 + vector(1, r))) + vector(0, r)).astype(BF)

    def project(p):
        hidden = modulate(lat[p], 0)
        rows = slice(PAIR * p, PAIR * p + PAIR)
        first = PAIR * p + HALF * (p // 2)
        qv[0, rows, :] = jnp.dot(hidden, wqkv[0], preferred_element_type=F32)
        keys = jnp.dot(hidden, wqkv[1], preferred_element_type=F32).astype(BF)
        for i in range(2):
            kvown[i, first : first + PAIR, :] = keys[:, 128 * i : 128 * i + 128]
        qv[1, rows, :] = jnp.dot(hidden, wqkv[2], preferred_element_type=F32)

    for copy in loads[4:]:
        copy.wait()
    hidden = modulate(ctx[...], 1)
    keys = jnp.dot(hidden, wqkv[1], preferred_element_type=F32).astype(BF)
    values = jnp.dot(hidden, wqkv[2], preferred_element_type=F32).astype(BF)
    for i in range(2):
        kvown[i, 2 * OWN : 2 * OWN + CTXR, :] = keys[:, 128 * i : 128 * i + 128]
        kvown[i, 2 * OWN + CTXR : BLOCK, :] = values[:, 128 * i : 128 * i + 128]
    lcp[0].wait_recv()
    project(0)
    lcp[7].wait_recv()
    project(1)

    primary = c == z // 2
    plus, minus = z * 4 + (x + 1) % 4, z * 4 + (x + 3) % 4

    def turn(part):
        for a in range(3 * part, 3 * part + 3):
            for i in range(2):
                rows, columns = slice(128 * a, 128 * a + 128), slice(128 * i, 128 * i + 128)
                qown[part, i, a % 3] = qv[0, rows, columns].T.astype(BF)
                first = OWN * part + HALF + 128 * (a % 3)
                kvown[i, first : first + 128, :] = qv[1, rows, columns].T.astype(BF)

    def distance(i):
        return (2 * c + i - z + 4) % 4

    def slot_of(dz):
        return 3 * (dz == 0).astype(jnp.int32) + (dz == 1).astype(jnp.int32) + 2 * (dz == 3).astype(jnp.int32)

    def q_to(i, part):
        slot = slot_of((z - 2 * c - i + 4) % 4)
        return remote(
            qown.at[part, i], qb.at[slot], zqsend.at[i, part], qrecv.at[slot], (2 * c + i) * 4 + x, sib if part else t
        )

    def part_of(ref, b, part):
        return ref.at[b, pl.ds(*PARTS[part])]

    def kv_to(i, part):
        return remote(
            part_of(kvown, i, part), part_of(kv, s, part), zsend.at[i, part], kvrecv.at[part, s],
            (2 * c + i) * 4 + x, t,
        )

    def source(dz, dx):
        return ((z + dz) % 4) * 4 + (x + dx) % 4

    def onward(dz, dx, part):
        b = source(dz, dx)
        src = part_of(kvown, z % 2, part) if (dz, dx) == (0, 0) else part_of(kv, b, part)
        dst = part_of(kv, b, part)
        copies = []
        if dx == 0 or (dx == 3 and dz < 2):
            copies.append(remote(src, dst, fplus.at[part, b], kvrecv.at[part, b], plus, t))
        if dx == 0 or (dx == 1 and dz >= 2):
            copies.append(remote(src, dst, fminus.at[part, b], kvrecv.at[part, b], minus, t))
        copies.append(remote(src, dst, fsib.at[part, b], kvrecv.at[part, b], s, sib))
        return copies

    def arrive(b, part):
        pltpu.make_async_copy(part_of(kvown, 0, part), part_of(kv, b, part), kvrecv.at[part, b]).wait()

    def pass_on(dz, dx, part):
        arrive(source(dz, dx), part)
        for copy in onward(dz, dx, part):
            copy.start()

    def send_part(part):
        for i in range(2):
            if part:
                q_to(i, 1).start()

            @pl.when(distance(i) != 0)
            def _():
                if not part:
                    q_to(i, 0).start()

            @pl.when(distance(i) == 0)
            def _():
                if not part:
                    pltpu.make_async_copy(qown.at[0, i], qb.at[3], qrecv.at[3]).start()
                pltpu.make_async_copy(part_of(kvown, i, part), part_of(kv, s, part), kvrecv.at[part, s]).start()

        @pl.when(primary)
        def _():
            for copy in onward(0, 0, part):
                copy.start()

        for i in range(2):

            @pl.when(distance(i) % 2 == 1)
            def _():
                kv_to(i, part).start()

    def send_far(part):
        for i in range(2):

            @pl.when(distance(i) == 2)
            def _():
                kv_to(i, part).start()

    turn(0)
    send_part(0)
    lcp[5].wait_recv()
    lcp[6].wait_recv()
    lcp[9].start()
    lcp[8].wait_recv()
    project(2)
    lcp[9].wait_recv()
    project(3)
    turn(1)
    send_part(1)
    wcp = round_y(wall, 256, wsend, wrecv, s, y, c)
    for k in (1, 2, 3, 4, 0):
        wcp[k].start()

    for u in range(UNITS):
        acc[u] = jnp.zeros_like(acc[u])
        peak[u] = jnp.full_like(peak[u], -1e30)
    for k in range(4):
        pltpu.make_async_copy(qown.at[0, 0], qb.at[k], qrecv.at[k]).wait()

    for chunk in range(12):
        tile, columns = chunk // 2, slice(128 * (chunk % 2), 128 * (chunk % 2) + 128)
        block = qb[chunk // 3, chunk % 3]
        zero = jnp.zeros((64, 128), BF)
        qm[0, tile, 0:64, columns] = block[0:64]
        qm[0, tile, 64:128, columns] = zero
        qm[1, tile, 0:64, columns] = zero
        qm[1, tile, 64:128, columns] = block[64:128]

    def score(u, at, keys, size):
        raw = jnp.dot(keys, qm[u % 2, u // 2], preferred_element_type=F32)
        sscr[at % (AHEAD + 1), 0:size, :] = raw
        tops[at % (AHEAD + 1)] = jnp.max(raw, axis=0, keepdims=True) * SCALE

    def weigh(u, at, lhs, size, bias):
        slot = at % (AHEAD + 1)
        top = tops[slot] if bias is None else tops[slot] + bias
        old = peak[u]
        new = jnp.maximum(old, top)
        peak[u] = new
        faded = jnp.exp2(old - new)
        shift = new if bias is None else new - bias
        probs = jnp.exp2(sscr[slot, 0:size, :] * SCALE - shift).astype(BF)
        acc[u] = acc[u] * faded + jnp.dot(lhs, probs, preferred_element_type=F32)

    def latent_keys(b):
        return jnp.concatenate([kv[b, 0:HALF, :], kv[b, OWN : OWN + HALF, :]], axis=0)

    def latent_lhs(b):
        lhs = jnp.concatenate([kv[b, k : k + 128, :] for a in (HALF, OWN + HALF) for k in range(a, a + HALF, 128)], axis=1)
        return jnp.concatenate([lhs, jnp.ones((16, OWN), BF)], axis=0)

    def block_at(n):
        late = (n >= 8).astype(jnp.int32)
        by = 2 * (n - 8 * late)
        dz = ((PACKED[0] * (1 - late) + PACKED[1] * late) >> by) % 4
        dx = ((PACKED[2] * (1 - late) + PACKED[3] * late) >> by) % 4
        return source(dz, dx)

    arrive(s, 0)
    arrive(s, 1)
    keys, lhs = latent_keys(s), latent_lhs(s)
    for u in range(AHEAD):
        score(u, u, keys, OWN)
    for u in range(UNITS):
        if u + AHEAD < UNITS:
            score(u + AHEAD, u + AHEAD, keys, OWN)
        weigh(u, u, lhs, OWN, None)


    @pl.when(primary)
    def _():
        for place in PASS[0]:
            pass_on(*place)

    @pl.when(jnp.logical_not(primary))
    def _():
        arrive(source(0, 1), 0)
        arrive(source(0, 1), 1)

    keys = latent_keys(source(0, 1))
    for u in range(AHEAD):
        score(u, u, keys, OWN)

    def step(n, b):
        following = block_at(n + 1)

        @pl.when(primary)
        def _():
            for steps in ((1, 2, 4), (6, 7, 8), (10, 11, 13)):

                @pl.when((n >= steps[0]) & (n <= steps[-1]))
                def _():
                    for k in steps:

                        @pl.when(n == k)
                        def _():
                            for place in PASS[k]:
                                pass_on(*place)

        @pl.when(jnp.logical_not(primary))
        def _():
            arrive(following, 0)
            arrive(following, 1)

        @pl.when(n == 2)
        def _():
            send_far(0)
            send_far(1)

        @pl.when(n == 7)
        def _():
            for k in (1, 2):
                wcp[k].wait_recv()
                wcp[k + 4].start()
            for k in (3, 4):
                wcp[k].wait_recv()
                wcp[k + 4].start()

        @pl.when(n == 13)
        def _():
            wcp[5].wait_recv()
            wcp[6].wait_recv()
            wcp[9].start()

        keys, later, lhs = latent_keys(b), latent_keys(following), latent_lhs(b)
        for u in range(UNITS):
            if u + AHEAD < UNITS:
                score(u + AHEAD, u + AHEAD, keys, OWN)
            else:
                score(u + AHEAD - UNITS, u + AHEAD, later, OWN)
            weigh(u, u, lhs, OWN, None)
        return following

    last = lax.fori_loop(1, 15, step, source(0, 1))

    lane = lax.broadcasted_iota(jnp.int32, (1, 128), 1)
    owner = y * 2 + z // 2

    def pick(row):
        return jnp.sum(jnp.where(lane == z % 2, mods[owner, row : row + 1, :], 0.0), axis=1, keepdims=True)

    bias, lam = pick(13) * LOG2E, pick(12)
    head = y * 4 + z
    half = 1 - primary.astype(jnp.int32)

    def piece(k):
        offset = half if k % 4 // 2 == 0 else 3 * half + 3
        target = ((y + offset) % 4) * 2 + k % 2
        src = nsend.at[ROWS * k : ROWS * k + ROWS]
        return remote(src, nrm.at[head], osend.at[k], orecv.at[head], ((z + (2, 1, 3, 0)[k // 4]) % 4) * 4 + x, target)

    for k in range(8):
        pair = jnp.concatenate([kv[2 * k, 2 * OWN + CTXR : BLOCK, :], kv[2 * k + 1, 2 * OWN + CTXR : BLOCK, :]], axis=0)
        vctx[:, 128 * k : 128 * k + 128] = pair.astype(F32).T.astype(BF)
    size = 16 * CTXR
    keys = (latent_keys(last), jnp.concatenate([kv[k, 2 * OWN : 2 * OWN + CTXR, :] for k in range(16)], axis=0))
    lhs = (latent_lhs(last), jnp.concatenate([vctx[...], jnp.ones((16, size), BF)], axis=0))
    sizes, biases = (OWN, size), (None, bias)
    turns = [(0, u) for u in range(4)]
    for u in range(0, UNITS, 2):
        turns += [(1, u), (1, u + 1)]
        turns += [(0, u + 4), (0, u + 5)] if u + 5 < UNITS else []
    pieces = 0
    for k, (which, u) in enumerate(turns):
        if k + AHEAD < len(turns):
            other, v = turns[k + AHEAD]
            score(v, k + AHEAD, keys[other], sizes[other])
        weigh(u, k, lhs[which], sizes[which], biases[which])
        if which == 0 or u % 2 == 0:
            continue
        tile = u // 2
        one, two = acc[2 * tile], acc[2 * tile + 1]
        mixed = one[0:128] / one[128:129] - lam * (two[0:128] / two[128:129])
        normed = mixed * lax.rsqrt(jnp.mean(mixed * mixed, axis=0, keepdims=True) + EPS)
        for r in range(QT // 128):
            block = normed[:, 128 * r : 128 * r + 128].T * head_gain[...]
            row = QT * tile + 128 * r
            nsend[row : row + 128, :] = block.astype(BF)
        if tile % 2 == 0:
            continue
        ready = QT * (tile + 1) // ROWS
        for e in range(pieces, ready):
            if e not in (12, 13):
                piece(e).start()
                continue
            mine = primary & (c == e - 12)

            @pl.when(mine)
            def _():
                src = nsend.at[ROWS * e : ROWS * e + ROWS]
                pltpu.make_async_copy(src, nrm.at[head], orecv.at[head]).start()

            @pl.when(jnp.logical_not(mine))
            def _():
                piece(e).start()

        pieces = ready

    for k in (0, 7, 8, 9):
        wcp[k].wait_recv()
    attended = jnp.zeros((ROWS, 2048), F32)
    for k in (1 - z // 2, z // 2):
        for p in range(4):
            first = 4 * ((y + (0, 3, 1, 2)[p]) % 4) + 2 * k
            for h in (first, first + 1):
                pltpu.make_async_copy(nsend.at[0:ROWS], nrm.at[h], orecv.at[h]).wait()
            rows = jnp.concatenate([nrm[first], nrm[first + 1]], axis=1)
            part_of_w = wall[p, pl.ds(pl.multiple_of(256 * k, 256), 256), :]
            product = jnp.dot(rows, part_of_w, preferred_element_type=F32)
            attended = attended + product.astype(BF).astype(F32)
    rows = lat[0, pl.ds(pl.multiple_of(c * ROWS, 16), ROWS), :].astype(F32)
    out[...] = (rows + vector(2, 0) * attended.astype(BF).astype(F32)).astype(BF)

    for copy in lcp + wcp + mcp + zcp + ncp:
        copy.wait_send()
    for i in range(2):
        q_to(i, 1).wait_send()

        @pl.when(distance(i) != 0)
        def _():
            q_to(i, 0).wait_send()
            for part in range(2):
                kv_to(i, part).wait_send()

    @pl.when(primary)
    def _():
        for place in ORDER:
            for part in range(2):
                for copy in onward(*place, part):
                    copy.wait_send()

    for e in range(16):
        if e not in (12, 13):
            piece(e).wait_send()
            continue

        @pl.when(jnp.logical_not(primary & (c == e - 12)))
        def _():
            piece(e).wait_send()


def per_device(
    latent, context, conditioning, norm_gain, mod_shift, mod_scale, mod_gate, w_query, w_key, w_value, w_out,
    lambdas, context_bias, head_gain,
):
    dma = pltpu.SemaphoreType.DMA
    vmem = pl.BlockSpec(memory_space=pltpu.VMEM)
    hbm = pl.BlockSpec(memory_space=pl.ANY)
    return pl.pallas_call(
        kernel,
        name="block",
        out_shape=jax.ShapeDtypeStruct(latent.shape, BF),
        in_specs=[hbm, hbm, vmem, vmem] + [hbm] * 7 + [vmem] * 3,
        out_specs=vmem,
        scratch_shapes=[
            pltpu.VMEM((4, PAIR, 2048), BF),
            pltpu.VMEM((CTXR, 2048), BF),
            pltpu.VMEM((3, 128, 256), BF),
            pltpu.VMEM((3, 2048, 256), BF),
            pltpu.VMEM((2, 4, 16, 128), F32),
            pltpu.VMEM((16, 128), F32),
            pltpu.VMEM((16, 128), F32),
            pltpu.VMEM((16, 128), F32),
            pltpu.VMEM((8, 16, 128), F32),
            pltpu.VMEM((2, OWN, 256), F32),
            pltpu.VMEM((2, BLOCK, 128), BF),
            pltpu.VMEM((2, 2, 3, 128, 128), BF),
            pltpu.VMEM((16, BLOCK, 128), BF),
            pltpu.VMEM((4, 3, 128, 128), BF),
            pltpu.VMEM((2, NQ, 128, QT), BF),
            pltpu.VMEM((128, 16 * CTXR), BF),
            pltpu.VMEM((AHEAD + 1, 16 * CTXR, QT), F32),
            pltpu.VMEM((AHEAD + 1, 1, QT), F32),
            pltpu.VMEM((UNITS, 144, QT), F32),
            pltpu.VMEM((UNITS, 1, QT), F32),
            pltpu.VMEM((1536, 128), BF),
            pltpu.VMEM((16, ROWS, 128), BF),
            pltpu.VMEM((4, 512, 2048), BF),
            dma((10,)), dma((10,)), dma((10,)), dma((10,)),
            dma((2, 4)), dma((2, 4)), dma((8,)), dma((8,)),
            dma((2, 2)), dma((2, 2)), dma((2, 16)), dma((4,)),
            dma((2, 16)), dma((2, 16)), dma((2, 16)),
            dma((16,)), dma((16,)), dma((9,)),
        ],
        compiler_params=pltpu.CompilerParams(
            collective_id=0, has_side_effects=True, vmem_limit_bytes=60 * 2**20
        ),
    )(
        latent, context, conditioning, norm_gain.reshape(1, -1), mod_shift, mod_scale, mod_gate, w_query, w_key,
        w_value, w_out, lambdas.reshape(1, -1), context_bias.reshape(1, -1), head_gain.reshape(1, -1),
    )


def solution(mesh):
    return jax.shard_map(
        per_device,
        mesh=mesh,
        in_specs=(
            P(("sp", "tp"), None),
            P("sp", None),
            P(),
            P(),
            P("sp", "tp"),
            P("sp", "tp"),
            P("sp", "tp"),
            P(None, "tp"),
            P(None, "tp"),
            P(None, "tp"),
            P("tp", None),
            P("tp"),
            P("tp"),
            P(),
        ),
        out_specs=P(("sp", "tp"), None),
        check_vma=False,
    )
```

```python
import functools
import math

import jax
import jax.numpy as jnp
from jax import lax
from jax.experimental import pallas as pl
from jax.experimental.pallas import tpu as pltpu
from jax.sharding import PartitionSpec as P

EPS = 1e-06
MESH = pl.DeviceIdType.MESH
BF = jnp.bfloat16
F32 = jnp.float32
LOG2E = math.log2(math.e)
SCALE = LOG2E / 8.0
ROWS = 96
PAIR = 192
OWN = 768
CTXR = 64
BLOCK = 2 * OWN + 2 * CTXR
QT = 256
NQ = 6
UNITS = 12
AHEAD = 3
ORDER = (
    (0, 0), (0, 1), (0, 3), (1, 0), (3, 0), (0, 2), (1, 1), (1, 3), (3, 1), (3, 3), (2, 0), (1, 2), (2, 1), (3, 2),
    (2, 3), (2, 2),
)
PACKED = tuple(sum(place[k] << 2 * (n % 8) for n, place in enumerate(ORDER[8 * h : 8 * h + 8])) for k in range(2) for h in range(2))
PASS = {
    0: ((0, 1, 0, 0), (0, 1, 1, 0), (0, 3, 0, 0)),
    1: ((0, 3, 1, 0),),
    2: ((1, 0, 0, 0), (1, 0, 1, 0), (3, 0, 0, 0), (3, 0, 1, 0)),
    4: ((0, 2, 0, 0), (0, 2, 1, 0)),
    5: ((1, 1, 0, 0), (1, 1, 1, 0)),
    6: ((1, 3, 0, 0), (1, 3, 1, 0), (2, 0, 0, 0), (2, 0, 1, 0)),
    7: ((3, 1, 0, 0), (3, 1, 1, 0)),
    8: ((3, 3, 0, 0), (3, 3, 1, 0)),
    10: ((1, 2, 0, 0), (1, 2, 1, 0), (2, 1, 0, 0), (2, 1, 1, 0)),
    11: ((3, 2, 0, 0), (3, 2, 1, 0)),
    12: ((2, 3, 0, 0), (2, 3, 1, 0)),
    14: ((2, 2, 0, 0), (2, 2, 1, 0)),
}
HALF = OWN // 2
PARTS = ((0, OWN), (OWN, BLOCK - OWN))


def remote(src, dst, send, recv, sp, tp):
    return pltpu.make_async_remote_copy(
        src_ref=src, dst_ref=dst, send_sem=send, recv_sem=recv, device_id=(sp, tp), device_id_type=MESH
    )


def round_y(buf, rows, send, recv, s, y, c):
    up, down = ((y + 1) % 4) * 2 + c, ((y + 3) % 4) * 2 + c
    sib = y * 2 + 1 - c
    half = rows // 2

    def at(slot, offset, size):
        return buf.at[slot, pl.ds(pl.multiple_of(c * rows + offset, 16), size)]

    def one(k, source, slot, offset, size, to):
        return remote(at(source, offset, size), at(slot, offset, size), send.at[k], recv.at[k], s, to)

    return [
        one(0, 0, 0, 0, rows, sib),
        one(1, 0, 1, 0, half, up),
        one(2, 0, 2, half, half, down),
        one(3, 0, 1, half, half, up),
        one(4, 0, 2, 0, half, down),
        one(5, 1, 3, 0, half, up),
        one(6, 2, 3, half, half, down),
        one(7, 1, 1, 0, rows, sib),
        one(8, 2, 2, 0, rows, sib),
        one(9, 3, 3, 0, rows, sib),
    ]


def kernel(
    latent, context, cond, gain, mod_shift, mod_scale, mod_gate, w_query, w_key, w_value, w_out, lambdas,
    context_bias, head_gain, out,
    lat, ctx, mod, wqkv, part, msg, msg2, mods, qv, kvown, qown, kv, qb, qm, vctx, sscr, tops, acc, peak, nsend, nrm,
    wall, lsend, lrecv, wsend, wrecv, msend, mrecv, nsd, nrc, zsend, zqsend, kvrecv, qrecv, fsib, fplus, fminus,
    osend, orecv, local, ready,
):
    s, t = lax.axis_index("sp"), lax.axis_index("tp")
    z, x, y, c = s // 4, s % 4, t // 2, t % 2
    sib = y * 2 + 1 - c

    barrier = pltpu.get_barrier_semaphore()
    for d in range(1, 8):
        pl.semaphore_signal(barrier, inc=1, device_id=(s, (t + d) % 8), device_id_type=MESH)
    for d in range(1, 4):
        pl.semaphore_signal(barrier, inc=1, device_id=(z * 4 + (x + d) % 4, t), device_id_type=MESH)
        pl.semaphore_signal(barrier, inc=1, device_id=((z + d) % 4 * 4 + x, t), device_id_type=MESH)
    loads = [
        pltpu.make_async_copy(src, dst, local.at[k])
        for k, (src, dst) in enumerate(
            (
                (mod_shift, mod.at[0]),
                (mod_scale, mod.at[1]),
                (mod_gate, mod.at[2]),
                (latent, lat.at[0, pl.ds(pl.multiple_of(c * ROWS, 16), ROWS)]),
                (context, ctx),
                (w_query, wqkv.at[0]),
                (w_key, wqkv.at[1]),
                (w_value, wqkv.at[2]),
                (w_out, wall.at[0, pl.ds(pl.multiple_of(c * 256, 256), 256)]),
            )
        )
    ]
    for copy in loads:
        copy.start()

    cols = cond[:, pl.ds(pl.multiple_of(s * 128, 128), 128)]
    activated = (cols / (1.0 + jnp.exp(-cols))).astype(BF)
    activated = jnp.concatenate([activated.astype(F32), jnp.zeros((6, 128), F32)], axis=0).astype(BF)
    msg[12:16, :] = jnp.zeros((4, 128), F32)
    for index in range(3):
        loads[index].wait()
        product = jnp.dot(activated, mod[index], preferred_element_type=F32)
        for r in range(2):
            for half in range(2):
                line = index * 4 + r * 2 + half
                msg[line : line + 1, :] = product[r : r + 1, half * 128 : half * 128 + 128]
    loads[3].wait()
    pl.semaphore_wait(barrier, 13)

    lcp = round_y(lat, ROWS, lsend, lrecv, s, y, c)
    for k in (1, 2, 3, 4, 0):
        lcp[k].start()
    for d in range(1, 4):
        pl.semaphore_signal(ready, inc=1, device_id=((z + d) % 4 * 4 + x, t), device_id_type=MESH)
    pl.semaphore_wait(ready, 3)
    mcp = [remote(msg, part.at[s], msend.at[d], mrecv.at[d], (s + d) % 16, t) for d in range(1, 16)]
    for copy in mcp:
        copy.start()
    part[s] = msg[...]
    for copy in mcp:
        copy.wait_recv()
    total = part[0]
    for k in range(1, 16):
        total = total + part[k]
    msg2[...] = total
    msg2[12:13, 0:2] = lambdas[...]
    msg2[13:14, 0:2] = context_bias[...]
    ncp = [remote(msg2, mods.at[t], nsd.at[d], nrc.at[d], s, (t + d) % 8) for d in range(1, 8)]
    for copy in ncp:
        copy.start()
    mods[t] = msg2[...]
    lcp[1].wait_recv()
    lcp[5].start()
    lcp[2].wait_recv()
    lcp[6].start()
    lcp[3].wait_recv()
    lcp[7].start()
    lcp[4].wait_recv()
    lcp[8].start()
    for copy in ncp:
        copy.wait_recv()

    def vector(index, r):
        row = index * 4 + r * 2
        return jnp.concatenate([mods[k, row + h : row + h + 1, :] for k in range(8) for h in range(2)], axis=1)

    def modulate(rows, r):
        rows = rows.astype(F32)
        normal = rows * lax.rsqrt(jnp.mean(rows * rows, axis=1, keepdims=True) + EPS)
        return (normal * (gain[...] * (1.0 + vector(1, r))) + vector(0, r)).astype(BF)

    def project(p):
        hidden = modulate(lat[p], 0)
        rows = slice(PAIR * p, PAIR * p + PAIR)
        first = PAIR * p + HALF * (p // 2)
        qv[0, rows, :] = jnp.dot(hidden, wqkv[0], preferred_element_type=F32)
        keys = jnp.dot(hidden, wqkv[1], preferred_element_type=F32).astype(BF)
        for i in range(2):
            kvown[i, first : first + PAIR, :] = keys[:, 128 * i : 128 * i + 128]
        qv[1, rows, :] = jnp.dot(hidden, wqkv[2], preferred_element_type=F32)

    for copy in loads[4:]:
        copy.wait()
    hidden = modulate(ctx[...], 1)
    keys = jnp.dot(hidden, wqkv[1], preferred_element_type=F32).astype(BF)
    values = jnp.dot(hidden, wqkv[2], preferred_element_type=F32).astype(BF)
    for i in range(2):
        kvown[i, 2 * OWN : 2 * OWN + CTXR, :] = keys[:, 128 * i : 128 * i + 128]
        kvown[i, 2 * OWN + CTXR : BLOCK, :] = values[:, 128 * i : 128 * i + 128]
    lcp[0].wait_recv()
    project(0)
    lcp[7].wait_recv()
    project(1)

    primary = c == z // 2
    plus, minus = z * 4 + (x + 1) % 4, z * 4 + (x + 3) % 4

    def turn(part):
        for a in range(3 * part, 3 * part + 3):
            for i in range(2):
                rows, columns = slice(128 * a, 128 * a + 128), slice(128 * i, 128 * i + 128)
                qown[part, i, a % 3] = qv[0, rows, columns].T.astype(BF)
                first = OWN * part + HALF + 128 * (a % 3)
                kvown[i, first : first + 128, :] = qv[1, rows, columns].T.astype(BF)

    def distance(i):
        return (2 * c + i - z + 4) % 4

    def slot_of(dz):
        return 3 * (dz == 0).astype(jnp.int32) + (dz == 1).astype(jnp.int32) + 2 * (dz == 3).astype(jnp.int32)

    def q_to(i, part):
        slot = slot_of((z - 2 * c - i + 4) % 4)
        return remote(
            qown.at[part, i], qb.at[slot], zqsend.at[i, part], qrecv.at[slot], (2 * c + i) * 4 + x, sib if part else t
        )

    def part_of(ref, b, part):
        return ref.at[b, pl.ds(*PARTS[part])]

    def kv_to(i, part):
        return remote(
            part_of(kvown, i, part), part_of(kv, s, part), zsend.at[i, part], kvrecv.at[part, s],
            (2 * c + i) * 4 + x, t,
        )

    def source(dz, dx):
        return ((z + dz) % 4) * 4 + (x + dx) % 4

    def onward(dz, dx, part):
        b = source(dz, dx)
        src = part_of(kvown, z % 2, part) if (dz, dx) == (0, 0) else part_of(kv, b, part)
        dst = part_of(kv, b, part)
        copies = []
        if dx == 0 or (dx == 3 and dz < 2):
            copies.append(remote(src, dst, fplus.at[part, b], kvrecv.at[part, b], plus, t))
        if dx == 0 or (dx == 1 and dz >= 2):
            copies.append(remote(src, dst, fminus.at[part, b], kvrecv.at[part, b], minus, t))
        copies.append(remote(src, dst, fsib.at[part, b], kvrecv.at[part, b], s, sib))
        return copies

    def arrive(b, part):
        pltpu.make_async_copy(part_of(kvown, 0, part), part_of(kv, b, part), kvrecv.at[part, b]).wait()

    def pass_on(dz, dx, part, how):
        if how < 2:
            arrive(source(dz, dx), part)
        for copy in onward(dz, dx, part):
            if how == 0 or (how == 1) == (copy.device_id[1] is sib):
                copy.start()

    def send_part(part):
        for i in range(2):
            if part:
                q_to(i, 1).start()

            @pl.when(distance(i) != 0)
            def _():
                if not part:
                    q_to(i, 0).start()

            @pl.when(distance(i) == 0)
            def _():
                if not part:
                    pltpu.make_async_copy(qown.at[0, i], qb.at[3], qrecv.at[3]).start()
                pltpu.make_async_copy(part_of(kvown, i, part), part_of(kv, s, part), kvrecv.at[part, s]).start()

        @pl.when(primary)
        def _():
            for copy in onward(0, 0, part):
                copy.start()

        if part:
            for i in range(2):

                @pl.when(distance(i) % 2 == 1)
                def _():
                    kv_to(i, 0).start()
                    kv_to(i, 1).start()

    def send_far(part):
        for i in range(2):

            @pl.when(distance(i) == 2)
            def _():
                kv_to(i, part).start()

    turn(0)
    send_part(0)
    lcp[5].wait_recv()
    lcp[6].wait_recv()
    lcp[9].start()
    lcp[8].wait_recv()
    project(2)
    lcp[9].wait_recv()
    project(3)
    turn(1)
    send_part(1)
    wcp = round_y(wall, 256, wsend, wrecv, s, y, c)
    for k in (1, 2, 3, 4, 0):
        wcp[k].start()

    for u in range(UNITS):
        acc[u] = jnp.zeros_like(acc[u])
        peak[u] = jnp.full_like(peak[u], -1e30)
    for k in range(4):
        pltpu.make_async_copy(qown.at[0, 0], qb.at[k], qrecv.at[k]).wait()

    for chunk in range(12):
        tile, columns = chunk // 2, slice(128 * (chunk % 2), 128 * (chunk % 2) + 128)
        block = qb[chunk // 3, chunk % 3]
        zero = jnp.zeros((64, 128), BF)
        qm[0, tile, 0:64, columns] = block[0:64]
        qm[0, tile, 64:128, columns] = zero
        qm[1, tile, 0:64, columns] = zero
        qm[1, tile, 64:128, columns] = block[64:128]

    def score(u, at, keys, size):
        raw = jnp.dot(keys, qm[u % 2, u // 2], preferred_element_type=F32)
        sscr[at % (AHEAD + 1), 0:size, :] = raw
        tops[at % (AHEAD + 1)] = jnp.max(raw, axis=0, keepdims=True) * SCALE

    def weigh(u, at, lhs, size, bias):
        slot = at % (AHEAD + 1)
        top = tops[slot] if bias is None else tops[slot] + bias
        old = peak[u]
        new = jnp.maximum(old, top)
        peak[u] = new
        faded = jnp.exp2(old - new)
        shift = new if bias is None else new - bias
        probs = jnp.exp2(sscr[slot, 0:size, :] * SCALE - shift).astype(BF)
        acc[u] = acc[u] * faded + jnp.dot(lhs, probs, preferred_element_type=F32)

    def latent_keys(b):
        return jnp.concatenate([kv[b, 0:HALF, :], kv[b, OWN : OWN + HALF, :]], axis=0)

    def latent_lhs(b):
        lhs = jnp.concatenate([kv[b, k : k + 128, :] for a in (HALF, OWN + HALF) for k in range(a, a + HALF, 128)], axis=1)
        return jnp.concatenate([lhs, jnp.ones((16, OWN), BF)], axis=0)

    def block_at(n):
        late = (n >= 8).astype(jnp.int32)
        by = 2 * (n - 8 * late)
        dz = ((PACKED[0] * (1 - late) + PACKED[1] * late) >> by) % 4
        dx = ((PACKED[2] * (1 - late) + PACKED[3] * late) >> by) % 4
        return source(dz, dx)

    arrive(s, 0)
    arrive(s, 1)
    keys, lhs = latent_keys(s), latent_lhs(s)
    for u in range(AHEAD):
        score(u, u, keys, OWN)
    for u in range(UNITS):
        if u + AHEAD < UNITS:
            score(u + AHEAD, u + AHEAD, keys, OWN)
        weigh(u, u, lhs, OWN, None)


    @pl.when(primary)
    def _():
        for place in PASS[0]:
            pass_on(*place)

    @pl.when(jnp.logical_not(primary))
    def _():
        arrive(source(0, 1), 0)
        arrive(source(0, 1), 1)

    keys = latent_keys(source(0, 1))
    for u in range(AHEAD):
        score(u, u, keys, OWN)

    def step(n, b):
        following = block_at(n + 1)

        @pl.when(primary)
        def _():
            for steps in ((1, 2, 4), (5, 6, 7), (8, 10, 11), (12, 14)):

                @pl.when((n >= steps[0]) & (n <= steps[-1]))
                def _():
                    for k in steps:

                        @pl.when(n == k)
                        def _():
                            for place in PASS[k]:
                                pass_on(*place)

        @pl.when(jnp.logical_not(primary))
        def _():
            arrive(following, 0)
            arrive(following, 1)

        @pl.when(n == 1)
        def _():
            send_far(0)
            send_far(1)

        @pl.when(n == 7)
        def _():
            for k in (1, 2):
                wcp[k].wait_recv()
                wcp[k + 4].start()
            for k in (3, 4):
                wcp[k].wait_recv()
                wcp[k + 4].start()

        @pl.when(n == 13)
        def _():
            wcp[5].wait_recv()
            wcp[6].wait_recv()
            wcp[9].start()

        keys, later, lhs = latent_keys(b), latent_keys(following), latent_lhs(b)
        for u in range(UNITS):
            if u + AHEAD < UNITS:
                score(u + AHEAD, u + AHEAD, keys, OWN)
            else:
                score(u + AHEAD - UNITS, u + AHEAD, later, OWN)
            weigh(u, u, lhs, OWN, None)
        return following

    last = lax.fori_loop(1, 15, step, source(0, 1))

    lane = lax.broadcasted_iota(jnp.int32, (1, 128), 1)
    owner = y * 2 + z // 2

    def pick(row):
        return jnp.sum(jnp.where(lane == z % 2, mods[owner, row : row + 1, :], 0.0), axis=1, keepdims=True)

    bias, lam = pick(13) * LOG2E, pick(12)
    head = y * 4 + z
    half = 1 - primary.astype(jnp.int32)

    def piece(k):
        offset = half if k % 4 // 2 == 0 else 3 * half + 3
        target = ((y + offset) % 4) * 2 + k % 2
        src = nsend.at[ROWS * k : ROWS * k + ROWS]
        return remote(src, nrm.at[head], osend.at[k], orecv.at[head], ((z + (2, 1, 3, 0)[k // 4]) % 4) * 4 + x, target)

    for k in range(8):
        pair = jnp.concatenate([kv[2 * k, 2 * OWN + CTXR : BLOCK, :], kv[2 * k + 1, 2 * OWN + CTXR : BLOCK, :]], axis=0)
        vctx[:, 128 * k : 128 * k + 128] = pair.astype(F32).T.astype(BF)
    size = 16 * CTXR
    keys = (latent_keys(last), jnp.concatenate([kv[k, 2 * OWN : 2 * OWN + CTXR, :] for k in range(16)], axis=0))
    lhs = (latent_lhs(last), jnp.concatenate([vctx[...], jnp.ones((16, size), BF)], axis=0))
    sizes, biases = (OWN, size), (None, bias)
    turns = [(0, u) for u in range(4)]
    for u in range(0, UNITS, 2):
        turns += [(1, u), (1, u + 1)]
        turns += [(0, u + 4), (0, u + 5)] if u + 5 < UNITS else []
    pieces = 0
    for k, (which, u) in enumerate(turns):
        if k + AHEAD < len(turns):
            other, v = turns[k + AHEAD]
            score(v, k + AHEAD, keys[other], sizes[other])
        weigh(u, k, lhs[which], sizes[which], biases[which])
        if which == 0 or u % 2 == 0:
            continue
        tile = u // 2
        one, two = acc[2 * tile], acc[2 * tile + 1]
        mixed = one[0:128] / one[128:129] - lam * (two[0:128] / two[128:129])
        normed = mixed * lax.rsqrt(jnp.mean(mixed * mixed, axis=0, keepdims=True) + EPS)
        for r in range(QT // 128):
            block = normed[:, 128 * r : 128 * r + 128].T * head_gain[...]
            row = QT * tile + 128 * r
            nsend[row : row + 128, :] = block.astype(BF)
        if tile in (0, 2):
            continue
        ready = QT * (tile + 1) // ROWS
        for e in range(pieces, ready):
            if e not in (12, 13):
                piece(e).start()
                continue
            mine = primary & (c == e - 12)

            @pl.when(mine)
            def _():
                src = nsend.at[ROWS * e : ROWS * e + ROWS]
                pltpu.make_async_copy(src, nrm.at[head], orecv.at[head]).start()

            @pl.when(jnp.logical_not(mine))
            def _():
                piece(e).start()

        pieces = ready

    for k in (0, 7, 8, 9):
        wcp[k].wait_recv()
    attended = jnp.zeros((ROWS, 2048), F32)
    for k in (1 - z // 2, z // 2):
        firsts = [4 * ((y + off) % 4) + 2 * k for off in (0, 3, 1, 2)]
        for first in firsts:
            for h in (first, first + 1):
                pltpu.make_async_copy(nsend.at[0:ROWS], nrm.at[h], orecv.at[h]).wait()
        for p, first in enumerate(firsts):
            rows = jnp.concatenate([nrm[first], nrm[first + 1]], axis=1)
            part_of_w = wall[p, pl.ds(pl.multiple_of(256 * k, 256), 256), :]
            product = jnp.dot(rows, part_of_w, preferred_element_type=F32)
            attended = attended + product.astype(BF).astype(F32)
    rows = lat[0, pl.ds(pl.multiple_of(c * ROWS, 16), ROWS), :].astype(F32)
    out[...] = (rows + vector(2, 0) * attended.astype(BF).astype(F32)).astype(BF)

    for copy in lcp + wcp + mcp + ncp:
        copy.wait_send()
    for i in range(2):
        q_to(i, 1).wait_send()

        @pl.when(distance(i) != 0)
        def _():
            q_to(i, 0).wait_send()
            for part in range(2):
                kv_to(i, part).wait_send()

    @pl.when(primary)
    def _():
        for place in ORDER:
            for part in range(2):
                for copy in onward(*place, part):
                    copy.wait_send()

    for e in range(16):
        if e not in (12, 13):
            piece(e).wait_send()
            continue

        @pl.when(jnp.logical_not(primary & (c == e - 12)))
        def _():
            piece(e).wait_send()


def per_device(
    latent, context, conditioning, norm_gain, mod_shift, mod_scale, mod_gate, w_query, w_key, w_value, w_out,
    lambdas, context_bias, head_gain,
):
    dma = pltpu.SemaphoreType.DMA
    vmem = pl.BlockSpec(memory_space=pltpu.VMEM)
    hbm = pl.BlockSpec(memory_space=pl.ANY)
    return pl.pallas_call(
        kernel,
        name="block",
        out_shape=jax.ShapeDtypeStruct(latent.shape, BF),
        in_specs=[hbm, hbm, vmem, vmem] + [hbm] * 7 + [vmem] * 3,
        out_specs=vmem,
        scratch_shapes=[
            pltpu.VMEM((4, PAIR, 2048), BF),
            pltpu.VMEM((CTXR, 2048), BF),
            pltpu.VMEM((3, 128, 256), BF),
            pltpu.VMEM((3, 2048, 256), BF),
            pltpu.VMEM((16, 16, 128), F32),
            pltpu.VMEM((16, 128), F32),
            pltpu.VMEM((16, 128), F32),
            pltpu.VMEM((8, 16, 128), F32),
            pltpu.VMEM((2, OWN, 256), F32),
            pltpu.VMEM((2, BLOCK, 128), BF),
            pltpu.VMEM((2, 2, 3, 128, 128), BF),
            pltpu.VMEM((16, BLOCK, 128), BF),
            pltpu.VMEM((4, 3, 128, 128), BF),
            pltpu.VMEM((2, NQ, 128, QT), BF),
            pltpu.VMEM((128, 16 * CTXR), BF),
            pltpu.VMEM((AHEAD + 1, 16 * CTXR, QT), F32),
            pltpu.VMEM((AHEAD + 1, 1, QT), F32),
            pltpu.VMEM((UNITS, 144, QT), F32),
            pltpu.VMEM((UNITS, 1, QT), F32),
            pltpu.VMEM((1536, 128), BF),
            pltpu.VMEM((16, ROWS, 128), BF),
            pltpu.VMEM((4, 512, 2048), BF),
            dma((10,)), dma((10,)), dma((10,)), dma((10,)),
            dma((16,)), dma((16,)), dma((8,)), dma((8,)),
            dma((2, 2)), dma((2, 2)), dma((2, 16)), dma((4,)),
            dma((2, 16)), dma((2, 16)), dma((2, 16)),
            dma((16,)), dma((16,)), dma((9,)),
            pltpu.SemaphoreType.REGULAR,
        ],
        compiler_params=pltpu.CompilerParams(
            collective_id=0, has_side_effects=True, vmem_limit_bytes=60 * 2**20
        ),
    )(
        latent, context, conditioning, norm_gain.reshape(1, -1), mod_shift, mod_scale, mod_gate, w_query, w_key,
        w_value, w_out, lambdas.reshape(1, -1), context_bias.reshape(1, -1), head_gain.reshape(1, -1),
    )


def solution(mesh):
    return jax.shard_map(
        per_device,
        mesh=mesh,
        in_specs=(
            P(("sp", "tp"), None),
            P("sp", None),
            P(),
            P(),
            P("sp", "tp"),
            P("sp", "tp"),
            P("sp", "tp"),
            P(None, "tp"),
            P(None, "tp"),
            P(None, "tp"),
            P("tp", None),
            P("tp"),
            P("tp"),
            P(),
        ),
        out_specs=P(("sp", "tp"), None),
        check_vma=False,
    )
```

```python
import functools
import math

import jax
import jax.numpy as jnp
from jax import lax
from jax.experimental import pallas as pl
from jax.experimental.pallas import tpu as pltpu
from jax.sharding import PartitionSpec as P

EPS = 1e-06
MESH = pl.DeviceIdType.MESH
BF = jnp.bfloat16
F32 = jnp.float32
LOG2E = math.log2(math.e)
SCALE = LOG2E / 8.0
ROWS = 96
PAIR = 192
OWN = 768
CTXR = 64
BLOCK = 2 * OWN + 2 * CTXR
QT = 256
NQ = 6
UNITS = 12
AHEAD = 3
FIRST = (
    (0, 0), (0, 1), (1, 0), (0, 1), (1, 0), (0, 2), (1, 1), (1, 3), (3, 1), (3, 3), (2, 0), (1, 2), (2, 1), (2, 3),
    (3, 2), (2, 2),
)
SECOND = (FIRST[0], (0, 3), (3, 0), (0, 3), (3, 0)) + FIRST[5:]
PACKED = tuple(
    tuple(sum(place[k] << 2 * n for n, place in enumerate(order[8 * word : 8 * word + 8])) for word in range(2))
    for order in (FIRST, SECOND)
    for k in range(2)
)
PASS = {
    3: ((1, 0, 1), (3, 0, 1)), 4: ((0, 2, 0), (0, 2, 1)), 5: ((1, 1, 0), (1, 1, 1)), 6: ((1, 3, 0), (1, 3, 1)),
    7: ((2, 0, 0), (2, 0, 1), (3, 1, 0), (3, 1, 1)), 8: ((3, 3, 0), (3, 3, 1)), 10: ((1, 2, 0), (1, 2, 1)),
    11: ((2, 1, 0), (2, 1, 1)), 12: ((2, 3, 0), (2, 3, 1)), 13: ((3, 2, 0), (3, 2, 1)), 14: ((2, 2, 0), (2, 2, 1)),
}
HALF = OWN // 2
PARTS = ((0, OWN), (OWN, BLOCK - OWN))


def remote(src, dst, send, recv, sp, tp):
    return pltpu.make_async_remote_copy(
        src_ref=src, dst_ref=dst, send_sem=send, recv_sem=recv, device_id=(sp, tp), device_id_type=MESH
    )


def round_y(buf, rows, send, recv, s, y, c):
    up, down = ((y + 1) % 4) * 2 + c, ((y + 3) % 4) * 2 + c
    sib = y * 2 + 1 - c
    half = rows // 2

    def at(slot, offset, size):
        return buf.at[slot, pl.ds(pl.multiple_of(c * rows + offset, 16), size)]

    def one(k, source, slot, offset, size, to):
        return remote(at(source, offset, size), at(slot, offset, size), send.at[k], recv.at[k], s, to)

    return [
        one(0, 0, 0, 0, rows, sib),
        one(1, 0, 1, 0, half, up),
        one(2, 0, 2, half, half, down),
        one(3, 0, 1, half, half, up),
        one(4, 0, 2, 0, half, down),
        one(5, 1, 3, 0, half, up),
        one(6, 2, 3, half, half, down),
        one(7, 1, 1, 0, rows, sib),
        one(8, 2, 2, 0, rows, sib),
        one(9, 3, 3, 0, rows, sib),
    ]


def kernel(
    latent, context, cond, gain, mod_shift, mod_scale, mod_gate, w_query, w_key, w_value, w_out, lambdas,
    context_bias, head_gain, out,
    lat, ctx, hctx, mod, wqkv, part, msg, msg2, mods, qv, kvown, qown, kv, qb, qm, vctx, sscr, tops, acc, peak, nsend, nrm,
    wall, lsend, lrecv, wsend, wrecv, msend, mrecv, nsd, nrc, zsend, zqsend, kvrecv, qrecv, fsib, fplus, fminus,
    osend, orecv, local, ready,
):
    s, t = lax.axis_index("sp"), lax.axis_index("tp")
    z, x, y, c = s // 4, s % 4, t // 2, t % 2
    sib = y * 2 + 1 - c

    barrier = pltpu.get_barrier_semaphore()
    for d in range(1, 8):
        pl.semaphore_signal(barrier, inc=1, device_id=(s, (t + d) % 8), device_id_type=MESH)
    for d in range(1, 4):
        pl.semaphore_signal(barrier, inc=1, device_id=(z * 4 + (x + d) % 4, t), device_id_type=MESH)
        pl.semaphore_signal(barrier, inc=1, device_id=((z + d) % 4 * 4 + x, t), device_id_type=MESH)
    loads = [
        pltpu.make_async_copy(src, dst, local.at[k])
        for k, (src, dst) in enumerate(
            (
                (mod_shift, mod.at[0]),
                (mod_scale, mod.at[1]),
                (mod_gate, mod.at[2]),
                (latent, lat.at[0, pl.ds(pl.multiple_of(c * ROWS, 16), ROWS)]),
                (context, ctx),
                (w_query, wqkv.at[0]),
                (w_key, wqkv.at[1]),
                (w_value, wqkv.at[2]),
                (w_out, wall.at[0, pl.ds(pl.multiple_of(c * 256, 256), 256)]),
            )
        )
    ]
    for copy in loads[:4]:
        copy.start()

    cols = cond[:, pl.ds(pl.multiple_of(s * 128, 128), 128)]
    activated = (cols / (1.0 + jnp.exp(-cols))).astype(BF)
    activated = jnp.concatenate([activated.astype(F32), jnp.zeros((6, 128), F32)], axis=0).astype(BF)
    msg[12:16, :] = jnp.zeros((4, 128), F32)
    for index in range(3):
        loads[index].wait()
        product = jnp.dot(activated, mod[index], preferred_element_type=F32)
        for r in range(2):
            for half in range(2):
                line = index * 4 + r * 2 + half
                msg[line : line + 1, :] = product[r : r + 1, half * 128 : half * 128 + 128]
    loads[3].wait()
    for copy in loads[4:]:
        copy.start()
    pl.semaphore_wait(barrier, 13)

    lcp = round_y(lat, ROWS, lsend, lrecv, s, y, c)
    for k in (1, 2, 3, 4, 0):
        lcp[k].start()
    for d in range(1, 4):
        pl.semaphore_signal(ready, inc=1, device_id=((z + d) % 4 * 4 + x, t), device_id_type=MESH)
    pl.semaphore_wait(ready, 3)
    mcp = [remote(msg, part.at[s], msend.at[d], mrecv.at[d], (s + d) % 16, t) for d in range(1, 16)]
    for copy in mcp:
        copy.start()
    part[s] = msg[...]
    for copy in mcp:
        copy.wait_recv()
    total = part[0]
    for k in range(1, 16):
        total = total + part[k]
    msg2[...] = total
    msg2[12:13, 0:2] = lambdas[...]
    msg2[13:14, 0:2] = context_bias[...]
    ncp = [remote(msg2, mods.at[t], nsd.at[d], nrc.at[d], s, (t + d) % 8) for d in range(1, 8)]
    for copy in ncp:
        copy.start()
    mods[t] = msg2[...]
    lcp[1].wait_recv()
    lcp[5].start()
    lcp[2].wait_recv()
    lcp[6].start()
    lcp[3].wait_recv()
    lcp[7].start()
    lcp[4].wait_recv()
    lcp[8].start()
    for copy in ncp:
        copy.wait_recv()

    def vector(index, r):
        row = index * 4 + r * 2
        return jnp.concatenate([mods[k, row + h : row + h + 1, :] for k in range(8) for h in range(2)], axis=1)

    def modulate(rows, r):
        rows = rows.astype(F32)
        normal = rows * lax.rsqrt(jnp.mean(rows * rows, axis=1, keepdims=True) + EPS)
        return (normal * (gain[...] * (1.0 + vector(1, r))) + vector(0, r)).astype(BF)

    def project(rows, p, more=None):
        size = rows.shape[0]
        hidden = modulate(rows, 0)
        queries = jnp.dot(hidden, wqkv[0], preferred_element_type=F32).astype(BF)
        if more is not None:
            hidden = jnp.concatenate([hidden, more[...]], axis=0)
        keys = jnp.dot(hidden, wqkv[1], preferred_element_type=F32).astype(BF)
        values = jnp.dot(hidden, wqkv[2], preferred_element_type=F32)
        first = PAIR * p + HALF * (p // 2)
        for i in range(2):
            columns = slice(128 * i, 128 * i + 128)
            kvown[i, first : first + size, :] = keys[:size, columns]
            for k in range(size // PAIR):
                qown[p + k, i] = queries[PAIR * k : PAIR * k + PAIR, columns]
            if more is not None:
                kvown[i, 2 * OWN : 2 * OWN + CTXR, :] = keys[size:, columns]
                kvown[i, 2 * OWN + CTXR : BLOCK, :] = values[size:, columns].astype(BF)
        qv[PAIR * p : PAIR * p + size, :] = values[:size]

    for copy in loads[4:]:
        copy.wait()
    lcp[0].wait_recv()
    lcp[7].wait_recv()
    project(lat[0:2].reshape(2 * PAIR, 2048), 0)

    primary = c == z // 2
    plus, minus = z * 4 + (x + 1) % 4, z * 4 + (x + 3) % 4

    def turn(part):
        for a in range(3 * part, 3 * part + 3):
            for i in range(2):
                first = OWN * part + HALF + 128 * (a % 3)
                block = qv[128 * a : 128 * a + 128, 128 * i : 128 * i + 128]
                kvown[i, first : first + 128, :] = block.T.astype(BF)

    def distance(i):
        return (2 * c + i - z + 4) % 4

    def slot_of(dz):
        return 3 * (dz == 0).astype(jnp.int32) + (dz == 1).astype(jnp.int32) + 2 * (dz == 3).astype(jnp.int32)

    def q_to(i, p):
        rows = pl.ds(pl.multiple_of(PAIR * slot_of((z - 2 * c - i + 4) % 4), 16), PAIR)
        return remote(
            qown.at[p, i], qb.at[p // 2, rows], zqsend.at[i, p], qrecv.at[p // 2, slot_of((z - 2 * c - i + 4) % 4)],
            (2 * c + i) * 4 + x, sib if p % 2 else t,
        )

    def send_q(p):
        for i in range(2):
            if p % 2:
                q_to(i, p).start()
                continue

            @pl.when(distance(i) != 0)
            def _():
                q_to(i, p).start()

            @pl.when(distance(i) == 0)
            def _():
                rows = qb.at[p // 2, 3 * PAIR : 4 * PAIR]
                pltpu.make_async_copy(qown.at[p, i], rows, qrecv.at[p // 2, 3]).start()

    def part_of(ref, b, part):
        return ref.at[b, pl.ds(*PARTS[part])]

    def kv_to(i, part):
        return remote(
            part_of(kvown, i, part), part_of(kv, s, part), zsend.at[i, part], kvrecv.at[part, s],
            (2 * c + i) * 4 + x, t,
        )

    def source(dz, dx):
        return ((z + dz) % 4) * 4 + (x + dx) % 4

    def onward(dz, dx, part):
        b = source(dz, dx)
        src = part_of(kvown, z % 2, part) if (dz, dx) == (0, 0) else part_of(kv, b, part)
        dst = part_of(kv, b, part)
        copies = {}
        if dx == 0 or (dx == 3 and dz < 2):
            copies["p"] = remote(src, dst, fplus.at[part, b], kvrecv.at[part, b], plus, t)
        if dx == 0 or (dx == 1 and dz >= 2):
            copies["m"] = remote(src, dst, fminus.at[part, b], kvrecv.at[part, b], minus, t)
        copies["s"] = remote(src, dst, fsib.at[part, b], kvrecv.at[part, b], s, sib)
        return copies

    def arrive(b, part):
        pltpu.make_async_copy(part_of(kvown, 0, part), part_of(kv, b, part), kvrecv.at[part, b]).wait()

    def go_on(dz, dx, part, ways="spm"):
        for way, copy in onward(dz, dx, part).items():
            if way in ways:
                copy.start()

    def pass_on(dz, dx, part, ways="spm"):
        arrive(source(dz, dx), part)
        go_on(dz, dx, part, ways)

    def send_part(part):
        for i in range(2):

            @pl.when(distance(i) == 0)
            def _():
                pltpu.make_async_copy(part_of(kvown, i, part), part_of(kv, s, part), kvrecv.at[part, s]).start()

        @pl.when(primary)
        def _():
            go_on(0, 0, part)

        for i in range(2):

            @pl.when(distance(i) % 2 == 1)
            def _():
                kv_to(i, part).start()

    def send_far(part):
        for i in range(2):

            @pl.when(distance(i) == 2)
            def _():
                kv_to(i, part).start()

    send_q(0)
    send_q(1)
    turn(0)
    send_part(0)
    lcp[5].wait_recv()
    lcp[6].wait_recv()
    lcp[9].start()
    lcp[8].wait_recv()
    project(lat[2], 2)
    send_q(2)
    hctx[...] = modulate(ctx[...], 1)
    lcp[9].wait_recv()
    project(lat[3], 3, hctx)
    send_q(3)
    turn(1)
    send_part(1)
    wcp = round_y(wall, 256, wsend, wrecv, s, y, c)
    for k in (1, 2, 3, 4, 0):
        wcp[k].start()

    for u in range(UNITS):
        acc[u] = jnp.zeros_like(acc[u])
        peak[u] = jnp.full_like(peak[u], -1e30)

    @pl.when(primary)
    def _():
        pass_on(0, 1, 0)
        pass_on(0, 3, 0)

    def take_queries(part):
        for k in range(4):
            rows = qb.at[part, PAIR * k : PAIR * k + PAIR]
            pltpu.make_async_copy(qown.at[0, 0], rows, qrecv.at[part, k]).wait()
        for r in range(6):
            tile, columns = 3 * part + r // 2, slice(128 * (r % 2), 128 * (r % 2) + 128)
            block = qb[part, 128 * r : 128 * r + 128, :].astype(F32).T.astype(BF)
            zero = jnp.zeros((64, 128), BF)
            qm[0, tile, 0:64, columns] = block[0:64]
            qm[0, tile, 64:128, columns] = zero
            qm[1, tile, 0:64, columns] = zero
            qm[1, tile, 64:128, columns] = block[64:128]

    take_queries(0)

    def score(u, at, keys, size):
        raw = jnp.dot(keys, qm[u % 2, u // 2], preferred_element_type=F32)
        sscr[at % (AHEAD + 1), 0:size, :] = raw
        tops[at % (AHEAD + 1)] = jnp.max(raw, axis=0, keepdims=True) * SCALE

    def weigh(u, at, lhs, size, bias):
        slot = at % (AHEAD + 1)
        top = tops[slot] if bias is None else tops[slot] + bias
        old = peak[u]
        new = jnp.maximum(old, top)
        peak[u] = new
        faded = jnp.exp2(old - new)
        shift = new if bias is None else new - bias
        probs = jnp.exp2(sscr[slot, 0:size, :] * SCALE - shift).astype(BF)
        acc[u] = acc[u] * faded + jnp.dot(lhs, probs, preferred_element_type=F32)

    def parts_of(n):
        if isinstance(n, int):
            pair = source(*FIRST[n]), source(*SECOND[n])
            return *pair, OWN if n in (3, 4) else 0, 0 if n in (1, 2) else OWN
        late = (n >= 8).astype(jnp.int32)
        by = 2 * (n - 8 * late)
        dz, dx, ez, ex = (((w[0] * (1 - late) + w[1] * late) >> by) % 4 for w in PACKED)
        return source(dz, dx), source(ez, ex), OWN * (n < 5).astype(jnp.int32)

    def rows_of(b, row, offset):
        if not isinstance(row, int):
            row = pl.multiple_of(row, 128)
        return kv[b, pl.ds(row + offset, HALF), :]

    def latent_keys(a, b, p, q):
        return jnp.concatenate([rows_of(a, p, 0), rows_of(b, q, 0)], axis=0)

    def latent_lhs(a, b, p, q):
        halves = rows_of(a, p, HALF), rows_of(b, q, HALF)
        lhs = jnp.concatenate([half[128 * k : 128 * k + 128] for half in halves for k in range(3)], axis=1)
        return jnp.concatenate([lhs, jnp.ones((16, OWN), BF)], axis=0)

    def stream(turns, keys, lhs, at=0, done=0, sizes=None, biases=None, after=None, ends=()):
        size = lambda which: OWN if sizes is None else sizes[which]
        for k in range(done, AHEAD):
            which, u = turns[k]
            score(u, at + k, keys[which], size(which))
        coming = list(turns) + list(ends)
        for k, (which, u) in enumerate(turns):
            if k + AHEAD < len(coming):
                other, v = coming[k + AHEAD]
                score(v, at + k + AHEAD, keys[other], size(other))
            weigh(u, at + k, lhs[which], size(which), None if biases is None else biases[which])
            if after is not None:
                after(which, u)

    @pl.when(jnp.logical_not(primary))
    def _():
        arrive(source(0, 1), 0)
        arrive(source(0, 3), 0)

    arrive(s, 0)
    arrive(s, 1)
    held = [parts_of(n) for n in range(4)]
    keys, lhs = [latent_keys(*h) for h in held[:2]], [latent_lhs(*h) for h in held[:2]]
    stream([(n, u) for n in range(2) for u in range(6)], keys, lhs)
    both = primary, jnp.logical_not(primary)

    @pl.when(both[0])
    def _():
        pass_on(1, 0, 0)
        pass_on(3, 0, 0, "sm")

    @pl.when(both[1])
    def _():
        arrive(source(1, 0), 0)
        arrive(source(3, 0), 0)

    stream([(0, u) for u in range(6)], [latent_keys(*held[2])], [latent_lhs(*held[2])])

    @pl.when(both[0])
    def _():
        pass_on(0, 3, 1)
        pass_on(0, 1, 1)
        go_on(3, 0, 0, "p")

    @pl.when(both[1])
    def _():
        arrive(source(0, 1), 1)
        arrive(source(0, 3), 1)

    send_far(0)
    send_far(1)
    take_queries(1)
    keys, lhs = [latent_keys(*h) for h in held], [latent_lhs(*h) for h in held[:3]]
    stream(
        [(n, u) for n in range(3) for u in range(6, UNITS)], keys, lhs, at=2, ends=[(3, u) for u in range(AHEAD)]
    )

    def step(n, now):
        following = parts_of(n + 1)

        @pl.when(primary)
        def _():
            for steps in ((3, 4, 5), (6, 7, 8), (10, 11, 12), (13, 14)):

                @pl.when((n >= steps[0]) & (n <= steps[-1]))
                def _():
                    for k in steps:

                        @pl.when(n == k)
                        def _():
                            for place in PASS[k]:
                                pass_on(*place)

        @pl.when(jnp.logical_not(primary))
        def _():
            @pl.when(n == 3)
            def _():
                arrive(following[0], 1)

            @pl.when(n != 3)
            def _():
                arrive(following[0], 0)

            arrive(following[1], 1)

        @pl.when(n == 9)
        def _():
            for k in (1, 2):
                wcp[k].wait_recv()
                wcp[k + 4].start()
            for k in (3, 4):
                wcp[k].wait_recv()
                wcp[k + 4].start()

        stream(
            [(0, u) for u in range(UNITS)], [latent_keys(*now, OWN), latent_keys(*following, OWN)], [latent_lhs(*now, OWN)],
            done=AHEAD, ends=[(1, u) for u in range(AHEAD)],
        )
        return following

    last = lax.fori_loop(3, 15, step, (*held[3][:2], jnp.int32(OWN)))
    wcp[5].wait_recv()
    wcp[6].wait_recv()
    wcp[9].start()

    lane = lax.broadcasted_iota(jnp.int32, (1, 128), 1)
    owner = y * 2 + z // 2

    def pick(row):
        return jnp.sum(jnp.where(lane == z % 2, mods[owner, row : row + 1, :], 0.0), axis=1, keepdims=True)

    bias, lam = pick(13) * LOG2E, pick(12)
    head = y * 4 + z
    half = 1 - primary.astype(jnp.int32)

    def piece(k):
        offset = 3 * half if k < 8 else 1 + half
        target = ((y + offset) % 4) * 2 + k % 2
        src = nsend.at[ROWS * k : ROWS * k + ROWS]
        return remote(src, nrm.at[head], osend.at[k], orecv.at[head], ((z + (2, 1, 3, 0)[k % 8 // 2]) % 4) * 4 + x, target)

    for k in range(8):
        pair = jnp.concatenate([kv[2 * k, 2 * OWN + CTXR : BLOCK, :], kv[2 * k + 1, 2 * OWN + CTXR : BLOCK, :]], axis=0)
        vctx[:, 128 * k : 128 * k + 128] = pair.astype(F32).T.astype(BF)
    size = 16 * CTXR
    whole = source(*FIRST[15]), source(*FIRST[15]), 0, OWN
    keys = (latent_keys(*whole), jnp.concatenate([kv[k, 2 * OWN : 2 * OWN + CTXR, :] for k in range(16)], axis=0))
    lhs = (latent_lhs(*whole), jnp.concatenate([vctx[...], jnp.ones((16, size), BF)], axis=0))
    turns = [(0, u) for u in range(4)]
    for u in range(0, UNITS, 2):
        turns += [(1, u), (1, u + 1)]
        turns += [(0, u + 4), (0, u + 5)] if u + 5 < UNITS else []
    sent = {2: range(0, 8), 4: range(8, 13), 5: range(13, 16)}

    def finish(which, u):
        if which == 0 or u % 2 == 0:
            return
        tile = u // 2
        one, two = acc[2 * tile], acc[2 * tile + 1]
        mixed = one[0:128] / one[128:129] - lam * (two[0:128] / two[128:129])
        normed = mixed * lax.rsqrt(jnp.mean(mixed * mixed, axis=0, keepdims=True) + EPS)
        for r in range(QT // 128):
            block = normed[:, 128 * r : 128 * r + 128].T * head_gain[...]
            row = QT * tile + 128 * r
            nsend[row : row + 128, :] = block.astype(BF)
        for e in sent.get(tile, ()):
            if e not in (6, 7):
                piece(e).start()
                continue
            mine = primary & (c == e - 6)

            @pl.when(mine)
            def _():
                src = nsend.at[ROWS * e : ROWS * e + ROWS]
                pltpu.make_async_copy(src, nrm.at[head], orecv.at[head]).start()

            @pl.when(jnp.logical_not(mine))
            def _():
                piece(e).start()

    stream(turns, keys, lhs, done=AHEAD, sizes=(OWN, size), biases=(None, bias), after=finish)

    for k in (0, 7, 8, 9):
        wcp[k].wait_recv()
    attended = jnp.zeros((ROWS, 2048), F32)
    for k in (1 - z // 2, z // 2):
        firsts = [4 * ((y + off) % 4) + 2 * k for off in (0, 3, 1, 2)]
        for first in firsts:
            for h in (first, first + 1):
                pltpu.make_async_copy(nsend.at[0:ROWS], nrm.at[h], orecv.at[h]).wait()
        for p, first in enumerate(firsts):
            rows = jnp.concatenate([nrm[first], nrm[first + 1]], axis=1)
            part_of_w = wall[p, pl.ds(pl.multiple_of(256 * k, 256), 256), :]
            product = jnp.dot(rows, part_of_w, preferred_element_type=F32)
            attended = attended + product.astype(BF).astype(F32)
    rows = lat[0, pl.ds(pl.multiple_of(c * ROWS, 16), ROWS), :].astype(F32)
    out[...] = (rows + vector(2, 0) * attended.astype(BF).astype(F32)).astype(BF)

    for copy in lcp + wcp + mcp + ncp:
        copy.wait_send()
    for i in range(2):
        for p in (1, 3):
            q_to(i, p).wait_send()

        @pl.when(distance(i) != 0)
        def _():
            for p in (0, 2):
                q_to(i, p).wait_send()
            for part in range(2):
                kv_to(i, part).wait_send()

    @pl.when(primary)
    def _():
        for place in [(dz, dx) for dz in range(4) for dx in range(4)]:
            for part in range(2):
                for copy in onward(*place, part).values():
                    copy.wait_send()

    for e in range(16):
        if e not in (6, 7):
            piece(e).wait_send()
            continue

        @pl.when(jnp.logical_not(primary & (c == e - 6)))
        def _():
            piece(e).wait_send()


def per_device(
    latent, context, conditioning, norm_gain, mod_shift, mod_scale, mod_gate, w_query, w_key, w_value, w_out,
    lambdas, context_bias, head_gain,
):
    dma = pltpu.SemaphoreType.DMA
    vmem = pl.BlockSpec(memory_space=pltpu.VMEM)
    hbm = pl.BlockSpec(memory_space=pl.ANY)
    return pl.pallas_call(
        kernel,
        name="block",
        out_shape=jax.ShapeDtypeStruct(latent.shape, BF),
        in_specs=[hbm, hbm, vmem, vmem] + [hbm] * 7 + [vmem] * 3,
        out_specs=vmem,
        scratch_shapes=[
            pltpu.VMEM((4, PAIR, 2048), BF),
            pltpu.VMEM((CTXR, 2048), BF),
            pltpu.VMEM((CTXR, 2048), BF),
            pltpu.VMEM((3, 128, 256), BF),
            pltpu.VMEM((3, 2048, 256), BF),
            pltpu.VMEM((16, 16, 128), F32),
            pltpu.VMEM((16, 128), F32),
            pltpu.VMEM((16, 128), F32),
            pltpu.VMEM((8, 16, 128), F32),
            pltpu.VMEM((OWN, 256), F32),
            pltpu.VMEM((2, BLOCK, 128), BF),
            pltpu.VMEM((4, 2, PAIR, 128), BF),
            pltpu.VMEM((16, BLOCK, 128), BF),
            pltpu.VMEM((2, OWN, 128), BF),
            pltpu.VMEM((2, NQ, 128, QT), BF),
            pltpu.VMEM((128, 16 * CTXR), BF),
            pltpu.VMEM((AHEAD + 1, 16 * CTXR, QT), F32),
            pltpu.VMEM((AHEAD + 1, 1, QT), F32),
            pltpu.VMEM((UNITS, 144, QT), F32),
            pltpu.VMEM((UNITS, 1, QT), F32),
            pltpu.VMEM((1536, 128), BF),
            pltpu.VMEM((16, ROWS, 128), BF),
            pltpu.VMEM((4, 512, 2048), BF),
            dma((10,)), dma((10,)), dma((10,)), dma((10,)),
            dma((16,)), dma((16,)), dma((8,)), dma((8,)),
            dma((2, 2)), dma((2, 4)), dma((2, 16)), dma((2, 4)),
            dma((2, 16)), dma((2, 16)), dma((2, 16)),
            dma((16,)), dma((16,)), dma((9,)),
            pltpu.SemaphoreType.REGULAR,
        ],
        compiler_params=pltpu.CompilerParams(
            collective_id=0, has_side_effects=True, vmem_limit_bytes=60 * 2**20
        ),
    )(
        latent, context, conditioning, norm_gain.reshape(1, -1), mod_shift, mod_scale, mod_gate, w_query, w_key,
        w_value, w_out, lambdas.reshape(1, -1), context_bias.reshape(1, -1), head_gain.reshape(1, -1),
    )


def solution(mesh):
    return jax.shard_map(
        per_device,
        mesh=mesh,
        in_specs=(
            P(("sp", "tp"), None),
            P("sp", None),
            P(),
            P(),
            P("sp", "tp"),
            P("sp", "tp"),
            P("sp", "tp"),
            P(None, "tp"),
            P(None, "tp"),
            P(None, "tp"),
            P("tp", None),
            P("tp"),
            P("tp"),
            P(),
        ),
        out_specs=P(("sp", "tp"), None),
        check_vma=False,
    )
```

```python
import functools
import math

import jax
import jax.numpy as jnp
from jax import lax
from jax.experimental import pallas as pl
from jax.experimental.pallas import tpu as pltpu
from jax.sharding import PartitionSpec as P

EPS = 1e-06
MESH = pl.DeviceIdType.MESH
BF = jnp.bfloat16
F32 = jnp.float32
LOG2E = math.log2(math.e)
SCALE = LOG2E / 8.0
ROWS = 96
PAIR = 192
OWN = 768
CTXR = 64
BLOCK = 2 * OWN + 2 * CTXR
QT = 256
NQ = 6
UNITS = 12
AHEAD = 3
FIRST = (
    (0, 0), (0, 1), (1, 0), (0, 1), (1, 0), (0, 2), (1, 1), (1, 3), (3, 1), (3, 3), (2, 0), (1, 2), (2, 1), (2, 3),
    (3, 2), (2, 2),
)
SECOND = (FIRST[0], (0, 3), (3, 0), (0, 3), (3, 0)) + FIRST[5:]
PACKED = tuple(
    tuple(sum(place[k] << 2 * n for n, place in enumerate(order[8 * word : 8 * word + 8])) for word in range(2))
    for order in (FIRST, SECOND)
    for k in range(2)
)
PASS = {
    3: ((1, 0, 1), (3, 0, 1)), 4: ((0, 2, 0), (0, 2, 1)), 5: ((1, 1, 0), (1, 1, 1)), 6: ((1, 3, 0), (1, 3, 1)),
    7: ((2, 0, 0), (2, 0, 1), (3, 1, 0), (3, 1, 1)), 8: ((3, 3, 0), (3, 3, 1)), 10: ((1, 2, 0), (1, 2, 1)),
    11: ((2, 1, 0), (2, 1, 1)), 12: ((2, 3, 0), (2, 3, 1)), 13: ((3, 2, 0), (3, 2, 1)), 14: ((2, 2, 0), (2, 2, 1)),
}
HALF = OWN // 2
PARTS = ((0, OWN), (OWN, BLOCK - OWN))


def remote(src, dst, send, recv, sp, tp):
    return pltpu.make_async_remote_copy(
        src_ref=src, dst_ref=dst, send_sem=send, recv_sem=recv, device_id=(sp, tp), device_id_type=MESH
    )


def settle(ref, sem):
    pltpu.make_async_copy(ref, ref, sem).wait()


def round_y(buf, rows, send, recv, s, y, c):
    up, down = ((y + 1) % 4) * 2 + c, ((y + 3) % 4) * 2 + c
    sib = y * 2 + 1 - c
    half = rows // 2

    def at(slot, offset, size):
        return buf.at[slot, pl.ds(pl.multiple_of(c * rows + offset, 16), size)]

    def one(k, source, slot, offset, size, to):
        return remote(at(source, offset, size), at(slot, offset, size), send.at[k], recv.at[k], s, to)

    return [
        one(0, 0, 0, 0, rows, sib),
        one(1, 0, 1, 0, half, up),
        one(2, 0, 2, half, half, down),
        one(3, 0, 1, half, half, up),
        one(4, 0, 2, 0, half, down),
        one(5, 1, 3, 0, half, up),
        one(6, 2, 3, half, half, down),
        one(7, 1, 1, 0, rows, sib),
        one(8, 2, 2, 0, rows, sib),
        one(9, 3, 3, 0, rows, sib),
    ]


def kernel(
    latent, context, cond_in, gain_in, mod_shift, mod_scale, mod_gate, w_query, w_key, w_value, w_out, lambdas_in,
    bias_in, head_gain_in, out,
    lat, ctx, hctx, mod, wqkv, part, msg, msg2, mods, qv, kvown, qown, kv, qb, qm, vctx, sscr, tops, acc, peak, nsend, nrm,
    wall, cond, gain, lambdas, context_bias, head_gain, lsend, lrecv, wsend, wrecv, msend, mrecv, nsd, nrc, zsend, zqsend, kvrecv, qrecv, fwd,
    osend, orecv, local, ready,
):
    s, t = lax.axis_index("sp"), lax.axis_index("tp")
    z, x, y, c = s // 4, s % 4, t // 2, t % 2
    sib = y * 2 + 1 - c

    barrier = pltpu.get_barrier_semaphore()
    for d in range(1, 8):
        pl.semaphore_signal(barrier, inc=1, device_id=(s, (t + d) % 8), device_id_type=MESH)
    for d in range(1, 4):
        pl.semaphore_signal(barrier, inc=1, device_id=(z * 4 + (x + d) % 4, t), device_id_type=MESH)
        pl.semaphore_signal(barrier, inc=1, device_id=((z + d) % 4 * 4 + x, t), device_id_type=MESH)
    loads = [
        pltpu.make_async_copy(src, dst, local.at[k])
        for k, (src, dst) in enumerate(
            (
                (cond_in, cond),
                (mod_shift, mod.at[0]),
                (mod_scale, mod.at[1]),
                (mod_gate, mod.at[2]),
                (latent, lat.at[0, pl.ds(pl.multiple_of(c * ROWS, 16), ROWS)]),
                (context, ctx),
                (lambdas_in, lambdas),
                (bias_in, context_bias),
                (gain_in, gain),
                (head_gain_in, head_gain),
                (w_query, wqkv.at[0]),
                (w_key, wqkv.at[1]),
                (w_value, wqkv.at[2]),
                (w_out, wall.at[0, pl.ds(pl.multiple_of(c * 256, 256), 256)]),
            )
        )
    ]
    for copy in loads[:5]:
        copy.start()
    loads[0].wait()

    cols = cond[:, pl.ds(pl.multiple_of(s * 128, 128), 128)]
    activated = (cols / (1.0 + jnp.exp(-cols))).astype(BF)
    activated = jnp.concatenate([activated.astype(F32), jnp.zeros((6, 128), F32)], axis=0).astype(BF)
    msg[12:16, :] = jnp.zeros((4, 128), F32)
    for index in range(3):
        loads[index + 1].wait()
        product = jnp.dot(activated, mod[index], preferred_element_type=F32)
        for r in range(2):
            for half in range(2):
                line = index * 4 + r * 2 + half
                msg[line : line + 1, :] = product[r : r + 1, half * 128 : half * 128 + 128]
    loads[4].wait()
    for copy in loads[5:]:
        copy.start()
    pl.semaphore_wait(barrier, 13)

    lcp = round_y(lat, ROWS, lsend, lrecv, s, y, c)
    for k in (1, 2, 3, 4, 0):
        lcp[k].start()
    for d in range(1, 4):
        pl.semaphore_signal(ready, inc=1, device_id=((z + d) % 4 * 4 + x, t), device_id_type=MESH)
    pl.semaphore_wait(ready, 3)
    mcp = [remote(msg, part.at[s], msend.at[0], mrecv.at[0], (s + d) % 16, t) for d in range(1, 16)]
    for copy in mcp:
        copy.start()
    part[s] = msg[...]
    settle(part.at[0:15], mrecv.at[0])
    total = part[0]
    for k in range(1, 16):
        total = total + part[k]
    for copy in loads[5:]:
        copy.wait()
    msg2[...] = total
    msg2[12:13, 0:2] = lambdas[...]
    msg2[13:14, 0:2] = context_bias[...]
    ncp = [remote(msg2, mods.at[t], nsd.at[0], nrc.at[0], s, (t + d) % 8) for d in range(1, 8)]
    for copy in ncp:
        copy.start()
    mods[t] = msg2[...]
    lcp[1].wait_recv()
    lcp[5].start()
    lcp[2].wait_recv()
    lcp[6].start()
    lcp[3].wait_recv()
    lcp[7].start()
    lcp[4].wait_recv()
    lcp[8].start()
    settle(mods.at[0:7], nrc.at[0])

    def vector(index, r):
        row = index * 4 + r * 2
        return jnp.concatenate([mods[k, row + h : row + h + 1, :] for k in range(8) for h in range(2)], axis=1)

    def modulate(rows, r):
        rows = rows.astype(F32)
        normal = rows * lax.rsqrt(jnp.mean(rows * rows, axis=1, keepdims=True) + EPS)
        return (normal * (gain[...] * (1.0 + vector(1, r))) + vector(0, r)).astype(BF)

    def project(rows, p, more=None):
        size = rows.shape[0]
        hidden = modulate(rows, 0)
        queries = jnp.dot(hidden, wqkv[0], preferred_element_type=F32).astype(BF)
        if more is not None:
            hidden = jnp.concatenate([hidden, more[...]], axis=0)
        keys = jnp.dot(hidden, wqkv[1], preferred_element_type=F32).astype(BF)
        values = jnp.dot(hidden, wqkv[2], preferred_element_type=F32)
        first = PAIR * p + HALF * (p // 2)
        for i in range(2):
            columns = slice(128 * i, 128 * i + 128)
            kvown[i, first : first + size, :] = keys[:size, columns]
            for k in range(size // PAIR):
                qown[p + k, i] = queries[PAIR * k : PAIR * k + PAIR, columns]
            if more is not None:
                kvown[i, 2 * OWN : 2 * OWN + CTXR, :] = keys[size:, columns]
                kvown[i, 2 * OWN + CTXR : BLOCK, :] = values[size:, columns].astype(BF)
        qv[PAIR * p : PAIR * p + size, :] = values[:size]

    lcp[0].wait_recv()
    lcp[7].wait_recv()
    project(lat[0:2].reshape(2 * PAIR, 2048), 0)

    primary = c == z // 2
    plus, minus = z * 4 + (x + 1) % 4, z * 4 + (x + 3) % 4

    def turn(part):
        for a in range(3 * part, 3 * part + 3):
            for i in range(2):
                first = OWN * part + HALF + 128 * (a % 3)
                block = qv[128 * a : 128 * a + 128, 128 * i : 128 * i + 128]
                kvown[i, first : first + 128, :] = block.T.astype(BF)

    def distance(i):
        return (2 * c + i - z + 4) % 4

    def slot_of(dz):
        return 3 * (dz == 0).astype(jnp.int32) + (dz == 1).astype(jnp.int32) + 2 * (dz == 3).astype(jnp.int32)

    def q_to(i, p):
        rows = pl.ds(pl.multiple_of(PAIR * slot_of((z - 2 * c - i + 4) % 4), 16), PAIR)
        return remote(
            qown.at[p, i], qb.at[p // 2, rows], zqsend.at[i, p], qrecv.at[p // 2],
            (2 * c + i) * 4 + x, sib if p % 2 else t,
        )

    def send_q(p):
        for i in range(2):
            if p % 2:
                q_to(i, p).start()
                continue

            @pl.when(distance(i) != 0)
            def _():
                q_to(i, p).start()

            @pl.when(distance(i) == 0)
            def _():
                rows = qb.at[p // 2, 3 * PAIR : 4 * PAIR]
                pltpu.make_async_copy(qown.at[p, i], rows, qrecv.at[p // 2]).start()

    def part_of(ref, b, part):
        return ref.at[b, pl.ds(*PARTS[part])]

    def kv_to(i, part):
        return remote(
            part_of(kvown, i, part), part_of(kv, s, part), zsend.at[i, part], kvrecv.at[part, s],
            (2 * c + i) * 4 + x, t,
        )

    def source(dz, dx):
        return ((z + dz) % 4) * 4 + (x + dx) % 4

    def onward(dz, dx, part):
        b = source(dz, dx)
        src = part_of(kvown, z % 2, part) if (dz, dx) == (0, 0) else part_of(kv, b, part)
        dst = part_of(kv, b, part)
        copies = {}
        if dx == 0 or (dx == 3 and dz < 2):
            copies["p"] = remote(src, dst, fwd.at[0], kvrecv.at[part, b], plus, t)
        if dx == 0 or (dx == 1 and dz >= 2):
            copies["m"] = remote(src, dst, fwd.at[1], kvrecv.at[part, b], minus, t)
        copies["s"] = remote(src, dst, fwd.at[2], kvrecv.at[part, b], s, sib)
        return copies

    def arrive(b, part):
        pltpu.make_async_copy(part_of(kvown, 0, part), part_of(kv, b, part), kvrecv.at[part, b]).wait()

    def go_on(dz, dx, part, ways="spm"):
        for way, copy in onward(dz, dx, part).items():
            if way in ways:
                copy.start()

    def pass_on(dz, dx, part, ways="spm"):
        arrive(source(dz, dx), part)
        go_on(dz, dx, part, ways)

    def send_part(part):
        for i in range(2):

            @pl.when(distance(i) == 0)
            def _():
                pltpu.make_async_copy(part_of(kvown, i, part), part_of(kv, s, part), kvrecv.at[part, s]).start()

        @pl.when(primary)
        def _():
            go_on(0, 0, part)

        for i in range(2):

            @pl.when(distance(i) % 2 == 1)
            def _():
                kv_to(i, part).start()

    def send_far(part):
        for i in range(2):

            @pl.when(distance(i) == 2)
            def _():
                kv_to(i, part).start()

    send_q(0)
    send_q(1)
    turn(0)
    send_part(0)
    lcp[5].wait_recv()
    lcp[6].wait_recv()
    lcp[9].start()
    lcp[8].wait_recv()
    project(lat[2], 2)
    send_q(2)
    hctx[...] = modulate(ctx[...], 1)
    lcp[9].wait_recv()
    project(lat[3], 3, hctx)
    send_q(3)
    turn(1)
    send_part(1)
    wcp = round_y(wall, 256, wsend, wrecv, s, y, c)
    for k in (1, 2, 3, 4, 0):
        wcp[k].start()

    for u in range(UNITS):
        acc[u] = jnp.zeros_like(acc[u])
        peak[u] = jnp.full_like(peak[u], -1e30)

    @pl.when(primary)
    def _():
        pass_on(0, 1, 0)
        pass_on(0, 3, 0)

    def take_queries(part):
        settle(qb.at[part], qrecv.at[part])
        for r in range(6):
            tile, columns = 3 * part + r // 2, slice(128 * (r % 2), 128 * (r % 2) + 128)
            block = qb[part, 128 * r : 128 * r + 128, :].astype(F32).T.astype(BF)
            zero = jnp.zeros((64, 128), BF)
            qm[0, tile, 0:64, columns] = block[0:64]
            qm[0, tile, 64:128, columns] = zero
            qm[1, tile, 0:64, columns] = zero
            qm[1, tile, 64:128, columns] = block[64:128]

    take_queries(0)

    def score(u, at, keys, size):
        raw = jnp.dot(keys, qm[u % 2, u // 2], preferred_element_type=F32)
        sscr[at % (AHEAD + 1), 0:size, :] = raw
        tops[at % (AHEAD + 1)] = jnp.max(raw, axis=0, keepdims=True) * SCALE

    def weigh(u, at, lhs, size, bias):
        slot = at % (AHEAD + 1)
        top = tops[slot] if bias is None else tops[slot] + bias
        old = peak[u]
        new = jnp.maximum(old, top)
        peak[u] = new
        faded = jnp.exp2(old - new)
        shift = new if bias is None else new - bias
        probs = jnp.exp2(sscr[slot, 0:size, :] * SCALE - shift).astype(BF)
        acc[u] = acc[u] * faded + jnp.dot(lhs, probs, preferred_element_type=F32)

    def parts_of(n):
        if isinstance(n, int):
            pair = source(*FIRST[n]), source(*SECOND[n])
            return *pair, OWN if n in (3, 4) else 0, 0 if n in (1, 2) else OWN
        late = (n >= 8).astype(jnp.int32)
        by = 2 * (n - 8 * late)
        dz, dx, ez, ex = (((w[0] * (1 - late) + w[1] * late) >> by) % 4 for w in PACKED)
        return source(dz, dx), source(ez, ex), OWN * (n < 5).astype(jnp.int32)

    def rows_of(b, row, offset):
        if not isinstance(row, int):
            row = pl.multiple_of(row, 128)
        return kv[b, pl.ds(row + offset, HALF), :]

    def latent_keys(a, b, p, q):
        return jnp.concatenate([rows_of(a, p, 0), rows_of(b, q, 0)], axis=0)

    def latent_lhs(a, b, p, q):
        halves = rows_of(a, p, HALF), rows_of(b, q, HALF)
        lhs = jnp.concatenate([half[128 * k : 128 * k + 128] for half in halves for k in range(3)], axis=1)
        return jnp.concatenate([lhs, jnp.ones((16, OWN), BF)], axis=0)

    def stream(turns, keys, lhs, at=0, done=0, sizes=None, biases=None, after=None, ends=()):
        size = lambda which: OWN if sizes is None else sizes[which]
        for k in range(done, AHEAD):
            which, u = turns[k]
            score(u, at + k, keys[which], size(which))
        coming = list(turns) + list(ends)
        for k, (which, u) in enumerate(turns):
            if k + AHEAD < len(coming):
                other, v = coming[k + AHEAD]
                score(v, at + k + AHEAD, keys[other], size(other))
            weigh(u, at + k, lhs[which], size(which), None if biases is None else biases[which])
            if after is not None:
                after(which, u)

    @pl.when(jnp.logical_not(primary))
    def _():
        arrive(source(0, 1), 0)
        arrive(source(0, 3), 0)

    arrive(s, 0)
    arrive(s, 1)
    held = [parts_of(n) for n in range(4)]
    keys, lhs = [latent_keys(*h) for h in held[:2]], [latent_lhs(*h) for h in held[:2]]
    stream([(n, u) for n in range(2) for u in range(6)], keys, lhs)
    both = primary, jnp.logical_not(primary)

    @pl.when(both[0])
    def _():
        pass_on(1, 0, 0)
        pass_on(3, 0, 0, "sm")

    @pl.when(both[1])
    def _():
        arrive(source(1, 0), 0)
        arrive(source(3, 0), 0)

    stream([(0, u) for u in range(6)], [latent_keys(*held[2])], [latent_lhs(*held[2])])

    @pl.when(both[0])
    def _():
        pass_on(0, 3, 1)
        pass_on(0, 1, 1)
        go_on(3, 0, 0, "p")

    @pl.when(both[1])
    def _():
        arrive(source(0, 1), 1)
        arrive(source(0, 3), 1)

    send_far(0)
    send_far(1)
    take_queries(1)
    keys, lhs = [latent_keys(*h) for h in held], [latent_lhs(*h) for h in held[:3]]
    stream(
        [(n, u) for n in range(3) for u in range(6, UNITS)], keys, lhs, at=2, ends=[(3, u) for u in range(AHEAD)]
    )

    def step(n, now):
        following = parts_of(n + 1)

        @pl.when(primary)
        def _():
            for steps in ((3, 4, 5), (6, 7, 8), (10, 11, 12), (13, 14)):

                @pl.when((n >= steps[0]) & (n <= steps[-1]))
                def _():
                    for k in steps:

                        @pl.when(n == k)
                        def _():
                            for place in PASS[k]:
                                pass_on(*place)

        @pl.when(jnp.logical_not(primary))
        def _():
            @pl.when(n == 3)
            def _():
                arrive(following[0], 1)

            @pl.when(n != 3)
            def _():
                arrive(following[0], 0)

            arrive(following[1], 1)

        @pl.when(n == 9)
        def _():
            for k in (1, 2):
                wcp[k].wait_recv()
                wcp[k + 4].start()
            for k in (3, 4):
                wcp[k].wait_recv()
                wcp[k + 4].start()

        stream(
            [(0, u) for u in range(UNITS)], [latent_keys(*now, OWN), latent_keys(*following, OWN)], [latent_lhs(*now, OWN)],
            done=AHEAD, ends=[(1, u) for u in range(AHEAD)],
        )
        return following

    last = lax.fori_loop(3, 15, step, (*held[3][:2], jnp.int32(OWN)))
    wcp[5].wait_recv()
    wcp[6].wait_recv()
    wcp[9].start()

    lane = lax.broadcasted_iota(jnp.int32, (1, 128), 1)
    owner = y * 2 + z // 2

    def pick(row):
        return jnp.sum(jnp.where(lane == z % 2, mods[owner, row : row + 1, :], 0.0), axis=1, keepdims=True)

    bias, lam = pick(13) * LOG2E, pick(12)
    head = y * 4 + z
    half = 1 - primary.astype(jnp.int32)

    def spot(h, row):
        return 8 * (h % 4 // 2 == row // 2).astype(jnp.int32) + h // 4 * 2 + h % 2

    def piece(k):
        offset = 3 * half if k < 8 else 1 + half
        target = ((y + offset) % 4) * 2 + k % 2
        src = nsend.at[ROWS * k : ROWS * k + ROWS]
        row = (z + (2, 1, 3, 0)[k % 8 // 2]) % 4
        late = (row // 2 == z // 2).astype(jnp.int32)
        return remote(src, nrm.at[spot(head, row)], osend.at[0], orecv.at[late], row * 4 + x, target)

    for k in range(8):
        pair = jnp.concatenate([kv[2 * k, 2 * OWN + CTXR : BLOCK, :], kv[2 * k + 1, 2 * OWN + CTXR : BLOCK, :]], axis=0)
        vctx[:, 128 * k : 128 * k + 128] = pair.astype(F32).T.astype(BF)
    size = 16 * CTXR
    whole = source(*FIRST[15]), source(*FIRST[15]), 0, OWN
    keys = (latent_keys(*whole), jnp.concatenate([kv[k, 2 * OWN : 2 * OWN + CTXR, :] for k in range(16)], axis=0))
    lhs = (latent_lhs(*whole), jnp.concatenate([vctx[...], jnp.ones((16, size), BF)], axis=0))
    turns = [(0, u) for u in range(4)]
    for u in range(0, UNITS, 2):
        turns += [(1, u), (1, u + 1)]
        turns += [(0, u + 4), (0, u + 5)] if u + 5 < UNITS else []
    sent = {2: range(0, 8), 4: range(8, 13), 5: range(13, 16)}

    def finish(which, u):
        if which == 0 or u % 2 == 0:
            return
        tile = u // 2
        one, two = acc[2 * tile], acc[2 * tile + 1]
        mixed = one[0:128] / one[128:129] - lam * (two[0:128] / two[128:129])
        normed = mixed * lax.rsqrt(jnp.mean(mixed * mixed, axis=0, keepdims=True) + EPS)
        for r in range(QT // 128):
            block = normed[:, 128 * r : 128 * r + 128].T * head_gain[...]
            row = QT * tile + 128 * r
            nsend[row : row + 128, :] = block.astype(BF)
        for e in sent.get(tile, ()):
            if e not in (6, 7):
                piece(e).start()
                continue
            mine = primary & (c == e - 6)

            @pl.when(mine)
            def _():
                src = nsend.at[ROWS * e : ROWS * e + ROWS]
                pltpu.make_async_copy(src, nrm.at[spot(head, z)], orecv.at[1]).start()

            @pl.when(jnp.logical_not(mine))
            def _():
                piece(e).start()

    stream(turns, keys, lhs, done=AHEAD, sizes=(OWN, size), biases=(None, bias), after=finish)

    for k in (0, 7, 8, 9):
        wcp[k].wait_recv()
    attended = jnp.zeros((ROWS, 2048), F32)
    for late, k in enumerate((1 - z // 2, z // 2)):
        settle(nrm.at[8 * late : 8 * late + 8], orecv.at[late])
        for p, off in enumerate((0, 3, 1, 2)):
            first = 8 * late + 2 * ((y + off) % 4)
            rows = jnp.concatenate([nrm[first], nrm[first + 1]], axis=1)
            part_of_w = wall[p, pl.ds(pl.multiple_of(256 * k, 256), 256), :]
            product = jnp.dot(rows, part_of_w, preferred_element_type=F32)
            attended = attended + product.astype(BF).astype(F32)
    rows = lat[0, pl.ds(pl.multiple_of(c * ROWS, 16), ROWS), :].astype(F32)
    out[...] = (rows + vector(2, 0) * attended.astype(BF).astype(F32)).astype(BF)

    for copy in lcp + wcp:
        copy.wait_send()
    settle(part.at[0:15], msend.at[0])
    settle(mods.at[0:7], nsd.at[0])
    for i in range(2):
        for p in (1, 3):
            q_to(i, p).wait_send()

        @pl.when(distance(i) != 0)
        def _():
            for p in (0, 2):
                q_to(i, p).wait_send()
            for part in range(2):
                kv_to(i, part).wait_send()

    @pl.when(primary)
    def _():
        settle(kv.at[0:6], fwd.at[0])
        settle(kv.at[0:6], fwd.at[1])
        settle(kv, fwd.at[2])

    @pl.when(primary)
    def _():
        settle(nsend.at[0 : 15 * ROWS], osend.at[0])

    @pl.when(jnp.logical_not(primary))
    def _():
        settle(nsend, osend.at[0])


def per_device(
    latent, context, conditioning, norm_gain, mod_shift, mod_scale, mod_gate, w_query, w_key, w_value, w_out,
    lambdas, context_bias, head_gain,
):
    dma = pltpu.SemaphoreType.DMA
    vmem = pl.BlockSpec(memory_space=pltpu.VMEM)
    hbm = pl.BlockSpec(memory_space=pltpu.HBM)
    return pl.pallas_call(
        kernel,
        name="block",
        out_shape=jax.ShapeDtypeStruct(latent.shape, BF),
        in_specs=[hbm] * 14,
        out_specs=vmem,
        scratch_shapes=[
            pltpu.VMEM((4, PAIR, 2048), BF),
            pltpu.VMEM((CTXR, 2048), BF),
            pltpu.VMEM((CTXR, 2048), BF),
            pltpu.VMEM((3, 128, 256), BF),
            pltpu.VMEM((3, 2048, 256), BF),
            pltpu.VMEM((16, 16, 128), F32),
            pltpu.VMEM((16, 128), F32),
            pltpu.VMEM((16, 128), F32),
            pltpu.VMEM((8, 16, 128), F32),
            pltpu.VMEM((OWN, 256), F32),
            pltpu.VMEM((2, BLOCK, 128), BF),
            pltpu.VMEM((4, 2, PAIR, 128), BF),
            pltpu.VMEM((16, BLOCK, 128), BF),
            pltpu.VMEM((2, OWN, 128), BF),
            pltpu.VMEM((2, NQ, 128, QT), BF),
            pltpu.VMEM((128, 16 * CTXR), BF),
            pltpu.VMEM((AHEAD + 1, 16 * CTXR, QT), F32),
            pltpu.VMEM((AHEAD + 1, 1, QT), F32),
            pltpu.VMEM((UNITS, 144, QT), F32),
            pltpu.VMEM((UNITS, 1, QT), F32),
            pltpu.VMEM((1536, 128), BF),
            pltpu.VMEM((16, ROWS, 128), BF),
            pltpu.VMEM((4, 512, 2048), BF),
            pltpu.VMEM((2, 2048), F32),
            pltpu.VMEM((1, 2048), F32),
            pltpu.VMEM((1, 2), F32),
            pltpu.VMEM((1, 2), F32),
            pltpu.VMEM((1, 128), F32),
            dma((10,)), dma((10,)), dma((10,)), dma((10,)),
            dma((1,)), dma((1,)), dma((1,)), dma((1,)),
            dma((2, 2)), dma((2, 4)), dma((2, 16)), dma((2,)),
            dma((3,)),
            dma((1,)), dma((2,)), dma((14,)),
            pltpu.SemaphoreType.REGULAR,
        ],
        compiler_params=pltpu.CompilerParams(
            collective_id=0, has_side_effects=True, vmem_limit_bytes=60 * 2**20
        ),
    )(
        latent, context, conditioning, norm_gain.reshape(1, -1), mod_shift, mod_scale, mod_gate, w_query, w_key,
        w_value, w_out, lambdas.reshape(1, -1), context_bias.reshape(1, -1), head_gain.reshape(1, -1),
    )


def solution(mesh):
    return jax.shard_map(
        per_device,
        mesh=mesh,
        in_specs=(
            P(("sp", "tp"), None),
            P("sp", None),
            P(),
            P(),
            P("sp", "tp"),
            P("sp", "tp"),
            P("sp", "tp"),
            P(None, "tp"),
            P(None, "tp"),
            P(None, "tp"),
            P("tp", None),
            P("tp"),
            P("tp"),
            P(),
        ),
        out_specs=P(("sp", "tp"), None),
        check_vma=False,
    )
```

```python
import functools
import math

import jax
import jax.numpy as jnp
from jax import lax
from jax.experimental import pallas as pl
from jax.experimental.pallas import tpu as pltpu
from jax.sharding import PartitionSpec as P

EPS = 1e-06
MESH = pl.DeviceIdType.MESH
BF = jnp.bfloat16
F32 = jnp.float32
LOG2E = math.log2(math.e)
SCALE = LOG2E / 8.0
ROWS = 96
PAIR = 192
OWN = 768
CTXR = 64
BLOCK = 2 * OWN + 2 * CTXR
QT = 256
NQ = 6
UNITS = 12
AHEAD = 3
TURNS = (6, 7, 8, 9, 10, 11, 0, 1, 2, 3, 4, 5)
FIRST = (
    (0, 0), (0, 1), (1, 0), (0, 1), (1, 0), (0, 2), (1, 1), (1, 3), (3, 1), (3, 3), (2, 0), (1, 2), (2, 1), (2, 3),
    (3, 2), (2, 2),
)
SECOND = (FIRST[0], (0, 3), (3, 0), (0, 3), (3, 0)) + FIRST[5:]
PACKED = tuple(
    tuple(sum(place[k] << 2 * n for n, place in enumerate(order[8 * word : 8 * word + 8])) for word in range(2))
    for order in (FIRST, SECOND)
    for k in range(2)
)
PASS = {
    3: ((1, 0, 1), (3, 0, 1)), 4: ((0, 2, 0), (0, 2, 1)), 5: ((1, 1, 0), (1, 1, 1)), 6: ((1, 3, 0), (1, 3, 1)),
    7: ((2, 0, 0), (2, 0, 1), (3, 1, 0), (3, 1, 1)), 8: ((3, 3, 0), (3, 3, 1)), 10: ((1, 2, 0), (1, 2, 1)),
    11: ((2, 1, 0), (2, 1, 1)), 12: ((2, 3, 0), (2, 3, 1)), 13: ((3, 2, 0), (3, 2, 1)), 14: ((2, 2, 0), (2, 2, 1)),
}
HALF = OWN // 2
PARTS = ((0, OWN), (OWN, BLOCK - OWN))


def remote(src, dst, send, recv, sp, tp):
    return pltpu.make_async_remote_copy(
        src_ref=src, dst_ref=dst, send_sem=send, recv_sem=recv, device_id=(sp, tp), device_id_type=MESH
    )


def settle(ref, sem):
    pltpu.make_async_copy(ref, ref, sem).wait()


def round_y(buf, rows, send, recv, s, y, c):
    up, down = ((y + 1) % 4) * 2 + c, ((y + 3) % 4) * 2 + c
    sib = y * 2 + 1 - c
    half = rows // 2

    def at(slot, offset, size):
        return buf.at[slot, pl.ds(pl.multiple_of(c * rows + offset, 16), size)]

    def one(k, source, slot, offset, size, to):
        return remote(at(source, offset, size), at(slot, offset, size), send.at[(0, 1, 1, 1, 1, 2, 2, 0, 0, 0)[k]], recv.at[k], s, to)

    return [
        one(0, 0, 0, 0, rows, sib),
        one(1, 0, 1, 0, half, up),
        one(2, 0, 2, half, half, down),
        one(3, 0, 1, half, half, up),
        one(4, 0, 2, 0, half, down),
        one(5, 1, 3, 0, half, up),
        one(6, 2, 3, half, half, down),
        one(7, 1, 1, 0, rows, sib),
        one(8, 2, 2, 0, rows, sib),
        one(9, 3, 3, 0, rows, sib),
    ]


def kernel(
    latent, context, cond_in, gain_in, mod_shift, mod_scale, mod_gate, w_query, w_key, w_value, w_out, lambdas_in,
    bias_in, head_gain_in, out,
    lat, ctx, hctx, mod, wqkv, part, msg, msg2, mods, qv, kvown, qown, kv, qb, qm, vctx, sscr, tops, acc, peak, nsend, nrm,
    wall, cond, gain, lambdas, context_bias, head_gain, lsend, lrecv, wsend, wrecv, msend, mrecv, nsd, nrc, zsend, zqsend, kvrecv, qrecv, fwd,
    osend, orecv, local, ready,
):
    s, t = lax.axis_index("sp"), lax.axis_index("tp")
    z, x, y, c = s // 4, s % 4, t // 2, t % 2
    sib = y * 2 + 1 - c

    barrier = pltpu.get_barrier_semaphore()
    for d in range(1, 8):
        pl.semaphore_signal(barrier, inc=1, device_id=(s, (t + d) % 8), device_id_type=MESH)
    for d in range(1, 4):
        pl.semaphore_signal(barrier, inc=1, device_id=(z * 4 + (x + d) % 4, t), device_id_type=MESH)
        pl.semaphore_signal(barrier, inc=1, device_id=((z + d) % 4 * 4 + x, t), device_id_type=MESH)
    loads = [
        pltpu.make_async_copy(src, dst, local.at[k])
        for k, (src, dst) in enumerate(
            (
                (cond_in, cond),
                (mod_shift, mod.at[0]),
                (mod_scale, mod.at[1]),
                (mod_gate, mod.at[2]),
                (latent, lat.at[0, pl.ds(pl.multiple_of(c * ROWS, 16), ROWS)]),
                (context, ctx),
                (lambdas_in, lambdas),
                (bias_in, context_bias),
                (gain_in, gain),
                (head_gain_in, head_gain),
                (w_query, wqkv.at[0]),
                (w_key, wqkv.at[1]),
                (w_value, wqkv.at[2]),
                (w_out, wall.at[0, pl.ds(pl.multiple_of(c * 256, 256), 256)]),
            )
        )
    ]
    for copy in loads[:5]:
        copy.start()
    loads[0].wait()

    cols = cond[:, pl.ds(pl.multiple_of(s * 128, 128), 128)]
    activated = (cols / (1.0 + jnp.exp(-cols))).astype(BF)
    activated = jnp.concatenate([activated.astype(F32), jnp.zeros((6, 128), F32)], axis=0).astype(BF)
    msg[12:16, :] = jnp.zeros((4, 128), F32)
    for index in range(3):
        loads[index + 1].wait()
        product = jnp.dot(activated, mod[index], preferred_element_type=F32)
        for r in range(2):
            for half in range(2):
                line = index * 4 + r * 2 + half
                msg[line : line + 1, :] = product[r : r + 1, half * 128 : half * 128 + 128]
    loads[4].wait()
    for copy in loads[5:]:
        copy.start()
    pl.semaphore_wait(barrier, 13)

    lcp = round_y(lat, ROWS, lsend, lrecv, s, y, c)
    for k in (1, 2, 3, 4, 0):
        lcp[k].start()
    for d in range(1, 4):
        pl.semaphore_signal(ready, inc=1, device_id=((z + d) % 4 * 4 + x, t), device_id_type=MESH)
    pl.semaphore_wait(ready, 3)
    mcp = [remote(msg, part.at[s], msend.at[0], mrecv.at[0], (s + d) % 16, t) for d in range(1, 16)]
    for copy in mcp:
        copy.start()
    part[s] = msg[...]
    settle(part.at[0:15], mrecv.at[0])
    total = part[0]
    for k in range(1, 16):
        total = total + part[k]
    for copy in loads[5:]:
        copy.wait()
    msg2[...] = total
    msg2[12:13, 0:2] = lambdas[...]
    msg2[13:14, 0:2] = context_bias[...]
    ncp = [remote(msg2, mods.at[t], nsd.at[0], nrc.at[0], s, (t + d) % 8) for d in range(1, 8)]
    for copy in ncp:
        copy.start()
    mods[t] = msg2[...]
    lcp[1].wait_recv()
    lcp[5].start()
    lcp[2].wait_recv()
    lcp[6].start()
    lcp[3].wait_recv()
    lcp[7].start()
    lcp[4].wait_recv()
    lcp[8].start()
    settle(mods.at[0:7], nrc.at[0])

    def vector(index, r):
        row = index * 4 + r * 2
        return jnp.concatenate([mods[k, row + h : row + h + 1, :] for k in range(8) for h in range(2)], axis=1)

    def modulate(rows, r):
        rows = rows.astype(F32)
        normal = rows * lax.rsqrt(jnp.mean(rows * rows, axis=1, keepdims=True) + EPS)
        return (normal * (gain[...] * (1.0 + vector(1, r))) + vector(0, r)).astype(BF)

    def project(rows, p, more=None):
        size = rows.shape[0]
        hidden = modulate(rows, 0)
        queries = jnp.dot(hidden, wqkv[0], preferred_element_type=F32).astype(BF)
        if more is not None:
            hidden = jnp.concatenate([hidden, more[...]], axis=0)
        keys = jnp.dot(hidden, wqkv[1], preferred_element_type=F32).astype(BF)
        values = jnp.dot(hidden, wqkv[2], preferred_element_type=F32)
        first = PAIR * p + HALF * (p // 2)
        for i in range(2):
            columns = slice(128 * i, 128 * i + 128)
            kvown[i, first : first + size, :] = keys[:size, columns]
            for k in range(size // PAIR):
                qown[p + k, i] = queries[PAIR * k : PAIR * k + PAIR, columns]
            if more is not None:
                kvown[i, 2 * OWN : 2 * OWN + CTXR, :] = keys[size:, columns]
                kvown[i, 2 * OWN + CTXR : BLOCK, :] = values[size:, columns].astype(BF)
        qv[PAIR * p : PAIR * p + size, :] = values[:size]

    lcp[0].wait_recv()
    lcp[7].wait_recv()
    project(lat[0:2].reshape(2 * PAIR, 2048), 0)

    primary = c == z // 2
    plus, minus = z * 4 + (x + 1) % 4, z * 4 + (x + 3) % 4

    def turn(part):
        for a in range(3 * part, 3 * part + 3):
            for i in range(2):
                first = OWN * part + HALF + 128 * (a % 3)
                block = qv[128 * a : 128 * a + 128, 128 * i : 128 * i + 128]
                kvown[i, first : first + 128, :] = block.T.astype(BF)

    def distance(i):
        return (2 * c + i - z + 4) % 4

    def slot_of(dz):
        return 3 * (dz == 0).astype(jnp.int32) + (dz == 1).astype(jnp.int32) + 2 * (dz == 3).astype(jnp.int32)

    def q_to(i, p):
        rows = pl.ds(pl.multiple_of(PAIR * slot_of((z - 2 * c - i + 4) % 4), 16), PAIR)
        return remote(
            qown.at[p, i], qb.at[p // 2, rows], zqsend.at[i, p], qrecv.at[p // 2],
            (2 * c + i) * 4 + x, sib if p % 2 else t,
        )

    def send_q(p):
        for i in range(2):
            if p % 2:
                q_to(i, p).start()
                continue

            @pl.when(distance(i) != 0)
            def _():
                q_to(i, p).start()

            @pl.when(distance(i) == 0)
            def _():
                rows = qb.at[p // 2, 3 * PAIR : 4 * PAIR]
                pltpu.make_async_copy(qown.at[p, i], rows, qrecv.at[p // 2]).start()

    def part_of(ref, b, part):
        return ref.at[b, pl.ds(*PARTS[part])]

    def kv_to(i, part):
        return remote(
            part_of(kvown, i, part), part_of(kv, s, part), zsend.at[i, part], kvrecv.at[part, s],
            (2 * c + i) * 4 + x, t,
        )

    def source(dz, dx):
        return ((z + dz) % 4) * 4 + (x + dx) % 4

    def onward(dz, dx, part):
        b = source(dz, dx)
        src = part_of(kvown, z % 2, part) if (dz, dx) == (0, 0) else part_of(kv, b, part)
        dst = part_of(kv, b, part)
        copies = {}
        if dx == 0 or (dx == 3 and dz < 2):
            copies["p"] = remote(src, dst, fwd.at[0], kvrecv.at[part, b], plus, t)
        if dx == 0 or (dx == 1 and dz >= 2):
            copies["m"] = remote(src, dst, fwd.at[1], kvrecv.at[part, b], minus, t)
        copies["s"] = remote(src, dst, fwd.at[2], kvrecv.at[part, b], s, sib)
        return copies

    def arrive(b, part):
        pltpu.make_async_copy(part_of(kvown, 0, part), part_of(kv, b, part), kvrecv.at[part, b]).wait()

    def go_on(dz, dx, part, ways="spm"):
        for way, copy in onward(dz, dx, part).items():
            if way in ways:
                copy.start()

    def pass_on(dz, dx, part, ways="spm"):
        arrive(source(dz, dx), part)
        go_on(dz, dx, part, ways)

    def send_part(part):
        for i in range(2):

            @pl.when(distance(i) == 0)
            def _():
                pltpu.make_async_copy(part_of(kvown, i, part), part_of(kv, s, part), kvrecv.at[part, s]).start()

        @pl.when(primary)
        def _():
            go_on(0, 0, part)

        for i in range(2):

            @pl.when(distance(i) % 2 == 1)
            def _():
                kv_to(i, part).start()

    def send_far(part):
        for i in range(2):

            @pl.when(distance(i) == 2)
            def _():
                kv_to(i, part).start()

    send_q(0)
    send_q(1)
    turn(0)
    send_part(0)
    lcp[5].wait_recv()
    lcp[6].wait_recv()
    lcp[9].start()
    lcp[8].wait_recv()
    project(lat[2], 2)
    send_q(2)
    hctx[...] = modulate(ctx[...], 1)
    lcp[9].wait_recv()
    project(lat[3], 3, hctx)
    send_q(3)
    turn(1)
    send_part(1)
    wcp = round_y(wall, 256, wsend, wrecv, s, y, c)
    for k in (1, 2, 3, 4, 0):
        wcp[k].start()

    for u in range(UNITS):
        acc[u] = jnp.zeros_like(acc[u])
        peak[u] = jnp.full_like(peak[u], -1e30)

    @pl.when(primary)
    def _():
        pass_on(0, 1, 0)
        pass_on(0, 3, 0)

    def take_queries(part):
        settle(qb.at[part], qrecv.at[part])
        for r in range(6):
            tile, columns = 3 * part + r // 2, slice(128 * (r % 2), 128 * (r % 2) + 128)
            block = qb[part, 128 * r : 128 * r + 128, :].astype(F32).T.astype(BF)
            zero = jnp.zeros((64, 128), BF)
            qm[0, tile, 0:64, columns] = block[0:64]
            qm[0, tile, 64:128, columns] = zero
            qm[1, tile, 0:64, columns] = zero
            qm[1, tile, 64:128, columns] = block[64:128]

    take_queries(0)

    def score(u, at, keys, size):
        raw = jnp.dot(keys, qm[u % 2, u // 2], preferred_element_type=F32)
        sscr[at % (AHEAD + 1), 0:size, :] = raw
        tops[at % (AHEAD + 1)] = jnp.max(raw, axis=0, keepdims=True) * SCALE

    def weigh(u, at, lhs, size, bias):
        slot = at % (AHEAD + 1)
        top = tops[slot] if bias is None else tops[slot] + bias
        old = peak[u]
        new = jnp.maximum(old, top)
        peak[u] = new
        faded = jnp.exp2(old - new)
        shift = new if bias is None else new - bias
        probs = jnp.exp2(sscr[slot, 0:size, :] * SCALE - shift).astype(BF)
        acc[u] = acc[u] * faded + jnp.dot(lhs, probs, preferred_element_type=F32)

    def parts_of(n):
        if isinstance(n, int):
            pair = source(*FIRST[n]), source(*SECOND[n])
            return *pair, OWN if n in (3, 4) else 0, 0 if n in (1, 2) else OWN
        late = (n >= 8).astype(jnp.int32)
        by = 2 * (n - 8 * late)
        dz, dx, ez, ex = (((w[0] * (1 - late) + w[1] * late) >> by) % 4 for w in PACKED)
        return source(dz, dx), source(ez, ex), OWN * (n < 5).astype(jnp.int32)

    def rows_of(b, row, offset):
        if not isinstance(row, int):
            row = pl.multiple_of(row, 128)
        return kv[b, pl.ds(row + offset, HALF), :]

    def latent_keys(a, b, p, q):
        return jnp.concatenate([rows_of(a, p, 0), rows_of(b, q, 0)], axis=0)

    def latent_lhs(a, b, p, q):
        halves = rows_of(a, p, HALF), rows_of(b, q, HALF)
        lhs = jnp.concatenate([half[128 * k : 128 * k + 128] for half in halves for k in range(3)], axis=1)
        return jnp.concatenate([lhs, jnp.ones((16, OWN), BF)], axis=0)

    def stream(turns, keys, lhs, at=0, done=0, sizes=None, biases=None, after=None, ends=()):
        size = lambda which: OWN if sizes is None else sizes[which]
        for k in range(done, AHEAD):
            which, u = turns[k]
            score(u, at + k, keys[which], size(which))
        coming = list(turns) + list(ends)
        for k, (which, u) in enumerate(turns):
            if k + AHEAD < len(coming):
                other, v = coming[k + AHEAD]
                score(v, at + k + AHEAD, keys[other], size(other))
            weigh(u, at + k, lhs[which], size(which), None if biases is None else biases[which])
            if after is not None:
                after(which, u)

    @pl.when(jnp.logical_not(primary))
    def _():
        arrive(source(0, 1), 0)
        arrive(source(0, 3), 0)

    arrive(s, 0)
    arrive(s, 1)
    held = [parts_of(n) for n in range(4)]
    keys, lhs = [latent_keys(*h) for h in held[:2]], [latent_lhs(*h) for h in held[:2]]
    stream([(n, u) for n in range(2) for u in range(6)], keys, lhs)
    both = primary, jnp.logical_not(primary)

    @pl.when(both[0])
    def _():
        pass_on(1, 0, 0)
        pass_on(3, 0, 0, "sm")

    @pl.when(both[1])
    def _():
        arrive(source(1, 0), 0)
        arrive(source(3, 0), 0)

    stream([(0, u) for u in range(6)], [latent_keys(*held[2])], [latent_lhs(*held[2])])

    @pl.when(both[0])
    def _():
        pass_on(0, 3, 1)
        pass_on(0, 1, 1)
        go_on(3, 0, 0, "p")

    @pl.when(both[1])
    def _():
        arrive(source(0, 1), 1)
        arrive(source(0, 3), 1)

    send_far(0)
    send_far(1)
    take_queries(1)
    keys, lhs = [latent_keys(*h) for h in held], [latent_lhs(*h) for h in held[:3]]
    stream(
        [(n, u) for n in range(3) for u in range(6, UNITS)], keys, lhs, at=2, ends=[(3, u) for u in TURNS[:AHEAD]]
    )

    def step(n, now):
        following = parts_of(n + 1)

        @pl.when(primary)
        def _():
            for steps in ((3, 4, 5), (6, 7, 8), (10, 11, 12), (13, 14)):

                @pl.when((n >= steps[0]) & (n <= steps[-1]))
                def _():
                    for k in steps:

                        @pl.when(n == k)
                        def _():
                            for place in PASS[k]:
                                pass_on(*place)

        @pl.when(jnp.logical_not(primary))
        def _():
            @pl.when(n == 3)
            def _():
                arrive(following[0], 1)

            @pl.when(n != 3)
            def _():
                arrive(following[0], 0)

            arrive(following[1], 1)

        @pl.when(n == 9)
        def _():
            for k in (1, 2):
                wcp[k].wait_recv()
                wcp[k + 4].start()
            for k in (3, 4):
                wcp[k].wait_recv()
                wcp[k + 4].start()

        stream(
            [(0, u) for u in TURNS], [latent_keys(*now, OWN), latent_keys(*following, OWN)], [latent_lhs(*now, OWN)],
            done=AHEAD, ends=[(1, u) for u in TURNS[:AHEAD]],
        )
        return following

    last = lax.fori_loop(3, 15, step, (*held[3][:2], jnp.int32(OWN)))
    wcp[5].wait_recv()
    wcp[6].wait_recv()
    wcp[9].start()

    lane = lax.broadcasted_iota(jnp.int32, (1, 128), 1)
    owner = y * 2 + z // 2

    def pick(row):
        return jnp.sum(jnp.where(lane == z % 2, mods[owner, row : row + 1, :], 0.0), axis=1, keepdims=True)

    bias, lam = pick(13) * LOG2E, pick(12)
    head = y * 4 + z
    half = 1 - primary.astype(jnp.int32)

    def spot(h, row):
        return 8 * (h % 4 // 2 == row // 2).astype(jnp.int32) + h // 4 * 2 + h % 2

    def piece(k):
        offset = 3 * half if k < 8 else 1 + half
        target = ((y + offset) % 4) * 2 + k % 2
        src = nsend.at[ROWS * k : ROWS * k + ROWS]
        row = (z + (2, 1, 3, 0)[k % 8 // 2]) % 4
        late = (row // 2 == z // 2).astype(jnp.int32)
        return remote(src, nrm.at[spot(head, row)], osend.at[0], orecv.at[late], row * 4 + x, target)

    for k in range(8):
        pair = jnp.concatenate([kv[2 * k, 2 * OWN + CTXR : BLOCK, :], kv[2 * k + 1, 2 * OWN + CTXR : BLOCK, :]], axis=0)
        vctx[:, 128 * k : 128 * k + 128] = pair.astype(F32).T.astype(BF)
    size = 16 * CTXR
    whole = source(*FIRST[15]), source(*FIRST[15]), 0, OWN
    keys = (latent_keys(*whole), jnp.concatenate([kv[k, 2 * OWN : 2 * OWN + CTXR, :] for k in range(16)], axis=0))
    lhs = (latent_lhs(*whole), jnp.concatenate([vctx[...], jnp.ones((16, size), BF)], axis=0))
    turns = [(0, u) for u in TURNS[:4]]
    for k in range(0, UNITS, 2):
        turns += [(1, u) for u in TURNS[k : k + 2]] + [(0, u) for u in TURNS[k + 4 : k + 6]]
    sent = {5: range(8, 16), 0: range(0, 2), 1: range(2, 5), 2: range(5, 8)}

    def finish(which, u):
        if which == 0 or u % 2 == 0:
            return
        tile = u // 2
        one, two = acc[2 * tile], acc[2 * tile + 1]
        mixed = one[0:128] / one[128:129] - lam * (two[0:128] / two[128:129])
        normed = mixed * lax.rsqrt(jnp.mean(mixed * mixed, axis=0, keepdims=True) + EPS)
        for r in range(QT // 128):
            block = normed[:, 128 * r : 128 * r + 128].T * head_gain[...]
            row = QT * tile + 128 * r
            nsend[row : row + 128, :] = block.astype(BF)
        for e in sent.get(tile, ()):
            if e not in (6, 7):
                piece(e).start()
                continue
            mine = primary & (c == e - 6)

            @pl.when(mine)
            def _():
                src = nsend.at[ROWS * e : ROWS * e + ROWS]
                pltpu.make_async_copy(src, nrm.at[spot(head, z)], orecv.at[1]).start()

            @pl.when(jnp.logical_not(mine))
            def _():
                piece(e).start()

    stream(turns, keys, lhs, done=AHEAD, sizes=(OWN, size), biases=(None, bias), after=finish)

    for k in (0, 7, 8, 9):
        wcp[k].wait_recv()
    attended = jnp.zeros((ROWS, 2048), F32)
    for late, k in enumerate((1 - z // 2, z // 2)):
        settle(nrm.at[8 * late : 8 * late + 8], orecv.at[late])
        for p, off in enumerate((0, 3, 1, 2)):
            first = 8 * late + 2 * ((y + off) % 4)
            rows = jnp.concatenate([nrm[first], nrm[first + 1]], axis=1)
            part_of_w = wall[p, pl.ds(pl.multiple_of(256 * k, 256), 256), :]
            product = jnp.dot(rows, part_of_w, preferred_element_type=F32)
            attended = attended + product.astype(BF).astype(F32)
    rows = lat[0, pl.ds(pl.multiple_of(c * ROWS, 16), ROWS), :].astype(F32)
    out[...] = (rows + vector(2, 0) * attended.astype(BF).astype(F32)).astype(BF)

    for ref, rows, sem in ((lat, ROWS, lsend), (wall, 256, wsend)):
        settle(ref.at[0:2], sem.at[0])
        settle(ref.at[0], sem.at[1])
        settle(ref.at[0, 0:rows], sem.at[2])
    settle(part.at[0:15], msend.at[0])
    settle(mods.at[0:7], nsd.at[0])
    for i in range(2):
        for p in (1, 3):
            q_to(i, p).wait_send()

        @pl.when(distance(i) != 0)
        def _():
            for p in (0, 2):
                q_to(i, p).wait_send()
            for part in range(2):
                kv_to(i, part).wait_send()

    @pl.when(primary)
    def _():
        settle(kv.at[0:6], fwd.at[0])
        settle(kv.at[0:6], fwd.at[1])
        settle(kv, fwd.at[2])

    @pl.when(primary)
    def _():
        settle(nsend.at[0 : 15 * ROWS], osend.at[0])

    @pl.when(jnp.logical_not(primary))
    def _():
        settle(nsend, osend.at[0])


def per_device(
    latent, context, conditioning, norm_gain, mod_shift, mod_scale, mod_gate, w_query, w_key, w_value, w_out,
    lambdas, context_bias, head_gain,
):
    dma = pltpu.SemaphoreType.DMA
    vmem = pl.BlockSpec(memory_space=pltpu.VMEM)
    hbm = pl.BlockSpec(memory_space=pltpu.HBM)
    return pl.pallas_call(
        kernel,
        name="block",
        out_shape=jax.ShapeDtypeStruct(latent.shape, BF),
        in_specs=[hbm] * 14,
        out_specs=vmem,
        scratch_shapes=[
            pltpu.VMEM((4, PAIR, 2048), BF),
            pltpu.VMEM((CTXR, 2048), BF),
            pltpu.VMEM((CTXR, 2048), BF),
            pltpu.VMEM((3, 128, 256), BF),
            pltpu.VMEM((3, 2048, 256), BF),
            pltpu.VMEM((16, 16, 128), F32),
            pltpu.VMEM((16, 128), F32),
            pltpu.VMEM((16, 128), F32),
            pltpu.VMEM((8, 16, 128), F32),
            pltpu.VMEM((OWN, 256), F32),
            pltpu.VMEM((2, BLOCK, 128), BF),
            pltpu.VMEM((4, 2, PAIR, 128), BF),
            pltpu.VMEM((16, BLOCK, 128), BF),
            pltpu.VMEM((2, OWN, 128), BF),
            pltpu.VMEM((2, NQ, 128, QT), BF),
            pltpu.VMEM((128, 16 * CTXR), BF),
            pltpu.VMEM((AHEAD + 1, 16 * CTXR, QT), F32),
            pltpu.VMEM((AHEAD + 1, 1, QT), F32),
            pltpu.VMEM((UNITS, 144, QT), F32),
            pltpu.VMEM((UNITS, 1, QT), F32),
            pltpu.VMEM((1536, 128), BF),
            pltpu.VMEM((16, ROWS, 128), BF),
            pltpu.VMEM((4, 512, 2048), BF),
            pltpu.VMEM((2, 2048), F32),
            pltpu.VMEM((1, 2048), F32),
            pltpu.VMEM((1, 2), F32),
            pltpu.VMEM((1, 2), F32),
            pltpu.VMEM((1, 128), F32),
            dma((3,)), dma((10,)), dma((3,)), dma((10,)),
            dma((1,)), dma((1,)), dma((1,)), dma((1,)),
            dma((2, 2)), dma((2, 4)), dma((2, 16)), dma((2,)),
            dma((3,)),
            dma((1,)), dma((2,)), dma((14,)),
            pltpu.SemaphoreType.REGULAR,
        ],
        compiler_params=pltpu.CompilerParams(
            collective_id=0, has_side_effects=True, vmem_limit_bytes=60 * 2**20
        ),
    )(
        latent, context, conditioning, norm_gain.reshape(1, -1), mod_shift, mod_scale, mod_gate, w_query, w_key,
        w_value, w_out, lambdas.reshape(1, -1), context_bias.reshape(1, -1), head_gain.reshape(1, -1),
    )


def solution(mesh):
    return jax.shard_map(
        per_device,
        mesh=mesh,
        in_specs=(
            P(("sp", "tp"), None),
            P("sp", None),
            P(),
            P(),
            P("sp", "tp"),
            P("sp", "tp"),
            P("sp", "tp"),
            P(None, "tp"),
            P(None, "tp"),
            P(None, "tp"),
            P("tp", None),
            P("tp"),
            P("tp"),
            P(),
        ),
        out_specs=P(("sp", "tp"), None),
        check_vma=False,
    )
```

```python
import functools
import math

import jax
import jax.numpy as jnp
from jax import lax
from jax.experimental import pallas as pl
from jax.experimental.pallas import tpu as pltpu
from jax.sharding import PartitionSpec as P

EPS = 1e-06
MESH = pl.DeviceIdType.MESH
BF = jnp.bfloat16
F32 = jnp.float32
LOG2E = math.log2(math.e)
SCALE = LOG2E / 8.0
ROWS = 96
PAIR = 192
OWN = 768
CTXR = 64
BLOCK = 2 * OWN + 2 * CTXR
QT = 256
NQ = 6
UNITS = 12
AHEAD = 3
TURNS = (6, 7, 8, 9, 10, 11, 0, 1, 2, 3, 4, 5)
FIRST = (
    (0, 0), (0, 1), (1, 0), (0, 1), (1, 0), (0, 2), (1, 1), (1, 3), (3, 1), (3, 3), (2, 0), (1, 2), (2, 1), (2, 3),
    (3, 2), (2, 2),
)
SECOND = (FIRST[0], (0, 3), (3, 0), (0, 3), (3, 0)) + FIRST[5:]
PACKED = tuple(
    tuple(sum(place[k] << 2 * n for n, place in enumerate(order[8 * word : 8 * word + 8])) for word in range(2))
    for order in (FIRST, SECOND)
    for k in range(2)
)
PASS = {
    3: ((1, 0, 1), (3, 0, 1)), 4: ((0, 2, 0), (0, 2, 1)), 5: ((1, 1, 0), (1, 1, 1)), 6: ((1, 3, 0), (1, 3, 1)),
    7: ((3, 1, 0, "s"), (3, 1, 1, "s"), (2, 0, 0), (2, 0, 1), (3, 1, 0, "m"), (3, 1, 1, "m")), 8: ((3, 3, 0), (3, 3, 1)),
    10: ((1, 2, 0), (1, 2, 1)),
    11: ((2, 1, 0), (2, 1, 1)), 12: ((2, 3, 0), (2, 3, 1)), 13: ((3, 2, 0), (3, 2, 1)), 14: ((2, 2, 0), (2, 2, 1)),
}
HALF = OWN // 2
PARTS = ((0, OWN), (OWN, BLOCK - OWN))


def remote(src, dst, send, recv, sp, tp):
    return pltpu.make_async_remote_copy(
        src_ref=src, dst_ref=dst, send_sem=send, recv_sem=recv, device_id=(sp, tp), device_id_type=MESH
    )


def settle(ref, sem):
    pltpu.make_async_copy(ref, ref, sem).wait()


def round_y(buf, rows, send, recv, s, y, c):
    up, down = ((y + 1) % 4) * 2 + c, ((y + 3) % 4) * 2 + c
    sib = y * 2 + 1 - c
    half = rows // 2

    def at(slot, offset, size):
        return buf.at[slot, pl.ds(pl.multiple_of(c * rows + offset, 16), size)]

    def one(k, source, slot, offset, size, to):
        return remote(at(source, offset, size), at(slot, offset, size), send.at[(0, 1, 1, 1, 1, 2, 2, 0, 0, 0)[k]], recv.at[k], s, to)

    return [
        one(0, 0, 0, 0, rows, sib),
        one(1, 0, 1, 0, half, up),
        one(2, 0, 2, half, half, down),
        one(3, 0, 1, half, half, up),
        one(4, 0, 2, 0, half, down),
        one(5, 1, 3, 0, half, up),
        one(6, 2, 3, half, half, down),
        one(7, 1, 1, 0, rows, sib),
        one(8, 2, 2, 0, rows, sib),
        one(9, 3, 3, 0, rows, sib),
    ]


def kernel(
    latent, context, cond_in, gain_in, mod_shift, mod_scale, mod_gate, w_query, w_key, w_value, w_out, lambdas_in,
    bias_in, head_gain_in, out,
    lat, ctx, hctx, mod, wqkv, part, msg, msg2, mods, qv, kvown, qown, kv, qb, qm, vctx, sscr, tops, acc, peak, nsend, nrm,
    wall, cond, gain, lambdas, context_bias, head_gain, lsend, lrecv, wsend, wrecv, msend, mrecv, nsd, nrc, zsend, zqsend, kvrecv, qrecv, fwd,
    osend, orecv, local, ready,
):
    s, t = lax.axis_index("sp"), lax.axis_index("tp")
    z, x, y, c = s // 4, s % 4, t // 2, t % 2
    sib = y * 2 + 1 - c

    barrier = pltpu.get_barrier_semaphore()
    for d in range(1, 8):
        pl.semaphore_signal(barrier, inc=1, device_id=(s, (t + d) % 8), device_id_type=MESH)
    for d in range(1, 4):
        pl.semaphore_signal(barrier, inc=1, device_id=(z * 4 + (x + d) % 4, t), device_id_type=MESH)
        pl.semaphore_signal(barrier, inc=1, device_id=((z + d) % 4 * 4 + x, t), device_id_type=MESH)
    loads = [
        pltpu.make_async_copy(src, dst, local.at[k])
        for k, (src, dst) in enumerate(
            (
                (cond_in, cond),
                (mod_shift, mod.at[0]),
                (mod_scale, mod.at[1]),
                (mod_gate, mod.at[2]),
                (latent, lat.at[0, pl.ds(pl.multiple_of(c * ROWS, 16), ROWS)]),
                (context, ctx),
                (lambdas_in, lambdas),
                (bias_in, context_bias),
                (gain_in, gain),
                (head_gain_in, head_gain),
                (w_query, wqkv.at[0]),
                (w_key, wqkv.at[1]),
                (w_value, wqkv.at[2]),
                (w_out, wall.at[0, pl.ds(pl.multiple_of(c * 256, 256), 256)]),
            )
        )
    ]
    for copy in loads[:5]:
        copy.start()
    loads[0].wait()

    cols = cond[:, pl.ds(pl.multiple_of(s * 128, 128), 128)]
    activated = (cols / (1.0 + jnp.exp(-cols))).astype(BF)
    activated = jnp.concatenate([activated.astype(F32), jnp.zeros((6, 128), F32)], axis=0).astype(BF)
    msg[12:16, :] = jnp.zeros((4, 128), F32)
    for index in range(3):
        loads[index + 1].wait()
        product = jnp.dot(activated, mod[index], preferred_element_type=F32)
        for r in range(2):
            for half in range(2):
                line = index * 4 + r * 2 + half
                msg[line : line + 1, :] = product[r : r + 1, half * 128 : half * 128 + 128]
    loads[4].wait()
    for copy in loads[5:]:
        copy.start()
    pl.semaphore_wait(barrier, 13)

    lcp = round_y(lat, ROWS, lsend, lrecv, s, y, c)
    for k in (1, 2, 3, 4, 0):
        lcp[k].start()
    for d in range(1, 4):
        pl.semaphore_signal(ready, inc=1, device_id=((z + d) % 4 * 4 + x, t), device_id_type=MESH)
    pl.semaphore_wait(ready, 3)
    mcp = [remote(msg, part.at[s], msend.at[0], mrecv.at[0], (s + d) % 16, t) for d in range(1, 16)]
    for copy in mcp:
        copy.start()
    part[s] = msg[...]
    settle(part.at[0:15], mrecv.at[0])
    total = part[0]
    for k in range(1, 16):
        total = total + part[k]
    for copy in loads[5:]:
        copy.wait()
    msg2[...] = total
    msg2[12:13, 0:2] = lambdas[...]
    msg2[13:14, 0:2] = context_bias[...]
    ncp = [remote(msg2, mods.at[t], nsd.at[0], nrc.at[0], s, (t + d) % 8) for d in range(1, 8)]
    for copy in ncp:
        copy.start()
    mods[t] = msg2[...]
    lcp[1].wait_recv()
    lcp[5].start()
    lcp[2].wait_recv()
    lcp[6].start()
    lcp[3].wait_recv()
    lcp[7].start()
    lcp[4].wait_recv()
    lcp[8].start()
    settle(mods.at[0:7], nrc.at[0])

    def vector(index, r):
        row = index * 4 + r * 2
        return jnp.concatenate([mods[k, row + h : row + h + 1, :] for k in range(8) for h in range(2)], axis=1)

    def modulate(rows, r):
        rows = rows.astype(F32)
        normal = rows * lax.rsqrt(jnp.mean(rows * rows, axis=1, keepdims=True) + EPS)
        return (normal * (gain[...] * (1.0 + vector(1, r))) + vector(0, r)).astype(BF)

    def project(rows, p, more=None):
        size = rows.shape[0]
        hidden = modulate(rows, 0)
        queries = jnp.dot(hidden, wqkv[0], preferred_element_type=F32).astype(BF)
        if more is not None:
            hidden = jnp.concatenate([hidden, more[...]], axis=0)
        keys = jnp.dot(hidden, wqkv[1], preferred_element_type=F32).astype(BF)
        values = jnp.dot(hidden, wqkv[2], preferred_element_type=F32)
        first = PAIR * p + HALF * (p // 2)
        for i in range(2):
            columns = slice(128 * i, 128 * i + 128)
            kvown[i, first : first + size, :] = keys[:size, columns]
            for k in range(size // PAIR):
                qown[p + k, i] = queries[PAIR * k : PAIR * k + PAIR, columns]
            if more is not None:
                kvown[i, 2 * OWN : 2 * OWN + CTXR, :] = keys[size:, columns]
                kvown[i, 2 * OWN + CTXR : BLOCK, :] = values[size:, columns].astype(BF)
        qv[PAIR * p : PAIR * p + size, :] = values[:size]

    lcp[0].wait_recv()
    lcp[7].wait_recv()
    project(lat[0:2].reshape(2 * PAIR, 2048), 0)

    primary = c == z // 2
    plus, minus = z * 4 + (x + 1) % 4, z * 4 + (x + 3) % 4

    def turn(part):
        for a in range(3 * part, 3 * part + 3):
            for i in range(2):
                first = OWN * part + HALF + 128 * (a % 3)
                block = qv[128 * a : 128 * a + 128, 128 * i : 128 * i + 128]
                kvown[i, first : first + 128, :] = block.T.astype(BF)

    def distance(i):
        return (2 * c + i - z + 4) % 4

    def slot_of(dz):
        return 3 * (dz == 0).astype(jnp.int32) + (dz == 1).astype(jnp.int32) + 2 * (dz == 3).astype(jnp.int32)

    def q_to(i, p):
        rows = pl.ds(pl.multiple_of(PAIR * slot_of((z - 2 * c - i + 4) % 4), 16), PAIR)
        return remote(
            qown.at[p, i], qb.at[p // 2, rows], zqsend.at[2 if p % 2 else i], qrecv.at[p // 2],
            (2 * c + i) * 4 + x, sib if p % 2 else t,
        )

    def send_q(p):
        for i in range(2):
            if p % 2:
                q_to(i, p).start()
                continue

            @pl.when(distance(i) != 0)
            def _():
                q_to(i, p).start()

            @pl.when(distance(i) == 0)
            def _():
                rows = qb.at[p // 2, 3 * PAIR : 4 * PAIR]
                pltpu.make_async_copy(qown.at[p, i], rows, qrecv.at[p // 2]).start()

    def part_of(ref, b, part):
        return ref.at[b, pl.ds(*PARTS[part])]

    def kv_to(i, part):
        return remote(
            part_of(kvown, i, part), part_of(kv, s, part), zsend.at[i], kvrecv.at[part, s],
            (2 * c + i) * 4 + x, t,
        )

    def source(dz, dx):
        return ((z + dz) % 4) * 4 + (x + dx) % 4

    def onward(dz, dx, part):
        b = source(dz, dx)
        src = part_of(kvown, z % 2, part) if (dz, dx) == (0, 0) else part_of(kv, b, part)
        dst = part_of(kv, b, part)
        copies = {}
        if dx == 0 or (dx == 3 and dz < 2):
            copies["p"] = remote(src, dst, fwd.at[0], kvrecv.at[part, b], plus, t)
        if dx == 0 or (dx == 1 and dz >= 2):
            copies["m"] = remote(src, dst, fwd.at[1], kvrecv.at[part, b], minus, t)
        copies["s"] = remote(src, dst, fwd.at[2], kvrecv.at[part, b], s, sib)
        return copies

    def arrive(b, part):
        pltpu.make_async_copy(part_of(kvown, 0, part), part_of(kv, b, part), kvrecv.at[part, b]).wait()

    def go_on(dz, dx, part, ways="spm"):
        for way, copy in onward(dz, dx, part).items():
            if way in ways:
                copy.start()

    def pass_on(dz, dx, part, ways="spm"):
        if "s" in ways:
            arrive(source(dz, dx), part)
        go_on(dz, dx, part, ways)

    def send_part(part):
        for i in range(2):

            @pl.when(distance(i) == 0)
            def _():
                pltpu.make_async_copy(part_of(kvown, i, part), part_of(kv, s, part), kvrecv.at[part, s]).start()

        @pl.when(primary)
        def _():
            go_on(0, 0, part)

        for i in range(2):

            @pl.when(distance(i) % 2 == 1)
            def _():
                kv_to(i, part).start()

    def send_far(part):
        for i in range(2):

            @pl.when(distance(i) == 2)
            def _():
                kv_to(i, part).start()

    send_q(0)
    send_q(1)
    turn(0)
    send_part(0)
    lcp[5].wait_recv()
    lcp[6].wait_recv()
    lcp[9].start()
    lcp[8].wait_recv()
    project(lat[2], 2)
    send_q(2)
    hctx[...] = modulate(ctx[...], 1)
    lcp[9].wait_recv()
    project(lat[3], 3, hctx)
    send_q(3)
    turn(1)
    send_part(1)
    wcp = round_y(wall, 256, wsend, wrecv, s, y, c)
    for k in (1, 2, 3, 4, 0):
        wcp[k].start()

    for u in range(UNITS):
        acc[u] = jnp.zeros_like(acc[u])
        peak[u] = jnp.full_like(peak[u], -1e30)

    @pl.when(primary)
    def _():
        pass_on(0, 1, 0)
        pass_on(0, 3, 0)

    def take_queries(part):
        settle(qb.at[part], qrecv.at[part])
        for r in range(6):
            tile, columns = 3 * part + r // 2, slice(128 * (r % 2), 128 * (r % 2) + 128)
            block = qb[part, 128 * r : 128 * r + 128, :].astype(F32).T.astype(BF)
            zero = jnp.zeros((64, 128), BF)
            qm[0, tile, 0:64, columns] = block[0:64]
            qm[0, tile, 64:128, columns] = zero
            qm[1, tile, 0:64, columns] = zero
            qm[1, tile, 64:128, columns] = block[64:128]

    take_queries(0)

    def score(u, at, keys, size):
        raw = jnp.dot(keys, qm[u % 2, u // 2], preferred_element_type=F32)
        sscr[at % (AHEAD + 1), 0:size, :] = raw
        tops[at % (AHEAD + 1)] = jnp.max(raw, axis=0, keepdims=True) * SCALE

    def weigh(u, at, lhs, size, bias):
        slot = at % (AHEAD + 1)
        top = tops[slot] if bias is None else tops[slot] + bias
        old = peak[u]
        new = jnp.maximum(old, top)
        peak[u] = new
        faded = jnp.exp2(old - new)
        shift = new if bias is None else new - bias
        probs = jnp.exp2(sscr[slot, 0:size, :] * SCALE - shift).astype(BF)
        acc[u] = acc[u] * faded + jnp.dot(lhs, probs, preferred_element_type=F32)

    def parts_of(n):
        if isinstance(n, int):
            pair = source(*FIRST[n]), source(*SECOND[n])
            return *pair, OWN if n in (3, 4) else 0, 0 if n in (1, 2) else OWN
        late = (n >= 8).astype(jnp.int32)
        by = 2 * (n - 8 * late)
        dz, dx, ez, ex = (((w[0] * (1 - late) + w[1] * late) >> by) % 4 for w in PACKED)
        return source(dz, dx), source(ez, ex), OWN * (n < 5).astype(jnp.int32)

    def rows_of(b, row, offset):
        if not isinstance(row, int):
            row = pl.multiple_of(row, 128)
        return kv[b, pl.ds(row + offset, HALF), :]

    def latent_keys(a, b, p, q):
        return jnp.concatenate([rows_of(a, p, 0), rows_of(b, q, 0)], axis=0)

    def latent_lhs(a, b, p, q):
        halves = rows_of(a, p, HALF), rows_of(b, q, HALF)
        lhs = jnp.concatenate([half[128 * k : 128 * k + 128] for half in halves for k in range(3)], axis=1)
        return jnp.concatenate([lhs, jnp.ones((16, OWN), BF)], axis=0)

    def stream(turns, keys, lhs, at=0, done=0, sizes=None, biases=None, after=None, ends=()):
        size = lambda which: OWN if sizes is None else sizes[which]
        for k in range(done, AHEAD):
            which, u = turns[k]
            score(u, at + k, keys[which], size(which))
        coming = list(turns) + list(ends)
        for k, (which, u) in enumerate(turns):
            if k + AHEAD < len(coming):
                other, v = coming[k + AHEAD]
                score(v, at + k + AHEAD, keys[other], size(other))
            weigh(u, at + k, lhs[which], size(which), None if biases is None else biases[which])
            if after is not None:
                after(which, u)

    @pl.when(jnp.logical_not(primary))
    def _():
        arrive(source(0, 1), 0)
        arrive(source(0, 3), 0)

    arrive(s, 0)
    arrive(s, 1)
    held = [parts_of(n) for n in range(4)]
    keys, lhs = [latent_keys(*h) for h in held[:2]], [latent_lhs(*h) for h in held[:2]]
    stream([(n, u) for n in range(2) for u in range(6)], keys, lhs)
    both = primary, jnp.logical_not(primary)

    @pl.when(both[0])
    def _():
        pass_on(1, 0, 0)
        pass_on(3, 0, 0, "sm")

    @pl.when(both[1])
    def _():
        arrive(source(1, 0), 0)
        arrive(source(3, 0), 0)

    stream([(0, u) for u in range(6)], [latent_keys(*held[2])], [latent_lhs(*held[2])])

    @pl.when(both[0])
    def _():
        pass_on(0, 3, 1)
        pass_on(0, 1, 1)
        go_on(3, 0, 0, "p")

    @pl.when(both[1])
    def _():
        arrive(source(0, 1), 1)
        arrive(source(0, 3), 1)

    send_far(0)
    send_far(1)
    take_queries(1)
    keys, lhs = [latent_keys(*h) for h in held], [latent_lhs(*h) for h in held[:3]]
    stream(
        [(n, u) for n in range(3) for u in range(6, UNITS)], keys, lhs, at=2, ends=[(3, u) for u in TURNS[:AHEAD]]
    )

    def step(n, now):
        following = parts_of(n + 1)

        @pl.when(primary)
        def _():
            for steps in ((3, 4, 5), (6, 7, 8), (10, 11, 12), (13, 14)):

                @pl.when((n >= steps[0]) & (n <= steps[-1]))
                def _():
                    for k in steps:

                        @pl.when(n == k)
                        def _():
                            for place in PASS[k]:
                                pass_on(*place)

        @pl.when(jnp.logical_not(primary))
        def _():
            @pl.when(n == 3)
            def _():
                arrive(following[0], 1)

            @pl.when(n != 3)
            def _():
                arrive(following[0], 0)

            arrive(following[1], 1)

        @pl.when(n == 9)
        def _():
            for k in (1, 2):
                wcp[k].wait_recv()
                wcp[k + 4].start()
            for k in (3, 4):
                wcp[k].wait_recv()
                wcp[k + 4].start()

        stream(
            [(0, u) for u in TURNS], [latent_keys(*now, OWN), latent_keys(*following, OWN)], [latent_lhs(*now, OWN)],
            done=AHEAD, ends=[(1, u) for u in TURNS[:AHEAD]],
        )
        return following

    last = lax.fori_loop(3, 15, step, (*held[3][:2], jnp.int32(OWN)))
    wcp[5].wait_recv()
    wcp[6].wait_recv()
    wcp[9].start()

    lane = lax.broadcasted_iota(jnp.int32, (1, 128), 1)
    owner = y * 2 + z // 2

    def pick(row):
        return jnp.sum(jnp.where(lane == z % 2, mods[owner, row : row + 1, :], 0.0), axis=1, keepdims=True)

    bias, lam = pick(13) * LOG2E, pick(12)
    head = y * 4 + z
    half = 1 - primary.astype(jnp.int32)

    def spot(h, row):
        return 8 * (h % 4 // 2 == row // 2).astype(jnp.int32) + h // 4 * 2 + h % 2

    def piece(k):
        offset = 3 * half if k < 8 else 1 + half
        target = ((y + offset) % 4) * 2 + k % 2
        src = nsend.at[ROWS * k : ROWS * k + ROWS]
        row = (z + (2, 1, 3, 0)[k % 8 // 2]) % 4
        late = (row // 2 == z // 2).astype(jnp.int32)
        return remote(src, nrm.at[spot(head, row)], osend.at[0], orecv.at[late], row * 4 + x, target)

    for k in range(8):
        pair = jnp.concatenate([kv[2 * k, 2 * OWN + CTXR : BLOCK, :], kv[2 * k + 1, 2 * OWN + CTXR : BLOCK, :]], axis=0)
        vctx[:, 128 * k : 128 * k + 128] = pair.astype(F32).T.astype(BF)
    size = 16 * CTXR
    whole = source(*FIRST[15]), source(*FIRST[15]), 0, OWN
    keys = (latent_keys(*whole), jnp.concatenate([kv[k, 2 * OWN : 2 * OWN + CTXR, :] for k in range(16)], axis=0))
    lhs = (latent_lhs(*whole), jnp.concatenate([vctx[...], jnp.ones((16, size), BF)], axis=0))
    turns = [(0, u) for u in TURNS[:4]]
    for k in range(0, UNITS, 2):
        turns += [(1, u) for u in TURNS[k : k + 2]] + [(0, u) for u in TURNS[k + 4 : k + 6]]
    sent = {5: range(8, 16), 0: range(0, 2), 1: range(2, 5), 2: range(5, 8)}

    def finish(which, u):
        if which == 0 or u % 2 == 0:
            return
        tile = u // 2
        one, two = acc[2 * tile], acc[2 * tile + 1]
        mixed = one[0:128] / one[128:129] - lam * (two[0:128] / two[128:129])
        normed = mixed * lax.rsqrt(jnp.mean(mixed * mixed, axis=0, keepdims=True) + EPS)
        for r in range(QT // 128):
            block = normed[:, 128 * r : 128 * r + 128].T * head_gain[...]
            row = QT * tile + 128 * r
            nsend[row : row + 128, :] = block.astype(BF)
        for e in sent.get(tile, ()):
            if e not in (6, 7):
                piece(e).start()
                continue
            mine = primary & (c == e - 6)

            @pl.when(mine)
            def _():
                src = nsend.at[ROWS * e : ROWS * e + ROWS]
                pltpu.make_async_copy(src, nrm.at[spot(head, z)], orecv.at[1]).start()

            @pl.when(jnp.logical_not(mine))
            def _():
                piece(e).start()

    stream(turns, keys, lhs, done=AHEAD, sizes=(OWN, size), biases=(None, bias), after=finish)

    for k in (0, 7, 8, 9):
        wcp[k].wait_recv()
    attended = jnp.zeros((ROWS, 2048), F32)
    for late, k in enumerate((1 - z // 2, z // 2)):
        settle(nrm.at[8 * late : 8 * late + 8], orecv.at[late])
        for p, off in enumerate((0, 3, 1, 2)):
            first = 8 * late + 2 * ((y + off) % 4)
            rows = jnp.concatenate([nrm[first], nrm[first + 1]], axis=1)
            part_of_w = wall[p, pl.ds(pl.multiple_of(256 * k, 256), 256), :]
            product = jnp.dot(rows, part_of_w, preferred_element_type=F32)
            attended = attended + product.astype(BF).astype(F32)
    rows = lat[0, pl.ds(pl.multiple_of(c * ROWS, 16), ROWS), :].astype(F32)
    out[...] = (rows + vector(2, 0) * attended.astype(BF).astype(F32)).astype(BF)

    for ref, rows, sem in ((lat, ROWS, lsend), (wall, 256, wsend)):
        settle(ref.at[0:2], sem.at[0])
        settle(ref.at[0], sem.at[1])
        settle(ref.at[0, 0:rows], sem.at[2])
    settle(part.at[0:15], msend.at[0])
    settle(mods.at[0:7], nsd.at[0])
    settle(qb.at[0], zqsend.at[2])
    for i in range(2):

        @pl.when(distance(i) != 0)
        def _():
            settle(qb.at[0, 0 : 2 * PAIR], zqsend.at[i])
            settle(kv.at[0], zsend.at[i])

    @pl.when(primary)
    def _():
        settle(kv.at[0:6], fwd.at[0])
        settle(kv.at[0:6], fwd.at[1])
        settle(kv, fwd.at[2])

    @pl.when(primary)
    def _():
        settle(nsend.at[0 : 15 * ROWS], osend.at[0])

    @pl.when(jnp.logical_not(primary))
    def _():
        settle(nsend, osend.at[0])


def per_device(
    latent, context, conditioning, norm_gain, mod_shift, mod_scale, mod_gate, w_query, w_key, w_value, w_out,
    lambdas, context_bias, head_gain,
):
    dma = pltpu.SemaphoreType.DMA
    vmem = pl.BlockSpec(memory_space=pltpu.VMEM)
    hbm = pl.BlockSpec(memory_space=pltpu.HBM)
    return pl.pallas_call(
        kernel,
        name="block",
        out_shape=jax.ShapeDtypeStruct(latent.shape, BF),
        in_specs=[hbm] * 14,
        out_specs=vmem,
        scratch_shapes=[
            pltpu.VMEM((4, PAIR, 2048), BF),
            pltpu.VMEM((CTXR, 2048), BF),
            pltpu.VMEM((CTXR, 2048), BF),
            pltpu.VMEM((3, 128, 256), BF),
            pltpu.VMEM((3, 2048, 256), BF),
            pltpu.VMEM((16, 16, 128), F32),
            pltpu.VMEM((16, 128), F32),
            pltpu.VMEM((16, 128), F32),
            pltpu.VMEM((8, 16, 128), F32),
            pltpu.VMEM((OWN, 256), F32),
            pltpu.VMEM((2, BLOCK, 128), BF),
            pltpu.VMEM((4, 2, PAIR, 128), BF),
            pltpu.VMEM((16, BLOCK, 128), BF),
            pltpu.VMEM((2, OWN, 128), BF),
            pltpu.VMEM((2, NQ, 128, QT), BF),
            pltpu.VMEM((128, 16 * CTXR), BF),
            pltpu.VMEM((AHEAD + 1, 16 * CTXR, QT), F32),
            pltpu.VMEM((AHEAD + 1, 1, QT), F32),
            pltpu.VMEM((UNITS, 144, QT), F32),
            pltpu.VMEM((UNITS, 1, QT), F32),
            pltpu.VMEM((1536, 128), BF),
            pltpu.VMEM((16, ROWS, 128), BF),
            pltpu.VMEM((4, 512, 2048), BF),
            pltpu.VMEM((2, 2048), F32),
            pltpu.VMEM((1, 2048), F32),
            pltpu.VMEM((1, 2), F32),
            pltpu.VMEM((1, 2), F32),
            pltpu.VMEM((1, 128), F32),
            dma((3,)), dma((10,)), dma((3,)), dma((10,)),
            dma((1,)), dma((1,)), dma((1,)), dma((1,)),
            dma((2,)), dma((3,)), dma((2, 16)), dma((2,)),
            dma((3,)),
            dma((1,)), dma((2,)), dma((14,)),
            pltpu.SemaphoreType.REGULAR,
        ],
        compiler_params=pltpu.CompilerParams(
            collective_id=0, has_side_effects=True, vmem_limit_bytes=60 * 2**20
        ),
    )(
        latent, context, conditioning, norm_gain.reshape(1, -1), mod_shift, mod_scale, mod_gate, w_query, w_key,
        w_value, w_out, lambdas.reshape(1, -1), context_bias.reshape(1, -1), head_gain.reshape(1, -1),
    )


def solution(mesh):
    return jax.shard_map(
        per_device,
        mesh=mesh,
        in_specs=(
            P(("sp", "tp"), None),
            P("sp", None),
            P(),
            P(),
            P("sp", "tp"),
            P("sp", "tp"),
            P("sp", "tp"),
            P(None, "tp"),
            P(None, "tp"),
            P(None, "tp"),
            P("tp", None),
            P("tp"),
            P("tp"),
            P(),
        ),
        out_specs=P(("sp", "tp"), None),
        check_vma=False,
    )
```
